256 devices in a mesh: dp: 4 (over x), kv: 32 (over z, y), tp: 2 (over core).
Axes of the slice: x: 4, y: 4, z: 8, core: 2. Of those that a mesh axis runs over, the one named last changes fastest.
Arguments:
- tokens: bfloat16 [4, 8192, 1024], P('dp', 'kv', 'tp'), may hold values from -6 to 6
- norm_gain: float32 [1024], replicated, may hold values from 0.1 to 1.9
- w_query: bfloat16 [1024, 1024], P(None, 'tp'), may hold values from -0.1875 to 0.1875
- w_key: bfloat16 [1024, 256], P(None, 'tp'), may hold values from -0.1875 to 0.1875
- w_value: bfloat16 [1024, 256], P(None, 'tp'), may hold values from -0.1875 to 0.1875
- q_gain: float32 [64], replicated, may hold values from 0.1 to 1.9
- k_gain: float32 [64], replicated, may hold values from 0.1 to 1.9
- w_out: bfloat16 [1024, 1024], P('tp'), may hold values from -4 to 4
- chosen: int32 [4, 256, 16], P('dp', 'kv'), may hold values from -1 to 255, as said below
Outputs:
- mixed: bfloat16 [4, 8192, 1024], P('dp', 'kv', 'tp')
- log_total: float32 [4, 16, 8192], P('dp', 'tp', 'kv')
The draws below stay inside these ranges and needn't reach their ends.
Inputs may be any that keep to these rules, and one draw needn't show every extreme that they name: Each row of chosen (one query block b) holds distinct key block numbers, all at most b, and -1 for empty entries; b itself is always present; a row is full (16 blocks) whenever at least 16 blocks may be chosen by it. Over the 8 rows of one index of kv, the chosen blocks that lie on any one other index of kv are at most 4 distinct ones, and exactly 4 of those on the index just before, for every index but the first. Some blocks are chosen far more often than others.
All inputs are finite; a program needn't handle non-finite values.
Results may differ from the reference program's by a relative error of at most 0.015.
Values may be sent and summed in bfloat16 or wider, within the bound.
A program may use at most 64 MiB of HBM per device.

```python
import jax
import jax.numpy as jnp
from jax import lax

D = 1024
H = 16
HD = 64
KVH = 4
BLK = 32
TOPB = 16
MOST = 4
NB_DEV = 8
NBLK = 256
SEQ = 8192
SEQS = 4
N_KV = 32


def chosen_sequence(seq_key):
    pop_key, cand_key, pick_key = jax.random.split(jax.random.fold_in(seq_key, 11), 3)
    block_ids = jnp.arange(NBLK, dtype=jnp.int32)
    owner_dev = block_ids // NB_DEV
    level_draw = jax.random.randint(pop_key, (NBLK,), 0, 4)
    appeal = level_draw * level_draw
    devices = jnp.arange(N_KV, dtype=jnp.int32)[:, None]
    noise_draw = jax.random.randint(cand_key, (N_KV, NBLK), 0, 1000)
    base_score = (appeal[None, :] * 1000 + noise_draw) * NBLK + block_ids[None, :]
    pinned = (block_ids[None, :] == devices * NB_DEV - 1) | (block_ids[None, :] == (devices - N_KV // 2) * NB_DEV)
    priority = jnp.where(pinned, base_score + 268435456, base_score).reshape(N_KV, N_KV, NB_DEV)
    threshold_val = lax.top_k(priority, MOST)[0][..., -1:]
    kept_set = (priority >= threshold_val).reshape(N_KV, NBLK)
    kept_set = jnp.where(owner_dev[None, :] == devices, True, kept_set & (owner_dev[None, :] < devices))
    query_ids = block_ids[:, None]
    row_dev = query_ids // NB_DEV
    candidate = kept_set[row_dev[:, 0]]
    allowed = candidate & (block_ids[None, :] <= query_ids)
    local_pos = query_ids % NB_DEV
    forced = (block_ids[None, :] == query_ids) | (block_ids[None, :] == query_ids - 1)
    forced = forced | (local_pos == 0) & (block_ids[None, :] == (row_dev - N_KV // 2) * NB_DEV)
    forced = forced | (local_pos == NB_DEV - 1) & candidate & (owner_dev[None, :] == row_dev - 1)
    second_noise = jax.random.randint(pick_key, (NBLK, NBLK), 0, 1000)
    ranking = (appeal[None, :] * 1000 + second_noise) * NBLK + block_ids[None, :]
    ranking = jnp.where(forced, ranking + 268435456, ranking)
    ranking = jnp.where(allowed, ranking, -1 - block_ids[None, :])
    top_vals, top_ids = lax.top_k(ranking, TOPB)
    return jnp.where(top_vals >= 0, top_ids, -1).astype(jnp.int32)


def draw_chosen(key, part):
    seq_keys = jax.random.split(jax.random.fold_in(key, 5), SEQS)
    return jax.vmap(chosen_sequence)(seq_keys)


def block_scale(key, dims, cuts, least, largest):
    factor_of = 1.0
    for position, parts in cuts:
        steps = jax.random.uniform(jax.random.fold_in(jax.random.fold_in(key, 6), position), (parts,), jnp.float32, least / len(cuts), largest / len(cuts))
        factor_of = factor_of * jnp.repeat(jnp.exp(steps), dims[position] // parts).reshape((-1,) + (1,) * (len(dims) - 1 - position))
    return factor_of


def gaussian(rng, extent, scale, bound, cuts=(), kind=jnp.bfloat16):
    entries = jax.random.normal(rng, extent, jnp.float32) * scale
    if len(cuts) > 0:
        entries = block_scale(rng, extent, cuts, -0.22, 0.18) * entries
    return jnp.clip(entries, min=-bound, max=bound).astype(kind)


def setup_inputs(seed: int = 0) -> dict:
    key_of = jax.random.split(jax.random.key(seed), 10)
    return {
        "tokens": gaussian(key_of[0], (SEQS, SEQ, D), 1.0, 6.0, ((0, 4), (1, 32), (2, 2))),
        "norm_gain": jnp.clip(1.0 + 0.18 * jax.random.normal(key_of[1], (D,), jnp.float32), 0.1, 1.9),
        "w_query": gaussian(key_of[2], (D, H * HD), D ** -0.5, 0.1875, ((1, 2),)),
        "w_key": gaussian(key_of[3], (D, KVH * HD), D ** -0.5, 0.1875, ((1, 2),)),
        "w_value": gaussian(key_of[4], (D, KVH * HD), D ** -0.5, 0.1875, ((1, 2),)),
        "q_gain": jnp.clip(1.0 + 0.18 * jax.random.normal(key_of[5], (HD,), jnp.float32), 0.1, 1.9),
        "k_gain": jnp.clip(1.0 + 0.18 * jax.random.normal(key_of[6], (HD,), jnp.float32), 0.1, 1.9),
        "w_out": gaussian(key_of[7], (H * HD, D), (8 * (H * HD) ** -0.5), 4.0, ((0, 2),)),
        "chosen": draw_chosen(jax.random.fold_in(key_of[9], 71), 0),
    }


epsilon = 1e-06
alibi_reach = 4.0

def rms_norm(values, gain):
    return values * lax.rsqrt(lax.optimization_barrier(jnp.mean(values * values, axis=-1, keepdims=True)) + epsilon) * gain.astype(jnp.float32)

def reference(tokens, norm_gain, w_query, w_key, w_value, q_gain, k_gain, w_out, chosen):
    group_size = H // KVH
    slopes = jnp.exp2(-8.0 * jnp.arange(1, H + 1, dtype=jnp.float32) / H)

    def one_sequence(seq_args):
        sequence_tokens, sequence_chosen = seq_args
        hidden = rms_norm(sequence_tokens.astype(jnp.float32), norm_gain).astype(jnp.bfloat16)
        queries = rms_norm(jnp.dot(hidden, w_query, preferred_element_type=jnp.float32).reshape(SEQ, H, HD), q_gain).astype(jnp.bfloat16)
        key_rows = rms_norm(jnp.dot(hidden, w_key, preferred_element_type=jnp.float32).reshape(SEQ, KVH, HD), k_gain).astype(jnp.bfloat16)
        value_rows = jnp.dot(hidden, w_value, preferred_element_type=jnp.float32).astype(jnp.bfloat16).reshape(SEQ, KVH, HD)
        key_blocks = key_rows.reshape(NBLK, BLK, KVH, HD)
        value_blocks = value_rows.reshape(NBLK, BLK, KVH, HD)

        def one_block(block_args):
            block_index, requested, query_block = block_args
            present = requested >= 0
            clamped = jnp.maximum(requested, 0).astype(jnp.int32)
            picked_keys = jnp.repeat(key_blocks[clamped].reshape(TOPB * BLK, KVH, HD), group_size, axis=1)
            picked_values = jnp.repeat(value_blocks[clamped].reshape(TOPB * BLK, KVH, HD), group_size, axis=1)
            scores = jnp.einsum('qhd,khd->hqk', query_block.astype(jnp.float32), picked_keys.astype(jnp.float32), precision=lax.Precision.HIGHEST) * HD ** (-0.5)
            query_pos = block_index * BLK + jnp.arange(BLK, dtype=jnp.int32)
            key_pos = (clamped[:, None] * BLK + jnp.arange(BLK, dtype=jnp.int32)[None, :]).reshape(-1)
            offset = (query_pos[:, None] - key_pos[None, :]).astype(jnp.float32)
            scores = scores - slopes[:, None, None] * offset[None] * alibi_reach / SEQ
            allowed = jnp.repeat(present, BLK)[None, :] & (offset >= 0)
            scores = jnp.where(allowed[None], scores, -jnp.inf)
            row_max = lax.optimization_barrier(jnp.max(scores, axis=-1, keepdims=True))
            weights = jnp.exp(scores - row_max)
            row_sum = lax.optimization_barrier(jnp.sum(weights, axis=-1, keepdims=True))
            block_log = row_max[..., 0] + jnp.log(row_sum[..., 0])
            probs = lax.optimization_barrier((weights / row_sum).astype(jnp.bfloat16))
            block_out = jnp.einsum('hqk,khd->qhd', probs.astype(jnp.float32), picked_values.astype(jnp.float32), precision=lax.Precision.HIGHEST)
            return (block_out, block_log)
        block_ids = jnp.arange(NBLK, dtype=jnp.int32)
        block_out, block_log = lax.map(one_block, (block_ids, sequence_chosen, queries.reshape(NBLK, BLK, H, HD)))
        attended = block_out.reshape(SEQ, H * HD).astype(jnp.bfloat16)
        mixed = jnp.dot(attended, w_out, preferred_element_type=jnp.float32).astype(jnp.bfloat16)
        log_total = block_log.transpose(1, 0, 2).reshape(H, SEQ)
        return (mixed, log_total)
    mixed, log_total = lax.map(one_sequence, (tokens, chosen))
    return (mixed, log_total)
```

```python
import functools
import math

import jax
import jax.numpy as jnp
from jax import lax
from jax.experimental import pallas as pl
from jax.experimental.pallas import tpu as pltpu
from jax.sharding import PartitionSpec as P

HD = 64
BLK = 32
LANES = 128
PARTS = 2
N_Y = 4
CHUNKS = 2
UP, DOWN, LEFT, RIGHT = range(4)

epsilon = 1e-06
alibi_reach = 4.0
LOG2E = math.log2(math.e)
F32 = jnp.float32
BF16 = jnp.bfloat16
NT = (((1,), (1,)), ((), ()))
MESH = pl.DeviceIdType.MESH


def iota(shape, dim):
    return lax.broadcasted_iota(jnp.int32, shape, dim)


def dot(a, b):
    return jnp.dot(a, b, preferred_element_type=F32)


def dot_nt(a, b):
    return lax.dot_general(a, b, NT, preferred_element_type=F32)


def kernel(
    n_kv,
    tok, gain, wq, wk, wv, qg, kg, wo, ch,
    out_ref, lt_ref,
    x_buf, ch_s, ch_buf, raw_s, w_buf, wo_buf, g_buf, qg_buf, kg_buf,
    q_s, kv_all, kp_s, att_s, sum_s, part_send, part_recv,
    load_sem, x_sem, send_sem, recv_sem, part_sem,
):
    me = lax.axis_index("kv")
    tp = lax.axis_index("tp")
    partner = 1 - tp
    n_z = n_kv // N_Y
    z = me // N_Y
    y = me % N_Y
    rows, half = tok.shape
    q_cols = wq.shape[1]
    k_cols = wk.shape[1]
    heads = q_cols // HD
    kv_heads = k_cols // HD
    group = heads // kv_heads
    n_heads = heads * lax.axis_size("tp")
    nb, entries = ch.shape
    width = half * 2
    seq_len = rows * n_kv
    alibi = alibi_reach / seq_len
    keys = entries * BLK

    def span(start):
        return pl.ds(pl.multiple_of(start * half, LANES), half)

    loads = {}

    def load(name, src, dst):
        copy = pltpu.make_async_copy(src, dst, load_sem.at[len(loads)])
        copy.start()
        loads[name] = copy

    sides = ((0, tp), (1, partner))
    load("tok", tok, x_buf.at[0])
    load("g0", gain.at[:, span(tp)], g_buf.at[0])
    for side, which in sides:
        load(f"wk{side}", wk.at[span(which), :], w_buf.at[side, :, q_cols:q_cols + k_cols])
        load(f"wv{side}", wv.at[span(which), :], w_buf.at[side, :, q_cols + k_cols:q_cols + 2 * k_cols])
        load(f"wq{side}", wq.at[span(which), :], w_buf.at[side, :, 0:q_cols])
    load("g1", gain.at[:, span(partner)], g_buf.at[1])
    load("qg", qg, qg_buf)
    load("kg", kg, kg_buf)
    load("chs", ch, ch_s)
    load("ch", ch, ch_buf)
    for side, which in sides:
        for head in range(heads):
            to = head % group * LANES + head // group * HD
            load(f"wo{side}{head}", wo.at[head * HD:(head + 1) * HD, span(which)],
                 wo_buf.at[side, to:to + HD])

    def device(row, col):
        return lax.rem(row + n_z, n_z) * N_Y + lax.rem(col + N_Y, N_Y)

    neighbour = {
        UP: device(z + 1, y), DOWN: device(z - 1, y),
        LEFT: device(z, y - 1), RIGHT: device(z, y + 1),
    }
    barrier = pltpu.get_barrier_semaphore()
    pl.semaphore_signal(barrier, inc=1, device_id={"tp": partner}, device_id_type=MESH)
    for target in neighbour.values():
        pl.semaphore_signal(barrier, inc=1, device_id={"kv": target}, device_id_type=MESH)

    def scaled(side):
        x = x_buf[side].astype(F32)
        return (x * g_buf[side]).astype(BF16), jnp.sum(x * x, axis=1, keepdims=True)

    loads["tok"].wait()
    pl.semaphore_wait(barrier, 5)
    x_copy = pltpu.make_async_remote_copy(
        x_buf.at[0], x_buf.at[1], x_sem.at[0], x_sem.at[1],
        device_id={"tp": partner}, device_id_type=MESH)
    x_copy.start()

    for name in ("g0", "wk0", "wv0", "wq0"):
        loads[name].wait()
    y0, sq0 = scaled(0)
    raw_s[...] = dot(y0, w_buf[0])

    same_head = jnp.where(
        iota((LANES, LANES), 0) // HD == iota((LANES, LANES), 1) // HD, 1.0, 0.0).astype(BF16)

    def head_norm(v, gain_row):
        sq = v * v
        hi = sq.astype(BF16)
        lo = (sq - hi.astype(F32)).astype(BF16)
        total = dot(hi, same_head) + dot(lo, same_head)
        return v * lax.rsqrt(total / HD + epsilon) * gain_row

    for name in ("g1", "qg", "kg", "wk1", "wv1", "wq1"):
        loads[name].wait()
    qg_row = jnp.concatenate([qg_buf[...], qg_buf[...]], axis=1) * (HD ** -0.5 * LOG2E)
    kg_row = jnp.concatenate([kg_buf[...], kg_buf[...]], axis=1)
    x_copy.wait()
    y1, sq1 = scaled(1)
    row_scale = lax.rsqrt((sq0 + sq1) / width + epsilon)
    raw_kv = (raw_s[:, q_cols:] + dot(y1, w_buf[1, :, q_cols:])) * row_scale
    mine = pl.ds(1 + me * nb, nb)
    kv_all[0] = jnp.zeros((BLK, 2 * k_cols), BF16)
    key_part = head_norm(raw_kv[:, 0:k_cols], kg_row).astype(BF16)
    value_part = raw_kv[:, k_cols:].astype(BF16)
    kv_all[mine] = jnp.concatenate([key_part, value_part], axis=1).reshape(nb, BLK, 2 * k_cols)

    chunk_blocks = nb // CHUNKS
    sent = []

    def kv_copy(direction, owner, chunk):
        at = pl.ds(1 + owner * nb + chunk * chunk_blocks, chunk_blocks)
        return pltpu.make_async_remote_copy(
            kv_all.at[at], kv_all.at[at],
            send_sem.at[direction, chunk, owner], recv_sem.at[chunk, owner],
            device_id={"kv": neighbour[direction]}, device_id_type=MESH)

    def send(direction, owner, chunk, when):
        sent.append((direction, owner, chunk, when))

        @pl.when(when)
        def _():
            kv_copy(direction, owner, chunk).start()

    def arrive(owner, chunk, when):
        @pl.when(when)
        def _():
            kv_copy(UP, owner, chunk).wait_recv()

    last = n_z - 1
    reach_a, reach_b = n_z // 2, n_z // 2 - 1
    back_a, back_b = last - reach_a, last - reach_b
    for chunk in range(CHUNKS):
        send(RIGHT, me, chunk, (z < last) | (y < N_Y - 1))
        send(UP, me, chunk, z < last)
        send(DOWN, me, chunk, z < back_a)
        send(LEFT, me, chunk, y == 0)

    raw = (raw_s[:, 0:q_cols] + dot(y1, w_buf[1, :, 0:q_cols])) * row_scale
    low = iota((rows, LANES), 1) < HD
    for tile in range(q_cols // LANES):
        q = head_norm(raw[:, tile * LANES:(tile + 1) * LANES], qg_row)
        turned = pltpu.roll(q, HD, 1)
        for odd in range(2):
            head = 2 * tile + odd
            side = head // group
            here = q if odd == side else turned
            here = jnp.where(low if side == 0 else ~low, here, 0.0).astype(BF16)
            for r in range(nb):
                q_s[r, head * BLK:(head + 1) * BLK] = here[r * BLK:(r + 1) * BLK]

    loads["ch"].wait()
    loads["chs"].wait()
    lists = ch_buf[...]
    lane = iota((nb, keys), 1)
    block = jnp.full((nb, keys), -1, jnp.int32)
    for e in range(entries):
        block = jnp.where(lane // BLK == e, lists[:, e:e + 1], block)
    away = (block - (me * nb + iota((nb, keys), 0))) * BLK + lane % BLK
    kp_s[...] = jnp.where(block < 0, 1 << 24, away).astype(F32)

    left_col = lax.rem(y + N_Y - 1, N_Y)
    left_me = z * N_Y + left_col
    for chunk in range(CHUNKS):
        arrive(left_me, chunk, (z < last) | (y > 0))
        send(UP, left_me, chunk, z < last)
        send(DOWN, left_me, chunk, z < back_b)
        send(RIGHT, left_me, chunk, (y == 1) | (y == 2))

    for hop in range(1, n_z // 2 + 1):
        above = z - hop
        below = lax.rem(z + hop, n_z)
        for col, reach, back, side in ((y, reach_a, back_a, LEFT), (left_col, reach_b, back_b, RIGHT)):
            for chunk in range(CHUNKS):
                if hop <= reach:
                    owner = lax.max(above, 0) * N_Y + col
                    arrive(owner, chunk, above >= 0)
                    if hop < reach:
                        send(UP, owner, chunk, (above >= 0) & (z < last))
                    send(side, owner, chunk, above >= 0)
                if hop <= back:
                    owner = below * N_Y + col
                    valid = below < back
                    arrive(owner, chunk, valid)
                    if hop < back:
                        send(DOWN, owner, chunk, valid)
                    send(side, owner, chunk, valid & (below < z))

    right_col = lax.rem(y + 1, N_Y)
    far_col = lax.rem(y + 2, N_Y)
    for row in range(n_z):
        for chunk in range(CHUNKS):
            arrive(row * N_Y + right_col, chunk, (row < z) | ((row == z) & (y == N_Y - 1)))
            arrive(row * N_Y + far_col, chunk, (row < z) | ((row == z) & (y >= 2)))

    query_row = iota((BLK, keys), 0).astype(F32)
    ones = jnp.ones((keys, LANES), BF16)
    tile_low = iota((BLK, LANES), 1) < HD
    tile_lane = iota((BLK, LANES), 1)
    core_slope = jnp.where(tp == 0, 1.0, 2.0 ** (-8.0 * heads / n_heads)).astype(F32)

    def slope_of(head):
        return core_slope * (2.0 ** (-8.0 * (head + 1) / n_heads))

    def attend(r):
        key_rows, value_rows = [], []
        for e in range(entries):
            tile = kv_all[ch_s[r, e] + 1]
            key_rows.append(tile[:, 0:k_cols])
            value_rows.append(tile[:, k_cols:])
        key_rows = jnp.concatenate(key_rows, axis=0)
        value_rows = jnp.concatenate([jnp.concatenate(value_rows, axis=0), ones], axis=1)
        scores = dot_nt(q_s[r], key_rows)
        key_pos = kp_s[r:r + 1, :]
        allowed = key_pos <= query_row
        weights = []
        for head in range(heads):
            bias = key_pos * (slope_of(head) * (alibi * LOG2E))
            part = jnp.exp2(scores[head * BLK:(head + 1) * BLK] + bias)
            weights.append(jnp.where(allowed, part, 0.0).astype(BF16))
        found = dot(jnp.concatenate(weights, axis=0), value_rows)

        def of(head):
            return found[head * BLK:(head + 1) * BLK]

        sums = jnp.ones((BLK, LANES), F32)
        at = slice(r * BLK, (r + 1) * BLK)
        for t in range(group):
            first, second = of(t), of(t + group)
            top = jnp.where(tile_low, first[:, 0:LANES], second[:, 0:LANES])
            total = jnp.where(tile_low, first[:, LANES:], second[:, LANES:])
            att_s[at, t * LANES:(t + 1) * LANES] = (top / total).astype(BF16)
            sums = jnp.where(tile_lane == t, first[:, LANES:], sums)
            sums = jnp.where(tile_lane == t + group, second[:, LANES:], sums)
        sum_s[at] = sums

    for side in range(2):
        for head in range(heads):
            loads[f"wo{side}{head}"].wait()
    part_rows = rows // PARTS

    def part_copy(part):
        at = pl.ds(part * part_rows, part_rows)
        return pltpu.make_async_remote_copy(
            part_send.at[at], part_recv.at[at], part_sem.at[0, part], part_sem.at[1, part],
            device_id={"tp": partner}, device_id_type=MESH)

    for part in range(PARTS):
        at = slice(part * part_rows, (part + 1) * part_rows)
        for r in range(part * nb // PARTS, (part + 1) * nb // PARTS):
            attend(r)
        part_send[at] = dot(att_s[at], wo_buf[1]).astype(BF16)
        part_copy(part).start()

    own = dot(att_s[...], wo_buf[0])
    row_in = (iota((rows, LANES), 0) % BLK).astype(F32)
    slopes = jnp.exp2(-8.0 / n_heads * (tp * heads + iota((rows, LANES), 1) + 1).astype(F32))
    logs = jnp.log(sum_s[...]) - slopes * alibi * row_in
    lt_ref[...] = logs.T[0:heads]

    for direction, owner, chunk, when in sent:
        @pl.when(when)
        def _():
            kv_copy(direction, owner, chunk).wait_send()

    for part in range(PARTS):
        at = slice(part * part_rows, (part + 1) * part_rows)
        part_copy(part).wait()
        out_ref[at] = (own[at] + part_recv[at].astype(F32)).astype(BF16)


def write_out(mixed, log_total, mixed_out, log_out, sems):
    copies = [
        pltpu.make_async_copy(mixed, mixed_out, sems.at[0]),
        pltpu.make_async_copy(log_total, log_out, sems.at[1]),
    ]
    for copy in copies:
        copy.start()
    for copy in copies:
        copy.wait()


def shards(n_kv, tokens, norm_gain, w_query, w_key, w_value, q_gain, k_gain, w_out, chosen):
    seqs, rows, half = tokens.shape
    nb, entries = chosen.shape[1:]
    q_cols, k_cols = w_query.shape[1], w_key.shape[1]
    heads = q_cols // HD
    vmem = pltpu.VMEM
    dma = pltpu.SemaphoreType.DMA
    mixed, log_total = pl.pallas_call(
        functools.partial(kernel, n_kv),
        out_shape=(vmem((rows, half), BF16), vmem((heads, rows), F32)),
        in_specs=[pl.BlockSpec(memory_space=pltpu.HBM)] * 9,
        out_specs=(pl.BlockSpec(memory_space=vmem), pl.BlockSpec(memory_space=vmem)),
        scratch_shapes=[
            vmem((2, rows, half), BF16),
            pltpu.SMEM((nb, entries), jnp.int32),
            vmem((nb, entries), jnp.int32),
            vmem((rows, q_cols + 2 * k_cols), F32),
            vmem((2, half, q_cols + 2 * k_cols), BF16),
            vmem((2, q_cols, half), BF16),
            vmem((2, 1, half), F32),
            vmem((1, HD), F32),
            vmem((1, HD), F32),
            vmem((nb, heads * BLK, LANES), BF16),
            vmem((1 + n_kv * nb, BLK, 2 * k_cols), BF16),
            vmem((nb, entries * BLK), F32),
            vmem((rows, q_cols), BF16),
            vmem((rows, LANES), F32),
            vmem((rows, half), BF16),
            vmem((rows, half), BF16),
            dma((13 + 2 * heads,)),
            dma((2,)),
            dma((4, CHUNKS, n_kv)),
            dma((CHUNKS, n_kv)),
            dma((2, PARTS)),
        ],
        compiler_params=pltpu.CompilerParams(
            collective_id=0, has_side_effects=True, vmem_limit_bytes=66_700_000
        ),
    )(
        tokens.reshape(rows, half), norm_gain.reshape(1, -1), w_query, w_key, w_value,
        q_gain.reshape(1, -1), k_gain.reshape(1, -1), w_out, chosen.reshape(nb, entries),
    )
    mixed, log_total = pl.pallas_call(
        write_out,
        out_shape=(
            jax.ShapeDtypeStruct((rows, half), BF16),
            jax.ShapeDtypeStruct((heads, rows), F32),
        ),
        in_specs=[pl.BlockSpec(memory_space=pl.ANY)] * 2,
        out_specs=(pl.BlockSpec(memory_space=pltpu.HBM),) * 2,
        scratch_shapes=[dma((2,))],
        compiler_params=pltpu.CompilerParams(vmem_limit_bytes=1_000_000),
    )(mixed, log_total)
    return mixed.reshape(seqs, rows, half), log_total.reshape(seqs, heads, rows)


def solution(mesh):
    in_specs = (
        P("dp", "kv", "tp"),
        P(),
        P(None, "tp"),
        P(None, "tp"),
        P(None, "tp"),
        P(),
        P(),
        P("tp", None),
        P("dp", "kv", None),
    )
    out_specs = (P("dp", "kv", "tp"), P("dp", "tp", "kv"))
    return jax.shard_map(
        functools.partial(shards, mesh.shape["kv"]),
        mesh=mesh, in_specs=in_specs, out_specs=out_specs, check_vma=False)
```

```python
import functools
import math

import jax
import jax.numpy as jnp
from jax import lax
from jax.experimental import pallas as pl
from jax.experimental.pallas import tpu as pltpu
from jax.sharding import PartitionSpec as P

HD = 64
BLK = 32
LANES = 128
PARTS = 2
N_Y = 4
CHUNKS = 2
UP, DOWN, LEFT, RIGHT = range(4)

epsilon = 1e-06
alibi_reach = 4.0
LOG2E = math.log2(math.e)
F32 = jnp.float32
BF16 = jnp.bfloat16
NT = (((1,), (1,)), ((), ()))
MESH = pl.DeviceIdType.MESH


def iota(shape, dim):
    return lax.broadcasted_iota(jnp.int32, shape, dim)


def dot(a, b):
    return jnp.dot(a, b, preferred_element_type=F32)


def dot_nt(a, b):
    return lax.dot_general(a, b, NT, preferred_element_type=F32)


def kernel(
    n_kv,
    tok, gain, wq, wk, wv, qg, kg, wo, ch,
    out_ref, lt_ref,
    x_buf, ch_s, ch_buf, raw_s, w_buf, wo_buf, g_buf, hg_buf,
    q_s, kv_all, kp_s, att_s, sum_s, part_send, part_recv,
    load_sem, x_sem, send_sem, stage_sem, end_sem, part_sem,
):
    me = lax.axis_index("kv")
    tp = lax.axis_index("tp")
    partner = 1 - tp
    n_z = n_kv // N_Y
    z = me // N_Y
    y = me % N_Y
    rows, half = tok.shape
    q_cols = wq.shape[1]
    k_cols = wk.shape[1]
    heads = q_cols // HD
    kv_heads = k_cols // HD
    group = heads // kv_heads
    n_heads = heads * lax.axis_size("tp")
    nb, entries = ch.shape
    width = half * 2
    seq_len = rows * n_kv
    alibi = alibi_reach / seq_len
    keys = entries * BLK

    def span(start):
        return pl.ds(pl.multiple_of(start * half, LANES), half)

    def load(sem, *pairs):
        for src, dst in pairs:
            pltpu.make_async_copy(src, dst, load_sem.at[sem]).start()

    def loaded(sem, whole):
        pltpu.make_async_copy(whole, whole, load_sem.at[sem]).wait()

    def weights(side, which):
        return (
            (wk.at[span(which), :], w_buf.at[side, :, q_cols:q_cols + k_cols]),
            (wv.at[span(which), :], w_buf.at[side, :, q_cols + k_cols:q_cols + 2 * k_cols]),
            (wq.at[span(which), :], w_buf.at[side, :, 0:q_cols]),
        )

    TOK, GAIN, W0, W1, HEAD_GAIN, LIST, TABLE, OUT = range(8)
    load(TOK, (tok, x_buf.at[0]))
    load(GAIN, (gain.at[:, span(tp)], g_buf.at[0]), (gain.at[:, span(partner)], g_buf.at[1]))
    load(W0, *weights(0, tp))
    load(W1, *weights(1, partner))
    load(HEAD_GAIN, (qg, hg_buf.at[0]), (kg, hg_buf.at[1]))
    load(LIST, (ch, ch_s))
    load(TABLE, (ch, ch_buf))
    for side, which in ((0, tp), (1, partner)):
        for head in range(heads):
            to = head % group * LANES + head // group * HD
            load(OUT, (wo.at[head * HD:(head + 1) * HD, span(which)], wo_buf.at[side, to:to + HD]))

    def device(row, col):
        return lax.rem(row + n_z, n_z) * N_Y + lax.rem(col + N_Y, N_Y)

    neighbour = {
        UP: device(z + 1, y), DOWN: device(z - 1, y),
        LEFT: device(z, y - 1), RIGHT: device(z, y + 1),
    }
    barrier = pltpu.get_barrier_semaphore()
    pl.semaphore_signal(barrier, inc=1, device_id={"tp": partner}, device_id_type=MESH)
    for target in neighbour.values():
        pl.semaphore_signal(barrier, inc=1, device_id={"kv": target}, device_id_type=MESH)

    def scaled(side):
        x = x_buf[side].astype(F32)
        return (x * g_buf[side]).astype(BF16), jnp.sum(x * x, axis=1, keepdims=True)

    loaded(TOK, x_buf.at[0])
    pl.semaphore_wait(barrier, 5)
    x_copy = pltpu.make_async_remote_copy(
        x_buf.at[0], x_buf.at[1], x_sem.at[0], x_sem.at[1],
        device_id={"tp": partner}, device_id_type=MESH)
    x_copy.start()

    loaded(GAIN, g_buf)
    loaded(W0, w_buf.at[0])
    y0, sq0 = scaled(0)
    raw_s[...] = dot(y0, w_buf[0])

    same_head = jnp.where(
        iota((LANES, LANES), 0) // HD == iota((LANES, LANES), 1) // HD, 1.0, 0.0).astype(BF16)

    def head_norm(v, gain_row):
        sq = v * v
        hi = sq.astype(BF16)
        lo = (sq - hi.astype(F32)).astype(BF16)
        total = dot(hi, same_head) + dot(lo, same_head)
        return v * lax.rsqrt(total / HD + epsilon) * gain_row

    loaded(HEAD_GAIN, hg_buf)
    loaded(W1, w_buf.at[1])
    qg_row = jnp.concatenate([hg_buf[0], hg_buf[0]], axis=1) * (HD ** -0.5 * LOG2E)
    kg_row = jnp.concatenate([hg_buf[1], hg_buf[1]], axis=1)
    x_copy.wait()
    y1, sq1 = scaled(1)
    row_scale = lax.rsqrt((sq0 + sq1) / width + epsilon)
    raw_kv = (raw_s[:, q_cols:] + dot(y1, w_buf[1, :, q_cols:])) * row_scale
    mine = pl.ds(1 + me * nb, nb)
    kv_all[0] = jnp.zeros((BLK, 2 * k_cols), BF16)
    key_part = head_norm(raw_kv[:, 0:k_cols], kg_row).astype(BF16)
    value_part = raw_kv[:, k_cols:].astype(BF16)
    kv_all[mine] = jnp.concatenate([key_part, value_part], axis=1).reshape(nb, BLK, 2 * k_cols)

    chunk_blocks = nb // CHUNKS
    sent = {UP: 0, DOWN: 0, LEFT: 0, RIGHT: 0}
    most_sent = {UP: 0, DOWN: 0, LEFT: 0, RIGHT: 0}

    def kv_copy(direction, row, col, chunk, arrival):
        at = pl.ds(1 + (row * N_Y + col) * nb + chunk * chunk_blocks, chunk_blocks)
        return pltpu.make_async_remote_copy(
            kv_all.at[at], kv_all.at[at], send_sem.at[direction], arrival,
            device_id={"kv": neighbour[direction]}, device_id_type=MESH)

    def stage(kind, row, chunk):
        return stage_sem.at[kind, row, chunk]

    def send(direction, row, col, chunk, when, arrival):
        if chunk == 0:
            sent[direction] += jnp.where(when, 1, 0)
            most_sent[direction] += 1

        @pl.when(when)
        def _():
            kv_copy(direction, row, col, chunk, arrival).start()

    def arrive(kind, row, col, chunk, when):
        @pl.when(when)
        def _():
            kv_copy(UP, row, col, chunk, stage(kind, row, chunk)).wait_recv()

    def settle(count, most, sem):
        for k in range(1, most + 1):
            @pl.when(count == k)
            def _():
                whole = kv_all.at[0:k * nb]
                pltpu.make_async_copy(whole, whole, sem).wait()

    last = n_z - 1
    reach_a, reach_b = n_z // 2, n_z // 2 - 1
    back_a, back_b = last - reach_a, last - reach_b
    for chunk in range(CHUNKS):
        send(RIGHT, z, y, chunk, (z < last) | (y < N_Y - 1), stage(1, z, chunk))
        send(UP, z, y, chunk, z < last, stage(0, z, chunk))
        send(DOWN, z, y, chunk, z < back_a, stage(0, z, chunk))
        send(LEFT, z, y, chunk, y == 0, end_sem.at[0])

    raw = (raw_s[:, 0:q_cols] + dot(y1, w_buf[1, :, 0:q_cols])) * row_scale
    low = iota((rows, LANES), 1) < HD
    for tile in range(q_cols // LANES):
        q = head_norm(raw[:, tile * LANES:(tile + 1) * LANES], qg_row)
        turned = pltpu.roll(q, HD, 1)
        for odd in range(2):
            head = 2 * tile + odd
            side = head // group
            here = q if odd == side else turned
            here = jnp.where(low if side == 0 else ~low, here, 0.0).astype(BF16)
            for r in range(nb):
                q_s[r, head * BLK:(head + 1) * BLK] = here[r * BLK:(r + 1) * BLK]

    loaded(TABLE, ch_buf)
    loaded(LIST, ch_s)
    lists = ch_buf[...]
    lane = iota((nb, keys), 1)
    block = jnp.full((nb, keys), -1, jnp.int32)
    for e in range(entries):
        block = jnp.where(lane // BLK == e, lists[:, e:e + 1], block)
    away = (block - (me * nb + iota((nb, keys), 0))) * BLK + lane % BLK
    kp_s[...] = jnp.where(block < 0, 1 << 24, away).astype(F32)

    left_col = lax.rem(y + N_Y - 1, N_Y)
    for chunk in range(CHUNKS):
        arrive(1, z, left_col, chunk, (z < last) | (y > 0))
        send(UP, z, left_col, chunk, z < last, stage(1, z, chunk))
        send(DOWN, z, left_col, chunk, z < back_b, stage(1, z, chunk))
        send(RIGHT, z, left_col, chunk, (y == 1) | (y == 2), end_sem.at[1])

    routes = (
        (0, y, reach_a, back_a, LEFT, end_sem.at[0]),
        (1, left_col, reach_b, back_b, RIGHT, end_sem.at[1]),
    )
    for hop in range(1, n_z // 2 + 1):
        above = lax.max(z - hop, 0)
        below = lax.rem(z + hop, n_z)
        for kind, col, reach, back, side, end in routes:
            for chunk in range(CHUNKS):
                if hop <= reach:
                    valid = z >= hop
                    arrive(kind, above, col, chunk, valid)
                    if hop < reach:
                        send(UP, above, col, chunk, valid & (z < last), stage(kind, above, chunk))
                    send(side, above, col, chunk, valid, end)
                if hop <= back:
                    valid = below < back
                    arrive(kind, below, col, chunk, valid)
                    if hop < back:
                        send(DOWN, below, col, chunk, valid, stage(kind, below, chunk))
                    send(side, below, col, chunk, valid & (below < z), end)

    settle(z + jnp.where(y == N_Y - 1, 1, 0), n_z, end_sem.at[0])
    settle(z + jnp.where(y >= 2, 1, 0), n_z, end_sem.at[1])

    query_row = iota((BLK, keys), 0).astype(F32)
    ones = jnp.ones((keys, LANES), BF16)
    tile_low = iota((BLK, LANES), 1) < HD
    tile_lane = iota((BLK, LANES), 1)
    core_slope = jnp.where(tp == 0, 1.0, 2.0 ** (-8.0 * heads / n_heads)).astype(F32)

    def slope_of(head):
        return core_slope * (2.0 ** (-8.0 * (head + 1) / n_heads))

    def attend(r):
        key_rows, value_rows = [], []
        for e in range(entries):
            tile = kv_all[ch_s[r, e] + 1]
            key_rows.append(tile[:, 0:k_cols])
            value_rows.append(tile[:, k_cols:])
        key_rows = jnp.concatenate(key_rows, axis=0)
        value_rows = jnp.concatenate([jnp.concatenate(value_rows, axis=0), ones], axis=1)
        scores = dot_nt(q_s[r], key_rows)
        key_pos = kp_s[r:r + 1, :]
        allowed = key_pos <= query_row
        weights = []
        for head in range(heads):
            bias = key_pos * (slope_of(head) * (alibi * LOG2E))
            part = jnp.exp2(scores[head * BLK:(head + 1) * BLK] + bias)
            weights.append(jnp.where(allowed, part, 0.0).astype(BF16))
        found = dot(jnp.concatenate(weights, axis=0), value_rows)

        def of(head):
            return found[head * BLK:(head + 1) * BLK]

        sums = jnp.ones((BLK, LANES), F32)
        at = slice(r * BLK, (r + 1) * BLK)
        for t in range(group):
            first, second = of(t), of(t + group)
            top = jnp.where(tile_low, first[:, 0:LANES], second[:, 0:LANES])
            total = jnp.where(tile_low, first[:, LANES:], second[:, LANES:])
            att_s[at, t * LANES:(t + 1) * LANES] = (top / total).astype(BF16)
            sums = jnp.where(tile_lane == t, first[:, LANES:], sums)
            sums = jnp.where(tile_lane == t + group, second[:, LANES:], sums)
        sum_s[at] = sums

    loaded(OUT, wo_buf)
    part_rows = rows // PARTS

    def part_copy(part):
        at = pl.ds(part * part_rows, part_rows)
        return pltpu.make_async_remote_copy(
            part_send.at[at], part_recv.at[at], part_sem.at[0, part], part_sem.at[1, part],
            device_id={"tp": partner}, device_id_type=MESH)

    for part in range(PARTS):
        at = slice(part * part_rows, (part + 1) * part_rows)
        for r in range(part * nb // PARTS, (part + 1) * nb // PARTS):
            attend(r)
        part_send[at] = dot(att_s[at], wo_buf[1]).astype(BF16)
        part_copy(part).start()

    own = dot(att_s[...], wo_buf[0])
    row_in = (iota((rows, LANES), 0) % BLK).astype(F32)
    slopes = jnp.exp2(-8.0 / n_heads * (tp * heads + iota((rows, LANES), 1) + 1).astype(F32))
    logs = jnp.log(sum_s[...]) - slopes * alibi * row_in
    lt_ref[...] = logs.T[0:heads]

    for direction in sent:
        settle(sent[direction], most_sent[direction], send_sem.at[direction])

    for part in range(PARTS):
        at = slice(part * part_rows, (part + 1) * part_rows)
        part_copy(part).wait()
        out_ref[at] = (own[at] + part_recv[at].astype(F32)).astype(BF16)


def write_out(mixed, log_total, mixed_out, log_out, sems):
    copies = [
        pltpu.make_async_copy(mixed, mixed_out, sems.at[0]),
        pltpu.make_async_copy(log_total, log_out, sems.at[1]),
    ]
    for copy in copies:
        copy.start()
    for copy in copies:
        copy.wait()


def shards(n_kv, tokens, norm_gain, w_query, w_key, w_value, q_gain, k_gain, w_out, chosen):
    seqs, rows, half = tokens.shape
    nb, entries = chosen.shape[1:]
    q_cols, k_cols = w_query.shape[1], w_key.shape[1]
    heads = q_cols // HD
    vmem = pltpu.VMEM
    dma = pltpu.SemaphoreType.DMA
    mixed, log_total = pl.pallas_call(
        functools.partial(kernel, n_kv),
        out_shape=(vmem((rows, half), BF16), vmem((heads, rows), F32)),
        in_specs=[pl.BlockSpec(memory_space=pltpu.HBM)] * 9,
        out_specs=(pl.BlockSpec(memory_space=vmem), pl.BlockSpec(memory_space=vmem)),
        scratch_shapes=[
            vmem((2, rows, half), BF16),
            pltpu.SMEM((nb, entries), jnp.int32),
            vmem((nb, entries), jnp.int32),
            vmem((rows, q_cols + 2 * k_cols), F32),
            vmem((2, half, q_cols + 2 * k_cols), BF16),
            vmem((2, q_cols, half), BF16),
            vmem((2, 1, half), F32),
            vmem((2, 1, HD), F32),
            vmem((nb, heads * BLK, LANES), BF16),
            vmem((1 + n_kv * nb, BLK, 2 * k_cols), BF16),
            vmem((nb, entries * BLK), F32),
            vmem((rows, q_cols), BF16),
            vmem((rows, LANES), F32),
            vmem((rows, half), BF16),
            vmem((rows, half), BF16),
            dma((8,)),
            dma((2,)),
            dma((4,)),
            dma((2, n_kv // N_Y, CHUNKS)),
            dma((2,)),
            dma((2, PARTS)),
        ],
        compiler_params=pltpu.CompilerParams(
            collective_id=0, has_side_effects=True, vmem_limit_bytes=66_700_000
        ),
    )(
        tokens.reshape(rows, half), norm_gain.reshape(1, -1), w_query, w_key, w_value,
        q_gain.reshape(1, -1), k_gain.reshape(1, -1), w_out, chosen.reshape(nb, entries),
    )
    mixed, log_total = pl.pallas_call(
        write_out,
        out_shape=(
            jax.ShapeDtypeStruct((rows, half), BF16),
            jax.ShapeDtypeStruct((heads, rows), F32),
        ),
        in_specs=[pl.BlockSpec(memory_space=pl.ANY)] * 2,
        out_specs=(pl.BlockSpec(memory_space=pltpu.HBM),) * 2,
        scratch_shapes=[dma((2,))],
        compiler_params=pltpu.CompilerParams(vmem_limit_bytes=1_000_000),
    )(mixed, log_total)
    return mixed.reshape(seqs, rows, half), log_total.reshape(seqs, heads, rows)


def solution(mesh):
    in_specs = (
        P("dp", "kv", "tp"),
        P(),
        P(None, "tp"),
        P(None, "tp"),
        P(None, "tp"),
        P(),
        P(),
        P("tp", None),
        P("dp", "kv", None),
    )
    out_specs = (P("dp", "kv", "tp"), P("dp", "tp", "kv"))
    return jax.shard_map(
        functools.partial(shards, mesh.shape["kv"]),
        mesh=mesh, in_specs=in_specs, out_specs=out_specs, check_vma=False)
```

```python
import functools
import math

import jax
import jax.numpy as jnp
from jax import lax
from jax.experimental import pallas as pl
from jax.experimental.pallas import tpu as pltpu
from jax.sharding import PartitionSpec as P

HD = 64
BLK = 32
LANES = 128
MOST = 4
PARTS = 2
N_Y = 4
UP, DOWN, LEFT, RIGHT, FAR = range(5)

epsilon = 1e-06
alibi_reach = 4.0
LOG2E = math.log2(math.e)
F32 = jnp.float32
BF16 = jnp.bfloat16
NT = (((1,), (1,)), ((), ()))
MESH = pl.DeviceIdType.MESH


def iota(shape, dim):
    return lax.broadcasted_iota(jnp.int32, shape, dim)


def dot(a, b):
    return jnp.dot(a, b, preferred_element_type=F32)


def dot_nt(a, b):
    return lax.dot_general(a, b, NT, preferred_element_type=F32)


def kernel(
    n_kv,
    tok, gain, wq, wk, wv, qg, kg, wo, ch,
    out_ref, lt_ref,
    x_buf, ch_buf, raw_s, w_buf, wo_buf, g_buf, hg_buf,
    place_send, place_recv, code_s, index_v, index_s, left_s, right_s, far_s,
    q_s, kv, kp_s, att_s, sum_s, part_send, part_recv,
    load_sem, x_sem, place_sem, send_sem, stage_sem, end_sem, part_sem,
):
    me = lax.axis_index("kv")
    tp = lax.axis_index("tp")
    partner = 1 - tp
    n_z = n_kv // N_Y
    z = me // N_Y
    y = me % N_Y
    rows, half = tok.shape
    q_cols = wq.shape[1]
    k_cols = wk.shape[1]
    heads = q_cols // HD
    kv_heads = k_cols // HD
    group = heads // kv_heads
    n_heads = heads * lax.axis_size("tp")
    nb, entries = ch.shape
    n_blocks = n_kv * nb
    width = half * 2
    seq_len = rows * n_kv
    alibi = alibi_reach / seq_len
    keys = entries * BLK
    picked = MOST * BLK

    def span(start):
        return pl.ds(pl.multiple_of(start * half, LANES), half)

    def load(sem, *pairs):
        for src, dst in pairs:
            pltpu.make_async_copy(src, dst, load_sem.at[sem]).start()

    def loaded(sem, whole):
        pltpu.make_async_copy(whole, whole, load_sem.at[sem]).wait()

    def weights(side, which):
        return (
            (wk.at[span(which), :], w_buf.at[side, :, q_cols:q_cols + k_cols]),
            (wv.at[span(which), :], w_buf.at[side, :, q_cols + k_cols:q_cols + 2 * k_cols]),
            (wq.at[span(which), :], w_buf.at[side, :, 0:q_cols]),
        )

    TABLE, TOK, GAIN, W0, W1, HEAD_GAIN, OUT, INDEX = range(8)
    load(TABLE, (ch, ch_buf))
    load(TOK, (tok, x_buf.at[0]))
    load(GAIN, (gain.at[:, span(tp)], g_buf.at[0]), (gain.at[:, span(partner)], g_buf.at[1]))
    load(W0, *weights(0, tp))
    load(W1, *weights(1, partner))
    load(HEAD_GAIN, (qg, hg_buf.at[0]), (kg, hg_buf.at[1]))
    for side, which in ((0, tp), (1, partner)):
        for head in range(heads):
            to = head % group * LANES + head // group * HD
            load(OUT, (wo.at[head * HD:(head + 1) * HD, span(which)], wo_buf.at[side, to:to + HD]))

    def device(row, col):
        return lax.rem(row + n_z, n_z) * N_Y + lax.rem(col + N_Y, N_Y)

    neighbour = {
        UP: device(z + 1, y), DOWN: device(z - 1, y),
        LEFT: device(z, y - 1), RIGHT: device(z, y + 1), FAR: device(z, y + 2),
    }
    barrier = pltpu.get_barrier_semaphore()
    pl.semaphore_signal(barrier, inc=1, device_id={"tp": partner}, device_id_type=MESH)
    for target in neighbour.values():
        pl.semaphore_signal(barrier, inc=1, device_id={"kv": target}, device_id_type=MESH)

    loaded(TABLE, ch_buf)
    lists = ch_buf[...]
    lane_block = iota((nb, n_blocks), 1)
    hits = [lists[:, e:e + 1] == lane_block for e in range(entries)]
    hit = hits[0]
    for e in range(1, entries):
        hit = hit | hits[e]
    need = jnp.broadcast_to(jnp.max(jnp.where(hit, 1, 0), axis=0, keepdims=True), (nb, n_blocks))
    rank_of = jnp.zeros((nb, n_blocks), jnp.int32)
    for k in range(1, nb):
        rank_of = rank_of + jnp.where(lane_block % nb >= k, pltpu.roll(need, k, 1), 0)
    place_send[...] = jnp.where(need > 0, rank_of, -1).astype(F32)

    def scaled(side):
        x = x_buf[side].astype(F32)
        return (x * g_buf[side]).astype(BF16), jnp.sum(x * x, axis=1, keepdims=True)

    loaded(TOK, x_buf.at[0])
    pl.semaphore_wait(barrier, 1 + len(neighbour))
    x_copy = pltpu.make_async_remote_copy(
        x_buf.at[0], x_buf.at[1], x_sem.at[0], x_sem.at[1],
        device_id={"tp": partner}, device_id_type=MESH)
    x_copy.start()

    def place_copy(direction, slot):
        return pltpu.make_async_remote_copy(
            place_send, place_recv.at[slot], place_sem.at[0, slot], place_sem.at[1, slot],
            device_id={"kv": neighbour[direction]}, device_id_type=MESH)

    place_copies = [place_copy(RIGHT, 0), place_copy(LEFT, 1), place_copy(FAR, 2)]
    for copy in place_copies:
        copy.start()

    loaded(GAIN, g_buf)
    loaded(W0, w_buf.at[0])
    y0, sq0 = scaled(0)
    raw_s[...] = dot(y0, w_buf[0])

    same_head = jnp.where(
        iota((LANES, LANES), 0) // HD == iota((LANES, LANES), 1) // HD, 1.0, 0.0).astype(BF16)

    def head_norm(v, gain_row):
        sq = v * v
        hi = sq.astype(BF16)
        lo = (sq - hi.astype(F32)).astype(BF16)
        total = dot(hi, same_head) + dot(lo, same_head)
        return v * lax.rsqrt(total / HD + epsilon) * gain_row

    loaded(HEAD_GAIN, hg_buf)
    loaded(W1, w_buf.at[1])
    qg_row = jnp.concatenate([hg_buf[0], hg_buf[0]], axis=1) * (HD ** -0.5 * LOG2E)
    kg_row = jnp.concatenate([hg_buf[1], hg_buf[1]], axis=1)
    low = iota((rows, LANES), 1) < HD
    x_copy.wait()
    y1, sq1 = scaled(1)
    row_scale = lax.rsqrt((sq0 + sq1) / width + epsilon)
    raw_kv = (raw_s[:, q_cols:] + dot(y1, w_buf[1, :, q_cols:])) * row_scale
    key_part = pltpu.roll(head_norm(raw_kv[:, 0:k_cols], kg_row), HD, 1)
    value_part = raw_kv[:, k_cols:]

    def base(row, col):
        return 1 + (row * N_Y + col) * nb

    own_tiles = (jnp.where(low, value_part, key_part), jnp.where(low, key_part, value_part))
    for tile in range(2):
        kv[tile, 0] = jnp.zeros((BLK, LANES), BF16)
        kv[tile, pl.ds(base(z, y), nb)] = own_tiles[tile].astype(BF16).reshape(nb, BLK, LANES)

    last = n_z - 1
    reach_a, reach_b = n_z // 2, n_z // 2 - 1
    back_a, back_b = last - reach_a, last - reach_b
    sent = []

    def send(direction, src, dst, units, arrival, when, hop=None):
        sent.append((units, when, hop is not None))

        @pl.when(when(z, y, hop))
        def _():
            pltpu.make_async_remote_copy(
                src, dst, send_sem.at[0], arrival,
                device_id={"kv": neighbour[direction]}, device_id_type=MESH).start()

    def stage(kind, row):
        return stage_sem.at[kind, row]

    def tile_of(kind):
        return kind % 2

    def whole(kind, row, col):
        return kv.at[tile_of(kind), pl.ds(base(row, col), nb)]

    def send_whole(direction, kind, row, col, when, hop=None):
        part = whole(kind, row, col)
        send(direction, part, part, 2, stage(kind, row), when, hop)

    def arrive(kind, row, col, when, hop=None):
        @pl.when(when(z, y, hop))
        def _():
            part = whole(kind, row, col)
            pltpu.make_async_remote_copy(
                part, part, send_sem.at[0], stage(kind, row),
                device_id={"kv": neighbour[UP]}, device_id_type=MESH).wait_recv()

    same_row = iota((picked, rows), 0) % BLK == iota((picked, rows), 1) % BLK
    row_slot = (iota((picked, rows), 0) // BLK).astype(F32)

    def chooser(which, row):
        code = code_s[which, pl.ds(row, 1), :]
        return jnp.where(same_row & (code == row_slot), 1.0, 0.0).astype(BF16)

    def item(kind, row, col):
        return kv[tile_of(kind), pl.ds(base(row, col), nb)].reshape(rows, LANES)

    def blocks(x):
        return x.astype(BF16).reshape(-1, BLK, LANES)

    def choose_a(row, to_left, to_right, to_far, hop=None):
        @pl.when(to_left(z, y, hop) | to_right(z, y, hop) | to_far(z, y, hop))
        def _():
            left, right, far = (chooser(i, row) for i in range(3))
            left_s[row, 0] = blocks(dot(left, item(0, row, y)))
            found = blocks(dot(jnp.concatenate([left, right, far], axis=0), item(1, row, y)))
            left_s[row, 1] = found[0:MOST]
            right_s[row, 0] = found[MOST:2 * MOST]
            far_s[row] = found[2 * MOST:]

        at = pl.ds(base(row, y), MOST)
        send(LEFT, left_s.at[row], kv.at[:, at], 2, end_sem.at[0], to_left, hop)
        send(RIGHT, right_s.at[row, 0], kv.at[1, at], 1, end_sem.at[0], to_right, hop)
        send(FAR, far_s.at[row], kv.at[1, at], 1, end_sem.at[0], to_far, hop)

    def choose_b(row, to_right, hop=None):
        @pl.when(to_right(z, y, hop))
        def _():
            right_s[row, 1] = blocks(dot(chooser(3, row), item(2, row, left_col)))

        at = pl.ds(base(row, left_col), MOST)
        send(RIGHT, right_s.at[row, 1], kv.at[0, at], 1, end_sem.at[0], to_right, hop)

    left_col = lax.rem(y + N_Y - 1, N_Y)
    send_whole(UP, 0, z, y, lambda z, y, hop: z < last)
    send_whole(DOWN, 0, z, y, lambda z, y, hop: z < back_a)
    send(RIGHT, whole(0, z, y), whole(0, z, y), 2, stage(2, z), lambda z, y, hop: (z < last) | (y < N_Y - 1))
    send_whole(UP, 1, z, y, lambda z, y, hop: z < last)
    send_whole(DOWN, 1, z, y, lambda z, y, hop: z < back_a)

    raw = (raw_s[:, 0:q_cols] + dot(y1, w_buf[1, :, 0:q_cols])) * row_scale
    for tile in range(q_cols // LANES):
        q = head_norm(raw[:, tile * LANES:(tile + 1) * LANES], qg_row)
        turned = pltpu.roll(q, HD, 1)
        for odd in range(2):
            head = 2 * tile + odd
            side = head // group
            here = turned if odd == side else q
            here = jnp.where(low if side == 1 else ~low, here, 0.0).astype(BF16)
            for r in range(nb):
                q_s[r, head * BLK:(head + 1) * BLK] = here[r * BLK:(r + 1) * BLK]

    arrive(2, z, left_col, lambda z, y, hop: (z < last) | (y > 0))
    send_whole(UP, 2, z, left_col, lambda z, y, hop: z < last)
    send_whole(DOWN, 2, z, left_col, lambda z, y, hop: z < back_b)

    for copy in place_copies:
        copy.wait()
    spread = jnp.where(
        iota((n_blocks, rows), 0) % nb == iota((n_blocks, rows), 1) // BLK, 1.0, 0.0).astype(BF16)
    row_owner = iota((n_z, n_blocks), 0) * N_Y
    owner_lane = iota((n_z, n_blocks), 1) // nb
    for which, (slot, col) in enumerate(((0, y), (1, y), (2, y), (1, left_col))):
        mine = jnp.where(owner_lane == row_owner + col, place_recv[slot], 0.0)
        code_s[which] = dot(mine.astype(BF16), spread)

    lane_entry = iota((nb, entries), 1)
    rank = jnp.zeros((nb, entries), jnp.int32)
    for e in range(entries):
        found = jnp.max(jnp.where(hits[e], rank_of, 0), axis=1, keepdims=True)
        rank = jnp.where(lane_entry == e, found, rank)
    owner = lists // nb
    col = lax.rem(owner, N_Y)
    ranked = 1 + owner * nb + rank
    for tile in range(2):
        full = col == y
        if tile == 0:
            full = full | (col == left_col)
        index_v[tile] = jnp.where(lists < 0, 0, jnp.where(full, 1 + lists, ranked))
    index_copy = pltpu.make_async_copy(index_v, index_s, load_sem.at[INDEX])
    index_copy.start()

    lane = iota((nb, keys), 1)
    block = jnp.full((nb, keys), -1, jnp.int32)
    for e in range(entries):
        block = jnp.where(lane // BLK == e, lists[:, e:e + 1], block)
    away = (block - (me * nb + iota((nb, keys), 0))) * BLK + lane % BLK
    kp_s[...] = jnp.where(block < 0, 1 << 24, away).astype(F32)

    choose_a(z, lambda z, y, hop: y == 0, lambda z, y, hop: y < N_Y - 1, lambda z, y, hop: y < N_Y - 2)
    choose_b(z, lambda z, y, hop: (y == 1) | (y == 2))

    routes = (((0, 1), y, reach_a, back_a), ((2,), left_col, reach_b, back_b))
    hops = range(1, n_z // 2 + 1)

    def one_hop(hop, carry):
        above = lax.max(z - hop, 0)
        below = lax.rem(z + hop, n_z)
        for kinds, col, reach, back in routes:

            def from_above(z, y, hop, reach=reach):
                return (z >= hop) & (hop <= reach)

            def go_up(z, y, hop, reach=reach):
                return (z >= hop) & (hop < reach) & (z < last)

            def from_below(z, y, hop, back=back):
                return ((z + hop) % n_z < back) & (hop <= back)

            def go_down(z, y, hop, back=back):
                return ((z + hop) % n_z < back) & (hop < back)

            def use_below(z, y, hop, back=back):
                return ((z + hop) % n_z < back) & (hop <= back) & ((z + hop) % n_z < z)

            for kind in kinds:
                arrive(kind, above, col, from_above, hop)
                send_whole(UP, kind, above, col, go_up, hop)
                arrive(kind, below, col, from_below, hop)
                send_whole(DOWN, kind, below, col, go_down, hop)
            for row, use in ((above, from_above), (below, use_below)):
                if len(kinds) == 2:
                    choose_a(row, use, use, use, hop)
                else:
                    choose_b(row, use, hop)
        return carry

    lax.fori_loop(hops.start, hops.stop, one_hop, 0)

    def settle(count, sem):
        for k in range(n_z):
            @pl.when(z == k)
            def _():
                for j in range(N_Y):
                    units = count(k, j)
                    if units:
                        @pl.when(y == j)
                        def _():
                            part = kv.at[:, 0:units * MOST // 2]
                            pltpu.make_async_copy(part, part, sem).wait()

    settle(lambda z, y: 2 * (z + (y == N_Y - 1)) + (z + (y >= 1)) + 2 * (z + (y >= 2)), end_sem.at[0])
    index_copy.wait()

    query_row = iota((BLK, keys), 0).astype(F32)
    ones = jnp.ones((keys, LANES), BF16)
    tile_low = iota((BLK, LANES), 1) < HD
    tile_lane = iota((BLK, LANES), 1)
    core_slope = jnp.where(tp == 0, 1.0, 2.0 ** (-8.0 * heads / n_heads)).astype(F32)

    def slope_of(head):
        return core_slope * (2.0 ** (-8.0 * (head + 1) / n_heads))

    def attend(r):
        key_pos = kp_s[pl.ds(r, 1), :]
        allowed = key_pos <= query_row
        outs = []
        for side in range(kv_heads):
            both = jnp.concatenate([kv[side, index_s[side, r, e]] for e in range(entries)], axis=0)
            scores = dot_nt(q_s[r, side * group * BLK:(side + 1) * group * BLK], both)
            weights = []
            for t in range(group):
                bias = key_pos * (slope_of(side * group + t) * (alibi * LOG2E))
                part = jnp.exp2(scores[t * BLK:(t + 1) * BLK] + bias)
                weights.append(jnp.where(allowed, part, 0.0).astype(BF16))
            outs.append(dot(jnp.concatenate(weights, axis=0), jnp.concatenate([both, ones], axis=1)))

        sums = jnp.ones((BLK, LANES), F32)
        at = pl.ds(pl.multiple_of(r * BLK, BLK), BLK)
        for t in range(group):
            first, second = (o[t * BLK:(t + 1) * BLK] for o in outs)
            top = jnp.where(tile_low, first[:, 0:LANES], second[:, 0:LANES])
            total = jnp.where(tile_low, first[:, LANES:], second[:, LANES:])
            att_s[at, t * LANES:(t + 1) * LANES] = (top / total).astype(BF16)
            sums = jnp.where(tile_lane == t, first[:, LANES:], sums)
            sums = jnp.where(tile_lane == t + group, second[:, LANES:], sums)
        sum_s[at] = sums

    loaded(OUT, wo_buf)
    part_rows = rows // PARTS

    def part_at(part):
        return pl.ds(pl.multiple_of(part * part_rows, part_rows), part_rows)

    def part_copy(part):
        at = part_at(part)
        return pltpu.make_async_remote_copy(
            part_send.at[at], part_recv.at[at], part_sem.at[0, part], part_sem.at[1, part],
            device_id={"tp": partner}, device_id_type=MESH)

    def one_part(part, carry):
        for r in range(nb // PARTS):
            attend(part * (nb // PARTS) + r)
        at = part_at(part)
        part_send[at] = dot(att_s[at], wo_buf[1]).astype(BF16)
        part_copy(part).start()
        return carry

    lax.fori_loop(0, PARTS, one_part, 0)

    own = dot(att_s[...], wo_buf[0])
    row_in = (iota((rows, LANES), 0) % BLK).astype(F32)
    slopes = jnp.exp2(-8.0 / n_heads * (tp * heads + iota((rows, LANES), 1) + 1).astype(F32))
    logs = jnp.log(sum_s[...]) - slopes * alibi * row_in
    lt_ref[...] = logs.T[0:heads]

    def all_sent(z, y):
        return sum(
            units for units, when, looped in sent
            for hop in (hops if looped else (0,)) if when(z, y, hop))

    settle(all_sent, send_sem.at[0])

    for part in range(PARTS):
        at = slice(part * part_rows, (part + 1) * part_rows)
        part_copy(part).wait()
        out_ref[at] = (own[at] + part_recv[at].astype(F32)).astype(BF16)


def write_out(mixed, log_total, mixed_out, log_out, sems):
    copies = [
        pltpu.make_async_copy(mixed, mixed_out, sems.at[0]),
        pltpu.make_async_copy(log_total, log_out, sems.at[1]),
    ]
    for copy in copies:
        copy.start()
    for copy in copies:
        copy.wait()


def shards(n_kv, tokens, norm_gain, w_query, w_key, w_value, q_gain, k_gain, w_out, chosen):
    seqs, rows, half = tokens.shape
    nb, entries = chosen.shape[1:]
    q_cols, k_cols = w_query.shape[1], w_key.shape[1]
    heads = q_cols // HD
    n_z = n_kv // N_Y
    vmem = pltpu.VMEM
    dma = pltpu.SemaphoreType.DMA
    mixed, log_total = pl.pallas_call(
        functools.partial(kernel, n_kv),
        out_shape=(vmem((rows, half), BF16), vmem((heads, rows), F32)),
        in_specs=[pl.BlockSpec(memory_space=pltpu.HBM)] * 9,
        out_specs=(pl.BlockSpec(memory_space=vmem), pl.BlockSpec(memory_space=vmem)),
        scratch_shapes=[
            vmem((2, rows, half), BF16),
            vmem((nb, entries), jnp.int32),
            vmem((rows, q_cols + 2 * k_cols), F32),
            vmem((2, half, q_cols + 2 * k_cols), BF16),
            vmem((2, q_cols, half), BF16),
            vmem((2, 1, half), F32),
            vmem((2, 1, HD), F32),
            vmem((nb, n_kv * nb), F32),
            vmem((3, nb, n_kv * nb), F32),
            vmem((4, n_z, rows), F32),
            vmem((2, nb, entries), jnp.int32),
            pltpu.SMEM((2, nb, entries), jnp.int32),
            vmem((n_z, 2, MOST, BLK, LANES), BF16),
            vmem((n_z, 2, MOST, BLK, LANES), BF16),
            vmem((n_z, MOST, BLK, LANES), BF16),
            vmem((nb, heads * BLK, LANES), BF16),
            vmem((2, 1 + n_kv * nb, BLK, LANES), BF16),
            vmem((nb, entries * BLK), F32),
            vmem((rows, q_cols), BF16),
            vmem((rows, LANES), F32),
            vmem((rows, half), BF16),
            vmem((rows, half), BF16),
            dma((8,)),
            dma((2,)),
            dma((2, 3)),
            dma((1,)),
            dma((3, n_z)),
            dma((1,)),
            dma((2, PARTS)),
        ],
        compiler_params=pltpu.CompilerParams(
            collective_id=0, has_side_effects=True, vmem_limit_bytes=66_700_000
        ),
    )(
        tokens.reshape(rows, half), norm_gain.reshape(1, -1), w_query, w_key, w_value,
        q_gain.reshape(1, -1), k_gain.reshape(1, -1), w_out, chosen.reshape(nb, entries),
    )
    mixed, log_total = pl.pallas_call(
        write_out,
        out_shape=(
            jax.ShapeDtypeStruct((rows, half), BF16),
            jax.ShapeDtypeStruct((heads, rows), F32),
        ),
        in_specs=[pl.BlockSpec(memory_space=pl.ANY)] * 2,
        out_specs=(pl.BlockSpec(memory_space=pltpu.HBM),) * 2,
        scratch_shapes=[dma((2,))],
        compiler_params=pltpu.CompilerParams(vmem_limit_bytes=1_000_000),
    )(mixed, log_total)
    return mixed.reshape(seqs, rows, half), log_total.reshape(seqs, heads, rows)


def solution(mesh):
    in_specs = (
        P("dp", "kv", "tp"),
        P(),
        P(None, "tp"),
        P(None, "tp"),
        P(None, "tp"),
        P(),
        P(),
        P("tp", None),
        P("dp", "kv", None),
    )
    out_specs = (P("dp", "kv", "tp"), P("dp", "tp", "kv"))
    return jax.shard_map(
        functools.partial(shards, mesh.shape["kv"]),
        mesh=mesh, in_specs=in_specs, out_specs=out_specs, check_vma=False)
```

```python
import functools
import math

import jax
import jax.numpy as jnp
from jax import lax
from jax.experimental import pallas as pl
from jax.experimental.pallas import tpu as pltpu
from jax.sharding import PartitionSpec as P

HD = 64
BLK = 32
LANES = 128
MOST = 4
PARTS = 2
N_Y = 4
UP, DOWN, LEFT, RIGHT, FAR = range(5)

epsilon = 1e-06
alibi_reach = 4.0
LOG2E = math.log2(math.e)
F32 = jnp.float32
BF16 = jnp.bfloat16
NT = (((1,), (1,)), ((), ()))
MESH = pl.DeviceIdType.MESH


def iota(shape, dim):
    return lax.broadcasted_iota(jnp.int32, shape, dim)


def dot(a, b):
    return jnp.dot(a, b, preferred_element_type=F32)


def dot_nt(a, b):
    return lax.dot_general(a, b, NT, preferred_element_type=F32)


def kernel(
    n_kv,
    tok, gain, wq, wk, wv, qg, kg, wo, ch,
    out_ref, lt_ref,
    x_buf, ch_buf, raw_s, w_buf, wo_buf, g_buf, hg_buf,
    place_send, place_recv, code_s, index_v, index_s, left_s, right_s, far_s,
    q_s, kv0, kv1, kp_s, found_s, att_s, sum_s, part_send, part_recv,
    load_sem, x_sem, place_sem, send_sem, stage_sem, end_sem, part_sem,
):
    me = lax.axis_index("kv")
    tp = lax.axis_index("tp")
    partner = 1 - tp
    n_z = n_kv // N_Y
    z = me // N_Y
    y = me % N_Y
    rows, half = tok.shape
    q_cols = wq.shape[1]
    k_cols = wk.shape[1]
    heads = q_cols // HD
    kv_heads = k_cols // HD
    group = heads // kv_heads
    n_heads = heads * lax.axis_size("tp")
    nb, entries = ch.shape
    n_blocks = n_kv * nb
    width = half * 2
    seq_len = rows * n_kv
    alibi = alibi_reach / seq_len
    keys = entries * BLK
    picked = MOST * BLK
    kv = (kv0, kv1)

    def device(row, col):
        return lax.rem(row + n_z, n_z) * N_Y + lax.rem(col + N_Y, N_Y)

    neighbour = {
        UP: device(z + 1, y), DOWN: device(z - 1, y),
        LEFT: device(z, y - 1), RIGHT: device(z, y + 1), FAR: device(z, y + 2),
    }
    barrier = pltpu.get_barrier_semaphore()
    pl.semaphore_signal(barrier, inc=1, device_id={"tp": partner}, device_id_type=MESH)
    for target in neighbour.values():
        pl.semaphore_signal(barrier, inc=1, device_id={"kv": target}, device_id_type=MESH)

    def span(start):
        return pl.ds(pl.multiple_of(start * half, LANES), half)

    def load(sem, *pairs):
        for src, dst in pairs:
            pltpu.make_async_copy(src, dst, load_sem.at[sem]).start()

    def loaded(sem, whole):
        pltpu.make_async_copy(whole, whole, load_sem.at[sem]).wait()

    def weights(side, which):
        return (
            (wk.at[span(which), :], w_buf.at[side, :, q_cols:q_cols + k_cols]),
            (wv.at[span(which), :], w_buf.at[side, :, q_cols + k_cols:q_cols + 2 * k_cols]),
            (wq.at[span(which), :], w_buf.at[side, :, 0:q_cols]),
        )

    TABLE, TOK, GAIN, W0, W1, HEAD_GAIN, OUT, INDEX = range(8)
    load(TOK, (tok, x_buf.at[0]))
    load(TABLE, (ch, ch_buf))
    load(GAIN, (gain.at[:, span(tp)], g_buf.at[0]), (gain.at[:, span(partner)], g_buf.at[1]))
    load(W0, *weights(0, tp))
    load(W1, *weights(1, partner))
    load(HEAD_GAIN, (qg, hg_buf.at[0]), (kg, hg_buf.at[1]))

    def scaled(side):
        x = x_buf[side].astype(F32)
        return (x * g_buf[side]).astype(BF16), jnp.sum(x * x, axis=1, keepdims=True)

    loaded(TOK, x_buf.at[0])
    pl.semaphore_wait(barrier, 1 + len(neighbour))
    x_copy = pltpu.make_async_remote_copy(
        x_buf.at[0], x_buf.at[1], x_sem.at[0], x_sem.at[1],
        device_id={"tp": partner}, device_id_type=MESH)
    x_copy.start()

    loaded(TABLE, ch_buf)
    lists = ch_buf[...]
    lane_block = iota((nb, n_blocks), 1)
    hits = [lists[:, e:e + 1] == lane_block for e in range(entries)]
    hit = hits[0]
    for e in range(1, entries):
        hit = hit | hits[e]
    need = jnp.broadcast_to(jnp.max(jnp.where(hit, 1, 0), axis=0, keepdims=True), (nb, n_blocks))
    rank_of = jnp.zeros((nb, n_blocks), jnp.int32)
    for k in range(1, nb):
        rank_of = rank_of + jnp.where(lane_block % nb >= k, pltpu.roll(need, k, 1), 0)
    place_send[...] = jnp.where(need > 0, rank_of, -1).astype(F32)

    def place_copy(direction, slot):
        return pltpu.make_async_remote_copy(
            place_send, place_recv.at[slot], place_sem.at[0, slot], place_sem.at[1, slot],
            device_id={"kv": neighbour[direction]}, device_id_type=MESH)

    place_copies = [place_copy(RIGHT, 0), place_copy(LEFT, 1), place_copy(FAR, 2)]
    for copy in place_copies:
        copy.start()

    for side, which in ((0, tp), (1, partner)):
        for head in range(heads):
            to = head % group * LANES + head // group * HD
            load(OUT, (wo.at[head * HD:(head + 1) * HD, span(which)], wo_buf.at[side, to:to + HD]))

    loaded(GAIN, g_buf)
    loaded(W0, w_buf.at[0])
    y0, sq0 = scaled(0)
    raw_s[...] = dot(y0, w_buf[0])

    same_head = jnp.where(
        iota((LANES, LANES), 0) // HD == iota((LANES, LANES), 1) // HD, 1.0, 0.0).astype(BF16)

    def head_norm(v, gain_row):
        sq = v * v
        hi = sq.astype(BF16)
        lo = (sq - hi.astype(F32)).astype(BF16)
        total = dot(hi, same_head) + dot(lo, same_head)
        return v * lax.rsqrt(total / HD + epsilon) * gain_row

    loaded(HEAD_GAIN, hg_buf)
    loaded(W1, w_buf.at[1])
    qg_row = jnp.concatenate([hg_buf[0], hg_buf[0]], axis=1) * (HD ** -0.5 * LOG2E)
    kg_row = jnp.concatenate([hg_buf[1], hg_buf[1]], axis=1)
    low = iota((rows, LANES), 1) < HD
    x_copy.wait()
    y1, sq1 = scaled(1)
    row_scale = lax.rsqrt((sq0 + sq1) / width + epsilon)
    raw_kv = (raw_s[:, q_cols:] + dot(y1, w_buf[1, :, q_cols:])) * row_scale
    key_part = pltpu.roll(head_norm(raw_kv[:, 0:k_cols], kg_row), HD, 1)
    value_part = raw_kv[:, k_cols:]

    def base(row, col):
        return 1 + (row * N_Y + col) * nb

    own_tiles = (jnp.where(low, value_part, key_part), jnp.where(low, key_part, value_part))
    for tile in range(2):
        kv[tile][0] = jnp.zeros((BLK, LANES), BF16)
        kv[tile][pl.ds(base(z, y), nb)] = own_tiles[tile].astype(BF16).reshape(nb, BLK, LANES)

    last = n_z - 1
    reach_a, reach_b = n_z // 2, n_z // 2 - 1
    back_a, back_b = last - reach_a, last - reach_b
    sent = []

    def send(direction, src, dst, units, arrival, when, hop=None):
        chain = 0 if units == 2 else 1
        sent.append((units, when, hop is not None))

        @pl.when(when(z, y, hop))
        def _():
            pltpu.make_async_remote_copy(
                src, dst, send_sem.at[chain], arrival,
                device_id={"kv": neighbour[direction]}, device_id_type=MESH).start()

    def stage(kind, row):
        return stage_sem.at[kind, row]

    def tile_of(kind):
        return kind % 2

    def whole(kind, row, col):
        return kv[tile_of(kind)].at[pl.ds(base(row, col), nb)]

    def send_whole(direction, kind, row, col, when, hop=None):
        part = whole(kind, row, col)
        send(direction, part, part, 2, stage(kind, row), when, hop)

    def arrive(kind, row, col, when, hop=None):
        @pl.when(when(z, y, hop))
        def _():
            part = whole(kind, row, col)
            pltpu.make_async_remote_copy(
                part, part, send_sem.at[0], stage(kind, row),
                device_id={"kv": neighbour[UP]}, device_id_type=MESH).wait_recv()

    same_row = iota((picked, rows), 0) % BLK == iota((picked, rows), 1) % BLK
    row_slot = (iota((picked, rows), 0) // BLK).astype(F32)

    def chooser(which, row):
        code = code_s[which, pl.ds(row, 1), :]
        return jnp.where(same_row & (code == row_slot), 1.0, 0.0).astype(BF16)

    def item(kind, row, col):
        return kv[tile_of(kind)][pl.ds(base(row, col), nb)].reshape(rows, LANES)

    def blocks(x):
        return x.astype(BF16).reshape(-1, BLK, LANES)

    def send_chosen(direction, buf, tile, row, col, when, hop=None):
        send(direction, buf, kv[tile].at[pl.ds(base(row, col), MOST)], 1, end_sem.at[tile], when, hop)

    def choose_1(row, to_left, to_right, to_far, hop=None):
        @pl.when(to_left(z, y, hop) | to_right(z, y, hop) | to_far(z, y, hop))
        def _():
            code = jnp.concatenate([chooser(i, row) for i in (2, 0, 1)], axis=0)
            found = blocks(dot(code, item(1, row, y)))
            far_s[row, 1] = found[0:MOST]
            left_s[row, 1] = found[MOST:2 * MOST]
            right_s[row, 1] = found[2 * MOST:]

        send_chosen(FAR, far_s.at[row, 1], 1, row, y, to_far, hop)
        send_chosen(LEFT, left_s.at[row, 1], 1, row, y, to_left, hop)
        send_chosen(RIGHT, right_s.at[row, 1], 1, row, y, to_right, hop)

    def choose_0(row, to_left, hop=None):
        @pl.when(to_left(z, y, hop))
        def _():
            left_s[row, 0] = blocks(dot(chooser(0, row), item(0, row, y)))

        send_chosen(LEFT, left_s.at[row, 0], 0, row, y, to_left, hop)

    def choose_2(row, to_right, hop=None):
        @pl.when(to_right(z, y, hop))
        def _():
            right_s[row, 0] = blocks(dot(chooser(3, row), item(2, row, left_col)))

        send_chosen(RIGHT, right_s.at[row, 0], 0, row, left_col, to_right, hop)

    def choose_last(to_right, to_far):
        @pl.when(to_right(z, y, None))
        def _():
            code = jnp.concatenate([chooser(i, z) for i in (2, 1)], axis=0)
            found = blocks(dot(code, item(0, z, y)))
            far_s[z, 0] = found[0:MOST]
            right_s[z, 0] = found[MOST:]

        send_chosen(FAR, far_s.at[z, 0], 0, z, y, to_far)
        send_chosen(RIGHT, right_s.at[z, 0], 0, z, y, to_right)

    left_col = lax.rem(y + N_Y - 1, N_Y)
    send(RIGHT, whole(0, z, y), whole(0, z, y), 2, stage(2, z), lambda z, y, hop: z < last)
    for kind in (1, 0):
        send_whole(UP, kind, z, y, lambda z, y, hop: z < last)
        send_whole(DOWN, kind, z, y, lambda z, y, hop: z < back_a)

    raw = (raw_s[:, 0:q_cols] + dot(y1, w_buf[1, :, 0:q_cols])) * row_scale
    for tile in range(q_cols // LANES):
        q = head_norm(raw[:, tile * LANES:(tile + 1) * LANES], qg_row)
        turned = pltpu.roll(q, HD, 1)
        for odd in range(2):
            head = 2 * tile + odd
            side = head // group
            here = turned if odd == side else q
            here = jnp.where(low if side == 1 else ~low, here, 0.0).astype(BF16)
            for r in range(nb):
                q_s[r, head * BLK:(head + 1) * BLK] = here[r * BLK:(r + 1) * BLK]

    arrive(2, z, left_col, lambda z, y, hop: z < last)
    send_whole(UP, 2, z, left_col, lambda z, y, hop: z < last)
    send_whole(DOWN, 2, z, left_col, lambda z, y, hop: z < back_b)

    for copy in place_copies:
        copy.wait()
    spread = jnp.where(
        iota((n_blocks, rows), 0) % nb == iota((n_blocks, rows), 1) // BLK, 1.0, 0.0).astype(BF16)
    row_owner = iota((n_z, n_blocks), 0) * N_Y
    owner_lane = iota((n_z, n_blocks), 1) // nb
    for which, (slot, col) in enumerate(((0, y), (1, y), (2, y), (1, left_col))):
        mine = jnp.where(owner_lane == row_owner + col, place_recv[slot], 0.0)
        code_s[which] = dot(mine.astype(BF16), spread)

    lane_entry = iota((nb, entries), 1)
    rank = jnp.zeros((nb, entries), jnp.int32)
    for e in range(entries):
        found = jnp.max(jnp.where(hits[e], rank_of, 0), axis=1, keepdims=True)
        rank = jnp.where(lane_entry == e, found, rank)
    owner = lists // nb
    owner_row = owner // N_Y
    col = lax.rem(owner, N_Y)
    ranked = 1 + owner * nb + rank
    for tile in range(2):
        full = col == y
        if tile == 0:
            full = full | ((col == left_col) & (owner_row != last))
        index_v[tile] = jnp.where(lists < 0, 0, jnp.where(full, 1 + lists, ranked))
    index_copy = pltpu.make_async_copy(index_v, index_s, load_sem.at[INDEX])
    index_copy.start()

    lane = iota((nb, keys), 1)
    block = jnp.full((nb, keys), -1, jnp.int32)
    for e in range(entries):
        block = jnp.where(lane // BLK == e, lists[:, e:e + 1], block)
    away = (block - (me * nb + iota((nb, keys), 0))) * BLK + lane % BLK
    kp_s[...] = jnp.where(block < 0, 1 << 24, away).astype(F32)

    choose_1(z, lambda z, y, hop: y == 0, lambda z, y, hop: y < N_Y - 1, lambda z, y, hop: y < N_Y - 2)
    choose_0(z, lambda z, y, hop: y == 0)
    choose_last(
        lambda z, y, hop: (z == last) & (y < N_Y - 1), lambda z, y, hop: (z == last) & (y < N_Y - 2))
    choose_2(z, lambda z, y, hop: (z < last) & ((y == 1) | (y == 2)))

    routes = ((1, y, reach_a, back_a), (0, y, reach_a, back_a), (2, left_col, reach_b, back_b))
    hops = range(1, n_z // 2 + 1)

    def one_hop(hop, carry):
        above = lax.max(z - hop, 0)
        below = lax.rem(z + hop, n_z)
        for kind, col, reach, back in routes:

            def from_above(z, y, hop, reach=reach):
                return (z >= hop) & (hop <= reach)

            def go_up(z, y, hop, reach=reach):
                return (z >= hop) & (hop < reach) & (z < last)

            def from_below(z, y, hop, back=back):
                return ((z + hop) % n_z < back) & (hop <= back)

            def go_down(z, y, hop, back=back):
                return ((z + hop) % n_z < back) & (hop < back)

            def use_below(z, y, hop, back=back):
                return ((z + hop) % n_z < back) & (hop <= back) & ((z + hop) % n_z < z)

            arrive(kind, above, col, from_above, hop)
            send_whole(UP, kind, above, col, go_up, hop)
            arrive(kind, below, col, from_below, hop)
            send_whole(DOWN, kind, below, col, go_down, hop)
            for row, use in ((above, from_above), (below, use_below)):
                if kind == 1:
                    choose_1(row, use, use, use, hop)
                elif kind == 0:
                    choose_0(row, use, hop)
                else:
                    choose_2(row, use, hop)
        return carry

    lax.fori_loop(hops.start, hops.stop, one_hop, 0)

    def settle(count, sem):
        for k in range(n_z):
            @pl.when(z == k)
            def _():
                for j in range(N_Y):
                    units = count(k, j)
                    if units:
                        @pl.when(y == j)
                        def _():
                            part = kv0.at[0:units * MOST]
                            pltpu.make_async_copy(part, part, sem).wait()

    def due(tile):
        def count(z, y):
            if tile == 1:
                return (z + (y == N_Y - 1)) + (z + (y >= 1)) + (z + (y >= 2))
            if z == last:
                return (z + (y == N_Y - 1)) + z + (y >= 1) + (y >= 2)
            return (z + (y == N_Y - 1)) + (z + (y >= 2))
        return count

    query_row = iota((BLK, keys), 0).astype(F32)
    ones = jnp.ones((keys, LANES), BF16)
    tile_low = iota((BLK, LANES), 1) < HD
    tile_lane = iota((BLK, LANES), 1)
    core_slope = jnp.where(tp == 0, 1.0, 2.0 ** (-8.0 * heads / n_heads)).astype(F32)

    def slope_of(head):
        return core_slope * (2.0 ** (-8.0 * (head + 1) / n_heads))

    def attend(r, side):
        key_pos = kp_s[pl.ds(r, 1), :]
        allowed = key_pos <= query_row
        both = jnp.concatenate([kv[side][index_s[side, r, e]] for e in range(entries)], axis=0)
        scores = dot_nt(q_s[r, side * group * BLK:(side + 1) * group * BLK], both)
        weights = []
        for t in range(group):
            bias = key_pos * (slope_of(side * group + t) * (alibi * LOG2E))
            part = jnp.exp2(scores[t * BLK:(t + 1) * BLK] + bias)
            weights.append(jnp.where(allowed, part, 0.0).astype(BF16))
        return dot(jnp.concatenate(weights, axis=0), jnp.concatenate([both, ones], axis=1))

    def combine(r, outs):
        sums = jnp.ones((BLK, LANES), F32)
        at = pl.ds(pl.multiple_of(r * BLK, BLK), BLK)
        for t in range(group):
            first, second = (o[t * BLK:(t + 1) * BLK] for o in outs)
            top = jnp.where(tile_low, first[:, 0:LANES], second[:, 0:LANES])
            total = jnp.where(tile_low, first[:, LANES:], second[:, LANES:])
            att_s[at, t * LANES:(t + 1) * LANES] = (top / total).astype(BF16)
            sums = jnp.where(tile_lane == t, first[:, LANES:], sums)
            sums = jnp.where(tile_lane == t + group, second[:, LANES:], sums)
        sum_s[at] = sums

    loaded(OUT, wo_buf)
    part_rows = rows // PARTS

    def part_at(part):
        return pl.ds(pl.multiple_of(part * part_rows, part_rows), part_rows)

    def part_copy(part):
        at = part_at(part)
        return pltpu.make_async_remote_copy(
            part_send.at[at], part_recv.at[at], part_sem.at[0, part], part_sem.at[1, part],
            device_id={"tp": partner}, device_id_type=MESH)

    def one_part(part, carry):
        for i in range(nb // PARTS):
            r = part * (nb // PARTS) + i
            combine(r, (attend(r, 0), found_s[r]))
        at = part_at(part)
        part_send[at] = dot(att_s[at], wo_buf[1]).astype(BF16)
        part_copy(part).start()
        return carry

    def second_head(part, carry):
        for i in range(nb // PARTS):
            r = part * (nb // PARTS) + i
            found_s[r] = attend(r, 1)
        return carry

    index_copy.wait()
    settle(due(1), end_sem.at[1])
    lax.fori_loop(0, PARTS, second_head, 0)
    settle(due(0), end_sem.at[0])
    lax.fori_loop(0, PARTS, one_part, 0)

    own = dot(att_s[...], wo_buf[0])
    row_in = (iota((rows, LANES), 0) % BLK).astype(F32)
    slopes = jnp.exp2(-8.0 / n_heads * (tp * heads + iota((rows, LANES), 1) + 1).astype(F32))
    logs = jnp.log(sum_s[...]) - slopes * alibi * row_in
    lt_ref[...] = logs.T[0:heads]

    def all_sent(size):
        return lambda z, y: sum(
            units for units, when, looped in sent if units == size
            for hop in (hops if looped else (0,)) if when(z, y, hop))

    for chain in range(2):
        settle(all_sent(2 - chain), send_sem.at[chain])

    for part in range(PARTS):
        at = slice(part * part_rows, (part + 1) * part_rows)
        part_copy(part).wait()
        out_ref[at] = (own[at] + part_recv[at].astype(F32)).astype(BF16)


def write_out(mixed, log_total, mixed_out, log_out, sems):
    copies = [
        pltpu.make_async_copy(mixed, mixed_out, sems.at[0]),
        pltpu.make_async_copy(log_total, log_out, sems.at[1]),
    ]
    for copy in copies:
        copy.start()
    for copy in copies:
        copy.wait()


def shards(n_kv, tokens, norm_gain, w_query, w_key, w_value, q_gain, k_gain, w_out, chosen):
    seqs, rows, half = tokens.shape
    nb, entries = chosen.shape[1:]
    q_cols, k_cols = w_query.shape[1], w_key.shape[1]
    heads = q_cols // HD
    n_z = n_kv // N_Y
    vmem = pltpu.VMEM
    dma = pltpu.SemaphoreType.DMA
    mixed, log_total = pl.pallas_call(
        functools.partial(kernel, n_kv),
        out_shape=(vmem((rows, half), BF16), vmem((heads, rows), F32)),
        in_specs=[pl.BlockSpec(memory_space=pltpu.HBM)] * 9,
        out_specs=(pl.BlockSpec(memory_space=vmem), pl.BlockSpec(memory_space=vmem)),
        scratch_shapes=[
            vmem((2, rows, half), BF16),
            vmem((nb, entries), jnp.int32),
            vmem((rows, q_cols + 2 * k_cols), F32),
            vmem((2, half, q_cols + 2 * k_cols), BF16),
            vmem((2, q_cols, half), BF16),
            vmem((2, 1, half), F32),
            vmem((2, 1, HD), F32),
            vmem((nb, n_kv * nb), F32),
            vmem((3, nb, n_kv * nb), F32),
            vmem((4, n_z, rows), F32),
            vmem((2, nb, entries), jnp.int32),
            pltpu.SMEM((2, nb, entries), jnp.int32),
            vmem((n_z, 2, MOST, BLK, LANES), BF16),
            vmem((n_z, 2, MOST, BLK, LANES), BF16),
            vmem((n_z, 2, MOST, BLK, LANES), BF16),
            vmem((nb, heads * BLK, LANES), BF16),
            vmem((1 + n_kv * nb, BLK, LANES), BF16),
            vmem((1 + n_kv * nb, BLK, LANES), BF16),
            vmem((nb, entries * BLK), F32),
            vmem((nb, heads // 2 * BLK, 2 * LANES), F32),
            vmem((rows, q_cols), BF16),
            vmem((rows, LANES), F32),
            vmem((rows, half), BF16),
            vmem((rows, half), BF16),
            dma((8,)),
            dma((2,)),
            dma((2, 3)),
            dma((2,)),
            dma((3, n_z)),
            dma((2,)),
            dma((2, PARTS)),
        ],
        compiler_params=pltpu.CompilerParams(
            collective_id=0, has_side_effects=True, vmem_limit_bytes=66_700_000
        ),
    )(
        tokens.reshape(rows, half), norm_gain.reshape(1, -1), w_query, w_key, w_value,
        q_gain.reshape(1, -1), k_gain.reshape(1, -1), w_out, chosen.reshape(nb, entries),
    )
    mixed, log_total = pl.pallas_call(
        write_out,
        out_shape=(
            jax.ShapeDtypeStruct((rows, half), BF16),
            jax.ShapeDtypeStruct((heads, rows), F32),
        ),
        in_specs=[pl.BlockSpec(memory_space=pl.ANY)] * 2,
        out_specs=(pl.BlockSpec(memory_space=pltpu.HBM),) * 2,
        scratch_shapes=[dma((2,))],
        compiler_params=pltpu.CompilerParams(vmem_limit_bytes=1_000_000),
    )(mixed, log_total)
    return mixed.reshape(seqs, rows, half), log_total.reshape(seqs, heads, rows)


def solution(mesh):
    in_specs = (
        P("dp", "kv", "tp"),
        P(),
        P(None, "tp"),
        P(None, "tp"),
        P(None, "tp"),
        P(),
        P(),
        P("tp", None),
        P("dp", "kv", None),
    )
    out_specs = (P("dp", "kv", "tp"), P("dp", "tp", "kv"))
    return jax.shard_map(
        functools.partial(shards, mesh.shape["kv"]),
        mesh=mesh, in_specs=in_specs, out_specs=out_specs, check_vma=False)
```

```python
import functools
import math

import jax
import jax.numpy as jnp
from jax import lax
from jax.experimental import pallas as pl
from jax.experimental.pallas import tpu as pltpu
from jax.sharding import PartitionSpec as P

HD = 64
BLK = 32
LANES = 128
MOST = 4
PARTS = 2
N_Y = 4
UP, DOWN, LEFT, RIGHT, FAR = range(5)

epsilon = 1e-06
alibi_reach = 4.0
LOG2E = math.log2(math.e)
F32 = jnp.float32
BF16 = jnp.bfloat16
NT = (((1,), (1,)), ((), ()))
MESH = pl.DeviceIdType.MESH


def iota(shape, dim):
    return lax.broadcasted_iota(jnp.int32, shape, dim)


def dot(a, b):
    return jnp.dot(a, b, preferred_element_type=F32)


def dot_nt(a, b):
    return lax.dot_general(a, b, NT, preferred_element_type=F32)


def kernel(
    n_kv,
    tok, gain, wq, wk, wv, qg, kg, wo, ch,
    out_ref, lt_ref,
    x_buf, ch_buf, raw_s, w_buf, wo_buf, g_buf, hg_buf,
    place_send, place_recv, code_s, index_v, index_s, left_s, right_s, far_s,
    q_s, kv0, kv1, kp_s, found_s, att_s, sum_s, part_send, part_recv,
    load_sem, x_sem, place_sem, send_sem, stage_sem, end_sem, part_sem,
):
    me = lax.axis_index("kv")
    tp = lax.axis_index("tp")
    partner = 1 - tp
    n_z = n_kv // N_Y
    z = me // N_Y
    y = me % N_Y
    rows, half = tok.shape
    q_cols = wq.shape[1]
    k_cols = wk.shape[1]
    heads = q_cols // HD
    kv_heads = k_cols // HD
    group = heads // kv_heads
    n_heads = heads * lax.axis_size("tp")
    nb, entries = ch.shape
    n_blocks = n_kv * nb
    width = half * 2
    seq_len = rows * n_kv
    alibi = alibi_reach / seq_len
    keys = entries * BLK
    picked = MOST * BLK
    kv = (kv0, kv1)

    def device(row, col):
        return lax.rem(row + n_z, n_z) * N_Y + lax.rem(col + N_Y, N_Y)

    neighbour = {
        UP: device(z + 1, y), DOWN: device(z - 1, y),
        LEFT: device(z, y - 1), RIGHT: device(z, y + 1), FAR: device(z, y + 2),
    }
    barrier = pltpu.get_barrier_semaphore()
    pl.semaphore_signal(barrier, inc=1, device_id={"tp": partner}, device_id_type=MESH)
    for target in neighbour.values():
        pl.semaphore_signal(barrier, inc=1, device_id={"kv": target}, device_id_type=MESH)

    def span(start):
        return pl.ds(pl.multiple_of(start * half, LANES), half)

    def load(sem, *pairs):
        for src, dst in pairs:
            pltpu.make_async_copy(src, dst, load_sem.at[sem]).start()

    def loaded(sem, whole):
        pltpu.make_async_copy(whole, whole, load_sem.at[sem]).wait()

    def weights(side, which):
        return (
            (wk.at[span(which), :], w_buf.at[side, :, q_cols:q_cols + k_cols]),
            (wv.at[span(which), :], w_buf.at[side, :, q_cols + k_cols:q_cols + 2 * k_cols]),
            (wq.at[span(which), :], w_buf.at[side, :, 0:q_cols]),
        )

    TABLE, TOK, GAIN, W0, W1, HEAD_GAIN, OUT, INDEX = range(8)
    load(TOK, (tok, x_buf.at[0]))
    load(TABLE, (ch, ch_buf))
    load(GAIN, (gain.at[:, span(tp)], g_buf.at[0]), (gain.at[:, span(partner)], g_buf.at[1]))
    load(W0, *weights(0, tp))
    load(W1, *weights(1, partner))
    load(HEAD_GAIN, (qg, hg_buf.at[0]), (kg, hg_buf.at[1]))

    def scaled(side):
        x = x_buf[side].astype(F32)
        return (x * g_buf[side]).astype(BF16), jnp.sum(x * x, axis=1, keepdims=True)

    loaded(TOK, x_buf.at[0])
    pl.semaphore_wait(barrier, 1 + len(neighbour))
    x_copy = pltpu.make_async_remote_copy(
        x_buf.at[0], x_buf.at[1], x_sem.at[0], x_sem.at[1],
        device_id={"tp": partner}, device_id_type=MESH)
    x_copy.start()

    loaded(TABLE, ch_buf)
    lists = ch_buf[...]
    lane_block = iota((nb, n_blocks), 1)
    hits = [lists[:, e:e + 1] == lane_block for e in range(entries)]
    hit = hits[0]
    for e in range(1, entries):
        hit = hit | hits[e]
    need = jnp.broadcast_to(jnp.max(jnp.where(hit, 1, 0), axis=0, keepdims=True), (nb, n_blocks))
    rank_of = jnp.zeros((nb, n_blocks), jnp.int32)
    for k in range(1, nb):
        rank_of = rank_of + jnp.where(lane_block % nb >= k, pltpu.roll(need, k, 1), 0)
    place_send[...] = jnp.where(need > 0, rank_of, -1).astype(F32)

    def place_copy(direction, slot):
        return pltpu.make_async_remote_copy(
            place_send, place_recv.at[slot], place_sem.at[0, slot], place_sem.at[1, slot],
            device_id={"kv": neighbour[direction]}, device_id_type=MESH)

    place_copies = [place_copy(RIGHT, 0), place_copy(LEFT, 1), place_copy(FAR, 2)]
    for copy in place_copies:
        copy.start()

    for side, which in ((0, tp), (1, partner)):
        for head in range(heads):
            to = head % group * LANES + head // group * HD
            load(OUT, (wo.at[head * HD:(head + 1) * HD, span(which)], wo_buf.at[side, to:to + HD]))

    loaded(GAIN, g_buf)
    loaded(W0, w_buf.at[0])
    y0, sq0 = scaled(0)
    raw_s[...] = dot(y0, w_buf[0])

    same_head = jnp.where(
        iota((LANES, LANES), 0) // HD == iota((LANES, LANES), 1) // HD, 1.0, 0.0).astype(BF16)

    def head_norm(v, gain_row):
        sq = v * v
        hi = sq.astype(BF16)
        lo = (sq - hi.astype(F32)).astype(BF16)
        total = dot(hi, same_head) + dot(lo, same_head)
        return v * lax.rsqrt(total / HD + epsilon) * gain_row

    loaded(HEAD_GAIN, hg_buf)
    loaded(W1, w_buf.at[1])
    qg_row = jnp.concatenate([hg_buf[0], hg_buf[0]], axis=1) * (HD ** -0.5 * LOG2E)
    kg_row = jnp.concatenate([hg_buf[1], hg_buf[1]], axis=1)
    low = iota((rows, LANES), 1) < HD
    x_copy.wait()
    y1, sq1 = scaled(1)
    row_scale = lax.rsqrt((sq0 + sq1) / width + epsilon)
    raw_kv = (raw_s[:, q_cols:] + dot(y1, w_buf[1, :, q_cols:])) * row_scale
    key_part = pltpu.roll(head_norm(raw_kv[:, 0:k_cols], kg_row), HD, 1)
    value_part = raw_kv[:, k_cols:]

    def base(row, col):
        return 1 + (row * N_Y + col) * nb

    own_tiles = (jnp.where(low, value_part, key_part), jnp.where(low, key_part, value_part))
    for tile in range(2):
        kv[tile][0] = jnp.zeros((BLK, LANES), BF16)
        kv[tile][pl.ds(base(z, y), nb)] = own_tiles[tile].astype(BF16).reshape(nb, BLK, LANES)

    last = n_z - 1
    reach_a, reach_b = n_z // 2, n_z // 2 - 1
    back_a, back_b = last - reach_a, last - reach_b
    sent = []

    def send(direction, src, dst, units, arrival, when, hop=None):
        chain = 0 if units == 2 else 1
        sent.append((units, when, hop is not None))

        @pl.when(when(z, y, hop))
        def _():
            pltpu.make_async_remote_copy(
                src, dst, send_sem.at[chain], arrival,
                device_id={"kv": neighbour[direction]}, device_id_type=MESH).start()

    def stage(kind, row):
        return stage_sem.at[kind, row]

    def tile_of(kind):
        return kind % 2

    def whole(kind, row, col):
        return kv[tile_of(kind)].at[pl.ds(base(row, col), nb)]

    def send_whole(direction, kind, row, col, when, hop=None):
        part = whole(kind, row, col)
        send(direction, part, part, 2, stage(kind, row), when, hop)

    def arrive(kind, row, col, when, hop=None):
        @pl.when(when(z, y, hop))
        def _():
            part = whole(kind, row, col)
            pltpu.make_async_remote_copy(
                part, part, send_sem.at[0], stage(kind, row),
                device_id={"kv": neighbour[UP]}, device_id_type=MESH).wait_recv()

    same_row = iota((picked, rows), 0) % BLK == iota((picked, rows), 1) % BLK
    row_slot = (iota((picked, rows), 0) // BLK).astype(F32)

    def chooser(which, row):
        code = code_s[which, pl.ds(row, 1), :]
        return jnp.where(same_row & (code == row_slot), 1.0, 0.0).astype(BF16)

    def item(kind, row, col):
        return kv[tile_of(kind)][pl.ds(base(row, col), nb)].reshape(rows, LANES)

    def blocks(x):
        return x.astype(BF16).reshape(-1, BLK, LANES)

    def send_chosen(direction, buf, tile, row, col, when, hop=None):
        send(direction, buf, kv[tile].at[pl.ds(base(row, col), MOST)], 1, end_sem.at[tile], when, hop)

    def choose_1(row, to_left, to_right, to_far, hop=None):
        @pl.when(to_left(z, y, hop) | to_right(z, y, hop) | to_far(z, y, hop))
        def _():
            code = jnp.concatenate([chooser(i, row) for i in (2, 0, 1)], axis=0)
            found = blocks(dot(code, item(1, row, y)))
            far_s[row, 1] = found[0:MOST]
            left_s[row, 1] = found[MOST:2 * MOST]
            right_s[row, 1] = found[2 * MOST:]

        send_chosen(FAR, far_s.at[row, 1], 1, row, y, to_far, hop)
        send_chosen(LEFT, left_s.at[row, 1], 1, row, y, to_left, hop)
        send_chosen(RIGHT, right_s.at[row, 1], 1, row, y, to_right, hop)

    def choose_0(row, to_left, hop=None):
        @pl.when(to_left(z, y, hop))
        def _():
            left_s[row, 0] = blocks(dot(chooser(0, row), item(0, row, y)))

        send_chosen(LEFT, left_s.at[row, 0], 0, row, y, to_left, hop)

    def choose_2(row, to_right, hop=None):
        @pl.when(to_right(z, y, hop))
        def _():
            right_s[row, 0] = blocks(dot(chooser(3, row), item(2, row, left_col)))

        send_chosen(RIGHT, right_s.at[row, 0], 0, row, left_col, to_right, hop)

    def choose_last(to_right, to_far):
        @pl.when(to_right(z, y, None))
        def _():
            code = jnp.concatenate([chooser(i, z) for i in (2, 1)], axis=0)
            found = blocks(dot(code, item(0, z, y)))
            far_s[z, 0] = found[0:MOST]
            right_s[z, 0] = found[MOST:]

        send_chosen(FAR, far_s.at[z, 0], 0, z, y, to_far)
        send_chosen(RIGHT, right_s.at[z, 0], 0, z, y, to_right)

    left_col = lax.rem(y + N_Y - 1, N_Y)
    send(RIGHT, whole(0, z, y), whole(0, z, y), 2, stage(2, z), lambda z, y, hop: z < last)
    for kind in (1, 0):
        send_whole(UP, kind, z, y, lambda z, y, hop: z < last)
        send_whole(DOWN, kind, z, y, lambda z, y, hop: z < back_a)

    raw = (raw_s[:, 0:q_cols] + dot(y1, w_buf[1, :, 0:q_cols])) * row_scale
    for tile in range(q_cols // LANES):
        q = head_norm(raw[:, tile * LANES:(tile + 1) * LANES], qg_row)
        turned = pltpu.roll(q, HD, 1)
        for odd in range(2):
            head = 2 * tile + odd
            side = head // group
            here = turned if odd == side else q
            here = jnp.where(low if side == 1 else ~low, here, 0.0).astype(BF16)
            for r in range(nb):
                q_s[r, head * BLK:(head + 1) * BLK] = here[r * BLK:(r + 1) * BLK]

    for copy in place_copies:
        copy.wait()
    spread = jnp.where(
        iota((n_blocks, rows), 0) % nb == iota((n_blocks, rows), 1) // BLK, 1.0, 0.0).astype(BF16)
    row_owner = iota((n_z, n_blocks), 0) * N_Y
    owner_lane = iota((n_z, n_blocks), 1) // nb
    for which, (slot, col) in enumerate(((0, y), (1, y), (2, y), (1, left_col))):
        mine = jnp.where(owner_lane == row_owner + col, place_recv[slot], 0.0)
        code_s[which] = dot(mine.astype(BF16), spread)

    lane_entry = iota((nb, entries), 1)
    rank = jnp.zeros((nb, entries), jnp.int32)
    for e in range(entries):
        found = jnp.max(jnp.where(hits[e], rank_of, 0), axis=1, keepdims=True)
        rank = jnp.where(lane_entry == e, found, rank)
    owner = lists // nb
    owner_row = owner // N_Y
    col = lax.rem(owner, N_Y)
    ranked = 1 + owner * nb + rank
    for tile in range(2):
        full = col == y
        if tile == 0:
            full = full | ((col == left_col) & (owner_row != last))
        index_v[tile] = jnp.where(lists < 0, 0, jnp.where(full, 1 + lists, ranked))
    index_copy = pltpu.make_async_copy(index_v, index_s, load_sem.at[INDEX])
    index_copy.start()

    lane = iota((nb, keys), 1)
    block = jnp.full((nb, keys), -1, jnp.int32)
    for e in range(entries):
        block = jnp.where(lane // BLK == e, lists[:, e:e + 1], block)
    away = (block - (me * nb + iota((nb, keys), 0))) * BLK + lane % BLK
    kp_s[...] = jnp.where(block < 0, 1 << 24, away).astype(F32)

    arrive(2, z, left_col, lambda z, y, hop: z < last)
    send_whole(UP, 2, z, left_col, lambda z, y, hop: z < last)
    send_whole(DOWN, 2, z, left_col, lambda z, y, hop: z < back_b)
    choose_1(z, lambda z, y, hop: y == 0, lambda z, y, hop: y < N_Y - 1, lambda z, y, hop: y < N_Y - 2)
    choose_0(z, lambda z, y, hop: y == 0)
    choose_last(
        lambda z, y, hop: (z == last) & (y < N_Y - 1), lambda z, y, hop: (z == last) & (y < N_Y - 2))
    choose_2(z, lambda z, y, hop: (z < last) & ((y == 1) | (y == 2)))

    routes = ((1, y, reach_a, back_a), (0, y, reach_a, back_a), (2, left_col, reach_b, back_b))
    hops = range(1, n_z // 2 + 1)

    def one_hop(hop, carry):
        above = lax.max(z - hop, 0)
        below = lax.rem(z + hop, n_z)
        for kind, col, reach, back in routes:

            def from_above(z, y, hop, reach=reach):
                return (z >= hop) & (hop <= reach)

            def go_up(z, y, hop, reach=reach):
                return (z >= hop) & (hop < reach) & (z < last)

            def from_below(z, y, hop, back=back):
                return ((z + hop) % n_z < back) & (hop <= back)

            def go_down(z, y, hop, back=back):
                return ((z + hop) % n_z < back) & (hop < back)

            def use_below(z, y, hop, back=back):
                return ((z + hop) % n_z < back) & (hop <= back) & ((z + hop) % n_z < z)

            arrive(kind, above, col, from_above, hop)
            send_whole(UP, kind, above, col, go_up, hop)
            arrive(kind, below, col, from_below, hop)
            send_whole(DOWN, kind, below, col, go_down, hop)
            for row, use in ((above, from_above), (below, use_below)):
                if kind == 1:
                    choose_1(row, use, use, use, hop)
                elif kind == 0:
                    choose_0(row, use, hop)
                else:
                    choose_2(row, use, hop)
        return carry

    lax.fori_loop(hops.start, hops.stop, one_hop, 0)

    def settle(count, sem):
        for k in range(n_z):
            @pl.when(z == k)
            def _():
                for j in range(N_Y):
                    units = count(k, j)
                    if units:
                        @pl.when(y == j)
                        def _():
                            part = kv0.at[0:units * MOST]
                            pltpu.make_async_copy(part, part, sem).wait()

    def due(tile):
        def count(z, y):
            if tile == 1:
                return (z + (y == N_Y - 1)) + (z + (y >= 1)) + (z + (y >= 2))
            if z == last:
                return (z + (y == N_Y - 1)) + z + (y >= 1) + (y >= 2)
            return (z + (y == N_Y - 1)) + (z + (y >= 2))
        return count

    query_row = iota((BLK, keys), 0).astype(F32)
    ones = jnp.ones((keys, LANES), BF16)
    tile_low = iota((BLK, LANES), 1) < HD
    tile_lane = iota((BLK, LANES), 1)
    core_slope = jnp.where(tp == 0, 1.0, 2.0 ** (-8.0 * heads / n_heads)).astype(F32)

    def slope_of(head):
        return core_slope * (2.0 ** (-8.0 * (head + 1) / n_heads))

    def attend(r, side):
        key_pos = kp_s[pl.ds(r, 1), :]
        allowed = key_pos <= query_row
        both = jnp.concatenate([kv[side][index_s[side, r, e]] for e in range(entries)], axis=0)
        scores = dot_nt(q_s[r, side * group * BLK:(side + 1) * group * BLK], both)
        weights = []
        for t in range(group):
            bias = key_pos * (slope_of(side * group + t) * (alibi * LOG2E))
            part = jnp.exp2(scores[t * BLK:(t + 1) * BLK] + bias)
            weights.append(jnp.where(allowed, part, 0.0).astype(BF16))
        return dot(jnp.concatenate(weights, axis=0), jnp.concatenate([both, ones], axis=1))

    def combine(r, outs):
        sums = jnp.ones((BLK, LANES), F32)
        at = pl.ds(pl.multiple_of(r * BLK, BLK), BLK)
        for t in range(group):
            first, second = (o[t * BLK:(t + 1) * BLK] for o in outs)
            top = jnp.where(tile_low, first[:, 0:LANES], second[:, 0:LANES])
            total = jnp.where(tile_low, first[:, LANES:], second[:, LANES:])
            att_s[at, t * LANES:(t + 1) * LANES] = (top / total).astype(BF16)
            sums = jnp.where(tile_lane == t, first[:, LANES:], sums)
            sums = jnp.where(tile_lane == t + group, second[:, LANES:], sums)
        sum_s[at] = sums

    loaded(OUT, wo_buf)
    part_rows = rows // PARTS

    def part_at(part):
        return pl.ds(pl.multiple_of(part * part_rows, part_rows), part_rows)

    def part_copy(part):
        at = part_at(part)
        return pltpu.make_async_remote_copy(
            part_send.at[at], part_recv.at[at], part_sem.at[0, part], part_sem.at[1, part],
            device_id={"tp": partner}, device_id_type=MESH)

    def one_part(part, carry):
        for i in range(nb // PARTS):
            r = part * (nb // PARTS) + i
            combine(r, (attend(r, 0), found_s[r]))
        at = part_at(part)
        part_send[at] = dot(att_s[at], wo_buf[1]).astype(BF16)
        part_copy(part).start()
        return carry

    def second_head(part, carry):
        for i in range(nb // PARTS):
            r = part * (nb // PARTS) + i
            found_s[r] = attend(r, 1)
        return carry

    index_copy.wait()
    settle(due(1), end_sem.at[1])
    lax.fori_loop(0, PARTS, second_head, 0)
    settle(due(0), end_sem.at[0])
    lax.fori_loop(0, PARTS, one_part, 0)

    own = dot(att_s[...], wo_buf[0])
    row_in = (iota((rows, LANES), 0) % BLK).astype(F32)
    slopes = jnp.exp2(-8.0 / n_heads * (tp * heads + iota((rows, LANES), 1) + 1).astype(F32))
    logs = jnp.log(sum_s[...]) - slopes * alibi * row_in
    lt_ref[...] = logs.T[0:heads]

    def all_sent(size):
        return lambda z, y: sum(
            units for units, when, looped in sent if units == size
            for hop in (hops if looped else (0,)) if when(z, y, hop))

    for chain in range(2):
        settle(all_sent(2 - chain), send_sem.at[chain])

    for part in range(PARTS):
        at = slice(part * part_rows, (part + 1) * part_rows)
        part_copy(part).wait()
        out_ref[at] = (own[at] + part_recv[at].astype(F32)).astype(BF16)


def write_out(mixed, log_total, mixed_out, log_out, sems):
    copies = [
        pltpu.make_async_copy(mixed, mixed_out, sems.at[0]),
        pltpu.make_async_copy(log_total, log_out, sems.at[1]),
    ]
    for copy in copies:
        copy.start()
    for copy in copies:
        copy.wait()


def shards(n_kv, tokens, norm_gain, w_query, w_key, w_value, q_gain, k_gain, w_out, chosen):
    seqs, rows, half = tokens.shape
    nb, entries = chosen.shape[1:]
    q_cols, k_cols = w_query.shape[1], w_key.shape[1]
    heads = q_cols // HD
    n_z = n_kv // N_Y
    vmem = pltpu.VMEM
    dma = pltpu.SemaphoreType.DMA
    mixed, log_total = pl.pallas_call(
        functools.partial(kernel, n_kv),
        out_shape=(vmem((rows, half), BF16), vmem((heads, rows), F32)),
        in_specs=[pl.BlockSpec(memory_space=pltpu.HBM)] * 9,
        out_specs=(pl.BlockSpec(memory_space=vmem), pl.BlockSpec(memory_space=vmem)),
        scratch_shapes=[
            vmem((2, rows, half), BF16),
            vmem((nb, entries), jnp.int32),
            vmem((rows, q_cols + 2 * k_cols), F32),
            vmem((2, half, q_cols + 2 * k_cols), BF16),
            vmem((2, q_cols, half), BF16),
            vmem((2, 1, half), F32),
            vmem((2, 1, HD), F32),
            vmem((nb, n_kv * nb), F32),
            vmem((3, nb, n_kv * nb), F32),
            vmem((4, n_z, rows), F32),
            vmem((2, nb, entries), jnp.int32),
            pltpu.SMEM((2, nb, entries), jnp.int32),
            vmem((n_z, 2, MOST, BLK, LANES), BF16),
            vmem((n_z, 2, MOST, BLK, LANES), BF16),
            vmem((n_z, 2, MOST, BLK, LANES), BF16),
            vmem((nb, heads * BLK, LANES), BF16),
            vmem((1 + n_kv * nb, BLK, LANES), BF16),
            vmem((1 + n_kv * nb, BLK, LANES), BF16),
            vmem((nb, entries * BLK), F32),
            vmem((nb, heads // 2 * BLK, 2 * LANES), F32),
            vmem((rows, q_cols), BF16),
            vmem((rows, LANES), F32),
            vmem((rows, half), BF16),
            vmem((rows, half), BF16),
            dma((8,)),
            dma((2,)),
            dma((2, 3)),
            dma((2,)),
            dma((3, n_z)),
            dma((2,)),
            dma((2, PARTS)),
        ],
        compiler_params=pltpu.CompilerParams(
            collective_id=0, has_side_effects=True, vmem_limit_bytes=66_700_000
        ),
    )(
        tokens.reshape(rows, half), norm_gain.reshape(1, -1), w_query, w_key, w_value,
        q_gain.reshape(1, -1), k_gain.reshape(1, -1), w_out, chosen.reshape(nb, entries),
    )
    mixed, log_total = pl.pallas_call(
        write_out,
        out_shape=(
            jax.ShapeDtypeStruct((rows, half), BF16),
            jax.ShapeDtypeStruct((heads, rows), F32),
        ),
        in_specs=[pl.BlockSpec(memory_space=pl.ANY)] * 2,
        out_specs=(pl.BlockSpec(memory_space=pltpu.HBM),) * 2,
        scratch_shapes=[dma((2,))],
        compiler_params=pltpu.CompilerParams(vmem_limit_bytes=1_000_000),
    )(mixed, log_total)
    return mixed.reshape(seqs, rows, half), log_total.reshape(seqs, heads, rows)


def solution(mesh):
    in_specs = (
        P("dp", "kv", "tp"),
        P(),
        P(None, "tp"),
        P(None, "tp"),
        P(None, "tp"),
        P(),
        P(),
        P("tp", None),
        P("dp", "kv", None),
    )
    out_specs = (P("dp", "kv", "tp"), P("dp", "tp", "kv"))
    return jax.shard_map(
        functools.partial(shards, mesh.shape["kv"]),
        mesh=mesh, in_specs=in_specs, out_specs=out_specs, check_vma=False)
```

```python
import functools
import math

import jax
import jax.numpy as jnp
from jax import lax
from jax.experimental import pallas as pl
from jax.experimental.pallas import tpu as pltpu
from jax.sharding import PartitionSpec as P

HD = 64
BLK = 32
LANES = 128
MOST = 4
PARTS = 2
N_Y = 4
UP, DOWN, LEFT, RIGHT, FAR = range(5)

epsilon = 1e-06
alibi_reach = 4.0
LOG2E = math.log2(math.e)
F32 = jnp.float32
BF16 = jnp.bfloat16
NT = (((1,), (1,)), ((), ()))
MESH = pl.DeviceIdType.MESH


def iota(shape, dim):
    return lax.broadcasted_iota(jnp.int32, shape, dim)


def dot(a, b):
    return jnp.dot(a, b, preferred_element_type=F32)


def dot_nt(a, b):
    return lax.dot_general(a, b, NT, preferred_element_type=F32)


def kernel(
    n_kv,
    tok, gain, wq, wk, wv, qg, kg, wo, ch,
    out_ref, lt_ref,
    x_buf, ch_buf, raw_s, w_buf, wo_buf, g_buf, hg_buf,
    place_send, place_recv, code_s, index_v, index_s, left_s, right_s, far_s,
    q_s, kv0, kv1, kp_s, found_s, att_s, sum_s, part_send, part_recv,
    load_sem, x_sem, place_sem, send_sem, stage_sem, end_sem, part_sem,
):
    me = lax.axis_index("kv")
    tp = lax.axis_index("tp")
    partner = 1 - tp
    n_z = n_kv // N_Y
    z = me // N_Y
    y = me % N_Y
    rows, half = tok.shape
    q_cols = wq.shape[1]
    k_cols = wk.shape[1]
    heads = q_cols // HD
    kv_heads = k_cols // HD
    group = heads // kv_heads
    n_heads = heads * lax.axis_size("tp")
    nb, entries = ch.shape
    n_blocks = n_kv * nb
    width = half * 2
    seq_len = rows * n_kv
    alibi = alibi_reach / seq_len
    keys = entries * BLK
    picked = MOST * BLK
    kv = (kv0, kv1)

    def device(row, col):
        return lax.rem(row + n_z, n_z) * N_Y + lax.rem(col + N_Y, N_Y)

    neighbour = {
        UP: device(z + 1, y), DOWN: device(z - 1, y),
        LEFT: device(z, y - 1), RIGHT: device(z, y + 1), FAR: device(z, y + 2),
    }
    barrier = pltpu.get_barrier_semaphore()
    pl.semaphore_signal(barrier, inc=1, device_id={"tp": partner}, device_id_type=MESH)
    for target in neighbour.values():
        pl.semaphore_signal(barrier, inc=1, device_id={"kv": target}, device_id_type=MESH)

    def span(start):
        return pl.ds(pl.multiple_of(start * half, LANES), half)

    def load(sem, *pairs):
        for src, dst in pairs:
            pltpu.make_async_copy(src, dst, load_sem.at[sem]).start()

    def loaded(sem, whole):
        pltpu.make_async_copy(whole, whole, load_sem.at[sem]).wait()

    def weights(side, which):
        return (
            (wk.at[span(which), :], w_buf.at[side, :, q_cols:q_cols + k_cols]),
            (wv.at[span(which), :], w_buf.at[side, :, q_cols + k_cols:q_cols + 2 * k_cols]),
            (wq.at[span(which), :], w_buf.at[side, :, 0:q_cols]),
        )

    TABLE, TOK, GAIN, W0, W1, HEAD_GAIN, OUT, INDEX = range(8)
    load(TOK, (tok, x_buf.at[0]))
    load(TABLE, (ch, ch_buf))
    load(GAIN, (gain.at[:, span(tp)], g_buf.at[0]), (gain.at[:, span(partner)], g_buf.at[1]))
    load(W0, *weights(0, tp))
    load(W1, *weights(1, partner))
    load(HEAD_GAIN, (qg, hg_buf.at[0]), (kg, hg_buf.at[1]))

    def scaled(side):
        x = x_buf[side].astype(F32)
        return (x * g_buf[side]).astype(BF16), jnp.sum(x * x, axis=1, keepdims=True)

    loaded(TOK, x_buf.at[0])
    pl.semaphore_wait(barrier, 1 + len(neighbour))
    x_copy = pltpu.make_async_remote_copy(
        x_buf.at[0], x_buf.at[1], x_sem.at[0], x_sem.at[1],
        device_id={"tp": partner}, device_id_type=MESH)
    x_copy.start()

    loaded(TABLE, ch_buf)
    lists = ch_buf[...]
    lane_block = iota((nb, n_blocks), 1)
    hits = [lists[:, e:e + 1] == lane_block for e in range(entries)]
    hit = hits[0]
    for e in range(1, entries):
        hit = hit | hits[e]
    need = jnp.broadcast_to(jnp.max(jnp.where(hit, 1, 0), axis=0, keepdims=True), (nb, n_blocks))
    rank_of = jnp.zeros((nb, n_blocks), jnp.int32)
    for k in range(1, nb):
        rank_of = rank_of + jnp.where(lane_block % nb >= k, pltpu.roll(need, k, 1), 0)
    place_send[...] = jnp.where(need > 0, rank_of, -1).astype(F32)

    def place_copy(direction, slot):
        return pltpu.make_async_remote_copy(
            place_send, place_recv.at[slot], place_sem.at[0, slot], place_sem.at[1, slot],
            device_id={"kv": neighbour[direction]}, device_id_type=MESH)

    place_copies = [place_copy(RIGHT, 0), place_copy(LEFT, 1), place_copy(FAR, 2)]
    for copy in place_copies:
        copy.start()

    for side, which in ((0, tp), (1, partner)):
        for head in range(heads):
            to = head % group * LANES + head // group * HD
            load(OUT, (wo.at[head * HD:(head + 1) * HD, span(which)], wo_buf.at[side, to:to + HD]))

    loaded(GAIN, g_buf)
    loaded(W0, w_buf.at[0])
    y0, sq0 = scaled(0)
    raw_s[...] = dot(y0, w_buf[0])

    same_head = jnp.where(
        iota((LANES, LANES), 0) // HD == iota((LANES, LANES), 1) // HD, 1.0, 0.0).astype(BF16)

    def head_norm(v, gain_row):
        sq = v * v
        hi = sq.astype(BF16)
        lo = (sq - hi.astype(F32)).astype(BF16)
        total = dot(hi, same_head) + dot(lo, same_head)
        return v * lax.rsqrt(total / HD + epsilon) * gain_row

    loaded(HEAD_GAIN, hg_buf)
    loaded(W1, w_buf.at[1])
    qg_row = jnp.concatenate([hg_buf[0], hg_buf[0]], axis=1) * (HD ** -0.5 * LOG2E)
    kg_row = jnp.concatenate([hg_buf[1], hg_buf[1]], axis=1)
    low = iota((rows, LANES), 1) < HD
    x_copy.wait()
    y1, sq1 = scaled(1)
    row_scale = lax.rsqrt((sq0 + sq1) / width + epsilon)
    raw_kv = (raw_s[:, q_cols:] + dot(y1, w_buf[1, :, q_cols:])) * row_scale
    key_part = pltpu.roll(head_norm(raw_kv[:, 0:k_cols], kg_row), HD, 1)
    value_part = raw_kv[:, k_cols:]

    def base(row, col):
        return 1 + (row * N_Y + col) * nb

    own_tiles = (jnp.where(low, value_part, key_part), jnp.where(low, key_part, value_part))
    for tile in range(2):
        kv[tile][0] = jnp.zeros((BLK, LANES), BF16)
        kv[tile][pl.ds(base(z, y), nb)] = own_tiles[tile].astype(BF16).reshape(nb, BLK, LANES)

    last = n_z - 1
    reach_a, reach_b = n_z // 2, n_z // 2 - 1
    back_a, back_b = last - reach_a, last - reach_b
    sent = []

    def send(direction, src, dst, chain, units, arrival, when, hop=None):
        sent.append((chain, units, when, hop is not None))

        @pl.when(when(z, y, hop))
        def _():
            pltpu.make_async_remote_copy(
                src, dst, send_sem.at[chain], arrival,
                device_id={"kv": neighbour[direction]}, device_id_type=MESH).start()

    def stage(kind, row):
        return stage_sem.at[kind, row]

    def whole(kind, row, col):
        if kind < 2:
            return kv[kind].at[pl.ds(base(row, col), nb)]
        return kv0.at[pl.ds(base(row, col) + (kind - 2) * (nb // 2), nb // 2)]

    def send_whole(direction, kind, row, col, when, hop=None):
        part = whole(kind, row, col)
        send(direction, part, part, 0, 2 if kind < 2 else 1, stage(kind, row), when, hop)

    def arrive(kind, row, col, when, hop=None):
        @pl.when(when(z, y, hop))
        def _():
            part = whole(kind, row, col)
            pltpu.make_async_remote_copy(
                part, part, send_sem.at[0], stage(kind, row),
                device_id={"kv": neighbour[UP]}, device_id_type=MESH).wait_recv()

    same_row = iota((picked, rows), 0) % BLK == iota((picked, rows), 1) % BLK
    row_slot = (iota((picked, rows), 0) // BLK).astype(F32)

    def chooser(which, row):
        code = code_s[which, pl.ds(row, 1), :]
        return jnp.where(same_row & (code == row_slot), 1.0, 0.0).astype(BF16)

    def item(tile, row, col):
        return kv[tile][pl.ds(base(row, col), nb)].reshape(rows, LANES)

    def blocks(x):
        return x.astype(BF16).reshape(-1, BLK, LANES)

    def send_chosen(direction, buf, tile, row, col, when, hop=None):
        send(direction, buf, kv[tile].at[pl.ds(base(row, col), MOST)], 1, 1, end_sem.at[tile], when, hop)

    def choose_1(row, to_left, to_right, to_far, hop=None):
        @pl.when(to_left(z, y, hop) | to_right(z, y, hop) | to_far(z, y, hop))
        def _():
            code = jnp.concatenate([chooser(i, row) for i in (2, 0, 1)], axis=0)
            found = blocks(dot(code, item(1, row, y)))
            far_s[row, 1] = found[0:MOST]
            left_s[row, 1] = found[MOST:2 * MOST]
            right_s[row, 1] = found[2 * MOST:]

        send_chosen(FAR, far_s.at[row, 1], 1, row, y, to_far, hop)
        send_chosen(LEFT, left_s.at[row, 1], 1, row, y, to_left, hop)
        send_chosen(RIGHT, right_s.at[row, 1], 1, row, y, to_right, hop)

    def choose_0(row, to_left, hop=None):
        @pl.when(to_left(z, y, hop))
        def _():
            left_s[row, 0] = blocks(dot(chooser(0, row), item(0, row, y)))

        send_chosen(LEFT, left_s.at[row, 0], 0, row, y, to_left, hop)

    def choose_2(row, to_right, hop=None):
        @pl.when(to_right(z, y, hop))
        def _():
            right_s[row, 0] = blocks(dot(chooser(3, row), item(0, row, left_col)))

        send_chosen(RIGHT, right_s.at[row, 0], 0, row, left_col, to_right, hop)

    def choose_last(to_right, to_far):
        @pl.when(to_right(z, y, None))
        def _():
            code = jnp.concatenate([chooser(i, z) for i in (2, 1)], axis=0)
            found = blocks(dot(code, item(0, z, y)))
            far_s[z, 0] = found[0:MOST]
            right_s[z, 0] = found[MOST:]

        send_chosen(FAR, far_s.at[z, 0], 0, z, y, to_far)
        send_chosen(RIGHT, right_s.at[z, 0], 0, z, y, to_right)

    left_col = lax.rem(y + N_Y - 1, N_Y)
    for kind in (2, 3):
        send_whole(RIGHT, kind, z, y, lambda z, y, hop: z < last)
    for kind in (1, 0):
        send_whole(UP, kind, z, y, lambda z, y, hop: z < last)
        send_whole(DOWN, kind, z, y, lambda z, y, hop: z < back_a)

    raw = (raw_s[:, 0:q_cols] + dot(y1, w_buf[1, :, 0:q_cols])) * row_scale
    for tile in range(q_cols // LANES):
        q = head_norm(raw[:, tile * LANES:(tile + 1) * LANES], qg_row)
        turned = pltpu.roll(q, HD, 1)
        for odd in range(2):
            head = 2 * tile + odd
            side = head // group
            here = turned if odd == side else q
            here = jnp.where(low if side == 1 else ~low, here, 0.0).astype(BF16)
            for r in range(nb):
                q_s[r, head * BLK:(head + 1) * BLK] = here[r * BLK:(r + 1) * BLK]

    for copy in place_copies:
        copy.wait()
    spread = jnp.where(
        iota((n_blocks, rows), 0) % nb == iota((n_blocks, rows), 1) // BLK, 1.0, 0.0).astype(BF16)
    row_owner = iota((n_z, n_blocks), 0) * N_Y
    owner_lane = iota((n_z, n_blocks), 1) // nb
    for which, (slot, col) in enumerate(((0, y), (1, y), (2, y), (1, left_col))):
        mine = jnp.where(owner_lane == row_owner + col, place_recv[slot], 0.0)
        code_s[which] = dot(mine.astype(BF16), spread)

    lane_entry = iota((nb, entries), 1)
    rank = jnp.zeros((nb, entries), jnp.int32)
    for e in range(entries):
        found = jnp.max(jnp.where(hits[e], rank_of, 0), axis=1, keepdims=True)
        rank = jnp.where(lane_entry == e, found, rank)
    owner = lists // nb
    owner_row = owner // N_Y
    col = lax.rem(owner, N_Y)
    ranked = 1 + owner * nb + rank
    for tile in range(2):
        full = col == y
        if tile == 0:
            full = full | ((col == left_col) & (owner_row != last))
        index_v[tile] = jnp.where(lists < 0, 0, jnp.where(full, 1 + lists, ranked))
    index_copy = pltpu.make_async_copy(index_v, index_s, load_sem.at[INDEX])
    index_copy.start()

    lane = iota((nb, keys), 1)
    block = jnp.full((nb, keys), -1, jnp.int32)
    for e in range(entries):
        block = jnp.where(lane // BLK == e, lists[:, e:e + 1], block)
    away = (block - (me * nb + iota((nb, keys), 0))) * BLK + lane % BLK
    kp_s[...] = jnp.where(block < 0, 1 << 24, away).astype(F32)

    for kind in (2, 3):
        arrive(kind, z, left_col, lambda z, y, hop: z < last)
        send_whole(UP, kind, z, left_col, lambda z, y, hop: z < last)
        send_whole(DOWN, kind, z, left_col, lambda z, y, hop: z < back_b)
    choose_1(z, lambda z, y, hop: y == 0, lambda z, y, hop: y < N_Y - 1, lambda z, y, hop: y < N_Y - 2)
    choose_0(z, lambda z, y, hop: y == 0)
    choose_last(
        lambda z, y, hop: (z == last) & (y < N_Y - 1), lambda z, y, hop: (z == last) & (y < N_Y - 2))
    choose_2(z, lambda z, y, hop: (z < last) & ((y == 1) | (y == 2)))

    routes = (((1,), y, reach_a, back_a), ((0,), y, reach_a, back_a), ((2, 3), left_col, reach_b, back_b))
    hops = range(1, n_z // 2 + 1)

    def one_hop(hop, carry):
        above = lax.max(z - hop, 0)
        below = lax.rem(z + hop, n_z)
        for kinds, col, reach, back in routes:

            def from_above(z, y, hop, reach=reach):
                return (z >= hop) & (hop <= reach)

            def go_up(z, y, hop, reach=reach):
                return (z >= hop) & (hop < reach) & (z < last)

            def from_below(z, y, hop, back=back):
                return ((z + hop) % n_z < back) & (hop <= back)

            def go_down(z, y, hop, back=back):
                return ((z + hop) % n_z < back) & (hop < back)

            def use_below(z, y, hop, back=back):
                return ((z + hop) % n_z < back) & (hop <= back) & ((z + hop) % n_z < z)

            for kind in kinds:
                arrive(kind, above, col, from_above, hop)
                send_whole(UP, kind, above, col, go_up, hop)
                arrive(kind, below, col, from_below, hop)
                send_whole(DOWN, kind, below, col, go_down, hop)
            for row, use in ((above, from_above), (below, use_below)):
                if kinds == (1,):
                    choose_1(row, use, use, use, hop)
                elif kinds == (0,):
                    choose_0(row, use, hop)
                else:
                    choose_2(row, use, hop)
        return carry

    lax.fori_loop(hops.start, hops.stop, one_hop, 0)

    def settle(count, sem):
        for k in range(n_z):
            @pl.when(z == k)
            def _():
                for j in range(N_Y):
                    units = count(k, j)
                    if units:
                        @pl.when(y == j)
                        def _():
                            part = kv0.at[0:units * MOST]
                            pltpu.make_async_copy(part, part, sem).wait()

    def due(tile):
        def count(z, y):
            if tile == 1:
                return (z + (y == N_Y - 1)) + (z + (y >= 1)) + (z + (y >= 2))
            if z == last:
                return (z + (y == N_Y - 1)) + z + (y >= 1) + (y >= 2)
            return (z + (y == N_Y - 1)) + (z + (y >= 2))
        return count

    query_row = iota((BLK, keys), 0).astype(F32)
    ones = jnp.ones((keys, LANES), BF16)
    tile_low = iota((BLK, LANES), 1) < HD
    tile_lane = iota((BLK, LANES), 1)
    core_slope = jnp.where(tp == 0, 1.0, 2.0 ** (-8.0 * heads / n_heads)).astype(F32)

    def slope_of(head):
        return core_slope * (2.0 ** (-8.0 * (head + 1) / n_heads))

    def attend(r, side):
        key_pos = kp_s[pl.ds(r, 1), :]
        allowed = key_pos <= query_row
        both = jnp.concatenate([kv[side][index_s[side, r, e]] for e in range(entries)], axis=0)
        scores = dot_nt(q_s[r, side * group * BLK:(side + 1) * group * BLK], both)
        weights = []
        for t in range(group):
            bias = key_pos * (slope_of(side * group + t) * (alibi * LOG2E))
            part = jnp.exp2(scores[t * BLK:(t + 1) * BLK] + bias)
            weights.append(jnp.where(allowed, part, 0.0).astype(BF16))
        return dot(jnp.concatenate(weights, axis=0), jnp.concatenate([both, ones], axis=1))

    def combine(r, outs):
        sums = jnp.ones((BLK, LANES), F32)
        at = pl.ds(pl.multiple_of(r * BLK, BLK), BLK)
        for t in range(group):
            first, second = (o[t * BLK:(t + 1) * BLK] for o in outs)
            top = jnp.where(tile_low, first[:, 0:LANES], second[:, 0:LANES])
            total = jnp.where(tile_low, first[:, LANES:], second[:, LANES:])
            att_s[at, t * LANES:(t + 1) * LANES] = (top / total).astype(BF16)
            sums = jnp.where(tile_lane == t, first[:, LANES:], sums)
            sums = jnp.where(tile_lane == t + group, second[:, LANES:], sums)
        sum_s[at] = sums

    loaded(OUT, wo_buf)
    part_rows = rows // PARTS

    def part_at(part):
        return pl.ds(pl.multiple_of(part * part_rows, part_rows), part_rows)

    def part_copy(part):
        at = part_at(part)
        return pltpu.make_async_remote_copy(
            part_send.at[at], part_recv.at[at], part_sem.at[0, part], part_sem.at[1, part],
            device_id={"tp": partner}, device_id_type=MESH)

    def one_part(part, carry):
        for i in range(nb // PARTS):
            r = part * (nb // PARTS) + i
            combine(r, (attend(r, 0), found_s[r]))
        at = part_at(part)
        part_send[at] = dot(att_s[at], wo_buf[1]).astype(BF16)
        part_copy(part).start()
        return carry

    def second_head(part, carry):
        for i in range(nb // PARTS):
            r = part * (nb // PARTS) + i
            found_s[r] = attend(r, 1)
        return carry

    index_copy.wait()
    settle(due(1), end_sem.at[1])
    lax.fori_loop(0, PARTS, second_head, 0)
    settle(due(0), end_sem.at[0])
    lax.fori_loop(0, PARTS, one_part, 0)

    own = dot(att_s[...], wo_buf[0])
    row_in = (iota((rows, LANES), 0) % BLK).astype(F32)
    slopes = jnp.exp2(-8.0 / n_heads * (tp * heads + iota((rows, LANES), 1) + 1).astype(F32))
    logs = jnp.log(sum_s[...]) - slopes * alibi * row_in
    lt_ref[...] = logs.T[0:heads]

    def all_sent(which):
        return lambda z, y: sum(
            units for chain, units, when, looped in sent if chain == which
            for hop in (hops if looped else (0,)) if when(z, y, hop))

    for chain in range(2):
        settle(all_sent(chain), send_sem.at[chain])

    for part in range(PARTS):
        at = slice(part * part_rows, (part + 1) * part_rows)
        part_copy(part).wait()
        out_ref[at] = (own[at] + part_recv[at].astype(F32)).astype(BF16)


def write_out(mixed, log_total, mixed_out, log_out, sems):
    copies = [
        pltpu.make_async_copy(mixed, mixed_out, sems.at[0]),
        pltpu.make_async_copy(log_total, log_out, sems.at[1]),
    ]
    for copy in copies:
        copy.start()
    for copy in copies:
        copy.wait()


def shards(n_kv, tokens, norm_gain, w_query, w_key, w_value, q_gain, k_gain, w_out, chosen):
    seqs, rows, half = tokens.shape
    nb, entries = chosen.shape[1:]
    q_cols, k_cols = w_query.shape[1], w_key.shape[1]
    heads = q_cols // HD
    n_z = n_kv // N_Y
    vmem = pltpu.VMEM
    dma = pltpu.SemaphoreType.DMA
    mixed, log_total = pl.pallas_call(
        functools.partial(kernel, n_kv),
        out_shape=(vmem((rows, half), BF16), vmem((heads, rows), F32)),
        in_specs=[pl.BlockSpec(memory_space=pltpu.HBM)] * 9,
        out_specs=(pl.BlockSpec(memory_space=vmem), pl.BlockSpec(memory_space=vmem)),
        scratch_shapes=[
            vmem((2, rows, half), BF16),
            vmem((nb, entries), jnp.int32),
            vmem((rows, q_cols + 2 * k_cols), F32),
            vmem((2, half, q_cols + 2 * k_cols), BF16),
            vmem((2, q_cols, half), BF16),
            vmem((2, 1, half), F32),
            vmem((2, 1, HD), F32),
            vmem((nb, n_kv * nb), F32),
            vmem((3, nb, n_kv * nb), F32),
            vmem((4, n_z, rows), F32),
            vmem((2, nb, entries), jnp.int32),
            pltpu.SMEM((2, nb, entries), jnp.int32),
            vmem((n_z, 2, MOST, BLK, LANES), BF16),
            vmem((n_z, 2, MOST, BLK, LANES), BF16),
            vmem((n_z, 2, MOST, BLK, LANES), BF16),
            vmem((nb, heads * BLK, LANES), BF16),
            vmem((1 + n_kv * nb, BLK, LANES), BF16),
            vmem((1 + n_kv * nb, BLK, LANES), BF16),
            vmem((nb, entries * BLK), F32),
            vmem((nb, heads // 2 * BLK, 2 * LANES), F32),
            vmem((rows, q_cols), BF16),
            vmem((rows, LANES), F32),
            vmem((rows, half), BF16),
            vmem((rows, half), BF16),
            dma((8,)),
            dma((2,)),
            dma((2, 3)),
            dma((2,)),
            dma((4, n_z)),
            dma((2,)),
            dma((2, PARTS)),
        ],
        compiler_params=pltpu.CompilerParams(
            collective_id=0, has_side_effects=True, vmem_limit_bytes=66_700_000
        ),
    )(
        tokens.reshape(rows, half), norm_gain.reshape(1, -1), w_query, w_key, w_value,
        q_gain.reshape(1, -1), k_gain.reshape(1, -1), w_out, chosen.reshape(nb, entries),
    )
    mixed, log_total = pl.pallas_call(
        write_out,
        out_shape=(
            jax.ShapeDtypeStruct((rows, half), BF16),
            jax.ShapeDtypeStruct((heads, rows), F32),
        ),
        in_specs=[pl.BlockSpec(memory_space=pl.ANY)] * 2,
        out_specs=(pl.BlockSpec(memory_space=pltpu.HBM),) * 2,
        scratch_shapes=[dma((2,))],
        compiler_params=pltpu.CompilerParams(vmem_limit_bytes=1_000_000),
    )(mixed, log_total)
    return mixed.reshape(seqs, rows, half), log_total.reshape(seqs, heads, rows)


def solution(mesh):
    in_specs = (
        P("dp", "kv", "tp"),
        P(),
        P(None, "tp"),
        P(None, "tp"),
        P(None, "tp"),
        P(),
        P(),
        P("tp", None),
        P("dp", "kv", None),
    )
    out_specs = (P("dp", "kv", "tp"), P("dp", "tp", "kv"))
    return jax.shard_map(
        functools.partial(shards, mesh.shape["kv"]),
        mesh=mesh, in_specs=in_specs, out_specs=out_specs, check_vma=False)
```

```python
import functools
import math

import jax
import jax.numpy as jnp
from jax import lax
from jax.experimental import pallas as pl
from jax.experimental.pallas import tpu as pltpu
from jax.sharding import PartitionSpec as P

HD = 64
BLK = 32
LANES = 128
MOST = 4
PARTS = 2
N_Y = 4
UP, DOWN, LEFT, RIGHT, FAR = range(5)

epsilon = 1e-06
alibi_reach = 4.0
LOG2E = math.log2(math.e)
F32 = jnp.float32
BF16 = jnp.bfloat16
NT = (((1,), (1,)), ((), ()))
MESH = pl.DeviceIdType.MESH


def iota(shape, dim):
    return lax.broadcasted_iota(jnp.int32, shape, dim)


def dot(a, b):
    return jnp.dot(a, b, preferred_element_type=F32)


def dot_nt(a, b):
    return lax.dot_general(a, b, NT, preferred_element_type=F32)


def kernel(
    n_kv,
    tok, gain, wq, wk, wv, qg, kg, wo, ch,
    out_ref, lt_ref,
    x_buf, ch_buf, raw_s, w_buf, wo_buf, g_buf, hg_buf,
    place_send, place_recv, code_s, index_v, index_s, left_s, right_s, far_s,
    q_s, kv0, kv1, kp_s, found_s, att_s, sum_s, part_send, part_recv,
    load_sem, x_sem, place_sem, send_sem, stage_sem, end_sem, part_sem,
):
    me = lax.axis_index("kv")
    tp = lax.axis_index("tp")
    partner = 1 - tp
    n_z = n_kv // N_Y
    z = me // N_Y
    y = me % N_Y
    rows, half = tok.shape
    q_cols = wq.shape[1]
    k_cols = wk.shape[1]
    heads = q_cols // HD
    kv_heads = k_cols // HD
    group = heads // kv_heads
    n_heads = heads * lax.axis_size("tp")
    nb, entries = ch.shape
    n_blocks = n_kv * nb
    width = half * 2
    seq_len = rows * n_kv
    alibi = alibi_reach / seq_len
    keys = entries * BLK
    picked = MOST * BLK
    kv = (kv0, kv1)

    def device(row, col):
        return lax.rem(row + n_z, n_z) * N_Y + lax.rem(col + N_Y, N_Y)

    neighbour = {
        UP: device(z + 1, y), DOWN: device(z - 1, y),
        LEFT: device(z, y - 1), RIGHT: device(z, y + 1), FAR: device(z, y + 2),
    }
    barrier = pltpu.get_barrier_semaphore()
    pl.semaphore_signal(barrier, inc=1, device_id={"tp": partner}, device_id_type=MESH)
    for target in neighbour.values():
        pl.semaphore_signal(barrier, inc=1, device_id={"kv": target}, device_id_type=MESH)

    def span(start):
        return pl.ds(pl.multiple_of(start * half, LANES), half)

    def load(sem, *pairs):
        for src, dst in pairs:
            pltpu.make_async_copy(src, dst, load_sem.at[sem]).start()

    def loaded(sem, whole):
        pltpu.make_async_copy(whole, whole, load_sem.at[sem]).wait()

    def weights(side, which):
        return (
            (wk.at[span(which), :], w_buf.at[side, :, q_cols:q_cols + k_cols]),
            (wv.at[span(which), :], w_buf.at[side, :, q_cols + k_cols:q_cols + 2 * k_cols]),
            (wq.at[span(which), :], w_buf.at[side, :, 0:q_cols]),
        )

    TABLE, TOK, GAIN, W0, W1, HEAD_GAIN, OUT, INDEX = range(8)
    load(TOK, (tok, x_buf.at[0]))
    load(TABLE, (ch, ch_buf))
    load(GAIN, (gain.at[:, span(tp)], g_buf.at[0]), (gain.at[:, span(partner)], g_buf.at[1]))
    load(W0, *weights(0, tp))
    load(W1, *weights(1, partner))
    load(HEAD_GAIN, (qg, hg_buf.at[0]), (kg, hg_buf.at[1]))

    def scaled(side):
        x = x_buf[side].astype(F32)
        return (x * g_buf[side]).astype(BF16), jnp.sum(x * x, axis=1, keepdims=True)

    loaded(TOK, x_buf.at[0])
    pl.semaphore_wait(barrier, 1 + len(neighbour))
    x_copy = pltpu.make_async_remote_copy(
        x_buf.at[0], x_buf.at[1], x_sem.at[0], x_sem.at[1],
        device_id={"tp": partner}, device_id_type=MESH)
    x_copy.start()

    loaded(TABLE, ch_buf)
    lists = ch_buf[...]
    lane_block = iota((nb, n_blocks), 1)
    hits = [lists[:, e:e + 1] == lane_block for e in range(entries)]
    hit = hits[0]
    for e in range(1, entries):
        hit = hit | hits[e]
    need = jnp.broadcast_to(jnp.max(jnp.where(hit, 1, 0), axis=0, keepdims=True), (nb, n_blocks))
    rank_of = jnp.zeros((nb, n_blocks), jnp.int32)
    for k in range(1, nb):
        rank_of = rank_of + jnp.where(lane_block % nb >= k, pltpu.roll(need, k, 1), 0)
    place_send[...] = jnp.where(need > 0, rank_of, -1).astype(F32)

    def place_copy(direction, slot):
        return pltpu.make_async_remote_copy(
            place_send, place_recv.at[slot], place_sem.at[0, slot], place_sem.at[1, slot],
            device_id={"kv": neighbour[direction]}, device_id_type=MESH)

    place_copies = [place_copy(RIGHT, 0), place_copy(LEFT, 1), place_copy(FAR, 2)]
    for copy in place_copies:
        copy.start()

    for side, which in ((0, tp), (1, partner)):
        for head in range(heads):
            to = head % group * LANES + head // group * HD
            load(OUT, (wo.at[head * HD:(head + 1) * HD, span(which)], wo_buf.at[side, to:to + HD]))

    loaded(GAIN, g_buf)
    loaded(W0, w_buf.at[0])
    y0, sq0 = scaled(0)
    raw_s[...] = dot(y0, w_buf[0])

    same_head = jnp.where(
        iota((LANES, LANES), 0) // HD == iota((LANES, LANES), 1) // HD, 1.0, 0.0).astype(BF16)

    def head_norm(v, gain_row):
        sq = v * v
        hi = sq.astype(BF16)
        lo = (sq - hi.astype(F32)).astype(BF16)
        total = dot(hi, same_head) + dot(lo, same_head)
        return v * lax.rsqrt(total / HD + epsilon) * gain_row

    loaded(HEAD_GAIN, hg_buf)
    loaded(W1, w_buf.at[1])
    qg_row = jnp.concatenate([hg_buf[0], hg_buf[0]], axis=1) * (HD ** -0.5 * LOG2E)
    kg_row = jnp.concatenate([hg_buf[1], hg_buf[1]], axis=1)
    low = iota((rows, LANES), 1) < HD
    x_copy.wait()
    y1, sq1 = scaled(1)
    row_scale = lax.rsqrt((sq0 + sq1) / width + epsilon)
    raw_kv = (raw_s[:, q_cols:] + dot(y1, w_buf[1, :, q_cols:])) * row_scale
    key_part = pltpu.roll(head_norm(raw_kv[:, 0:k_cols], kg_row), HD, 1)
    value_part = raw_kv[:, k_cols:]

    def base(row, col):
        return 1 + (row * N_Y + col) * nb

    own_tiles = (jnp.where(low, value_part, key_part), jnp.where(low, key_part, value_part))
    for tile in range(2):
        kv[tile][0] = jnp.zeros((BLK, LANES), BF16)
        kv[tile][pl.ds(base(z, y), nb)] = own_tiles[tile].astype(BF16).reshape(nb, BLK, LANES)

    last = n_z - 1
    reach_a, reach_b = n_z // 2, n_z // 2 - 1
    back_a, back_b = last - reach_a, last - reach_b
    sent = []

    def send(direction, src, dst, units, arrival, when, hop=None):
        chain = 0 if units == 2 else 1
        sent.append((units, when, hop is not None))

        @pl.when(when(z, y, hop))
        def _():
            pltpu.make_async_remote_copy(
                src, dst, send_sem.at[chain], arrival,
                device_id={"kv": neighbour[direction]}, device_id_type=MESH).start()

    def stage(kind, row):
        return stage_sem.at[kind, row]

    def tile_of(kind):
        return kind % 2

    def whole(kind, row, col):
        return kv[tile_of(kind)].at[pl.ds(base(row, col), nb)]

    def send_whole(direction, kind, row, col, when, hop=None):
        part = whole(kind, row, col)
        send(direction, part, part, 2, stage(kind, row), when, hop)

    def arrive(kind, row, col, when, hop=None):
        @pl.when(when(z, y, hop))
        def _():
            part = whole(kind, row, col)
            pltpu.make_async_remote_copy(
                part, part, send_sem.at[0], stage(kind, row),
                device_id={"kv": neighbour[UP]}, device_id_type=MESH).wait_recv()

    same_row = iota((picked, rows), 0) % BLK == iota((picked, rows), 1) % BLK
    row_slot = (iota((picked, rows), 0) // BLK).astype(F32)

    def chooser(which, row):
        code = code_s[which, pl.ds(row, 1), :]
        return jnp.where(same_row & (code == row_slot), 1.0, 0.0).astype(BF16)

    def item(kind, row, col):
        return kv[tile_of(kind)][pl.ds(base(row, col), nb)].reshape(rows, LANES)

    def blocks(x):
        return x.astype(BF16).reshape(-1, BLK, LANES)

    def send_chosen(direction, buf, tile, row, col, when, hop=None):
        send(direction, buf, kv[tile].at[pl.ds(base(row, col), MOST)], 1, end_sem.at[tile], when, hop)

    def choose_1(row, to_left, to_right, to_far, hop=None):
        @pl.when(to_left(z, y, hop) | to_right(z, y, hop) | to_far(z, y, hop))
        def _():
            code = jnp.concatenate([chooser(i, row) for i in (2, 0, 1)], axis=0)
            found = blocks(dot(code, item(1, row, y)))
            far_s[row, 1] = found[0:MOST]
            left_s[row, 1] = found[MOST:2 * MOST]
            right_s[row, 1] = found[2 * MOST:]

        send_chosen(FAR, far_s.at[row, 1], 1, row, y, to_far, hop)
        send_chosen(LEFT, left_s.at[row, 1], 1, row, y, to_left, hop)
        send_chosen(RIGHT, right_s.at[row, 1], 1, row, y, to_right, hop)

    def choose_0(row, to_left, hop=None):
        @pl.when(to_left(z, y, hop))
        def _():
            left_s[row, 0] = blocks(dot(chooser(0, row), item(0, row, y)))

        send_chosen(LEFT, left_s.at[row, 0], 0, row, y, to_left, hop)

    def choose_2(row, to_right, hop=None):
        @pl.when(to_right(z, y, hop))
        def _():
            right_s[row, 0] = blocks(dot(chooser(3, row), item(2, row, left_col)))

        send_chosen(RIGHT, right_s.at[row, 0], 0, row, left_col, to_right, hop)

    def choose_last(to_right, to_far):
        @pl.when(to_right(z, y, None))
        def _():
            code = jnp.concatenate([chooser(i, z) for i in (2, 1)], axis=0)
            found = blocks(dot(code, item(0, z, y)))
            far_s[z, 0] = found[0:MOST]
            right_s[z, 0] = found[MOST:]

        send_chosen(FAR, far_s.at[z, 0], 0, z, y, to_far)
        send_chosen(RIGHT, right_s.at[z, 0], 0, z, y, to_right)

    left_col = lax.rem(y + N_Y - 1, N_Y)
    send(RIGHT, whole(0, z, y), whole(0, z, y), 2, stage(2, z), lambda z, y, hop: z < last)
    for kind in (1, 0):
        send_whole(UP, kind, z, y, lambda z, y, hop: z < last)
        send_whole(DOWN, kind, z, y, lambda z, y, hop: z < back_a)

    raw = (raw_s[:, 0:q_cols] + dot(y1, w_buf[1, :, 0:q_cols])) * row_scale
    for tile in range(q_cols // LANES):
        q = head_norm(raw[:, tile * LANES:(tile + 1) * LANES], qg_row)
        turned = pltpu.roll(q, HD, 1)
        for odd in range(2):
            head = 2 * tile + odd
            side = head // group
            here = turned if odd == side else q
            here = jnp.where(low if side == 1 else ~low, here, 0.0).astype(BF16)
            for r in range(nb):
                q_s[r, head * BLK:(head + 1) * BLK] = here[r * BLK:(r + 1) * BLK]

    for copy in place_copies:
        copy.wait()
    spread = jnp.where(
        iota((n_blocks, rows), 0) % nb == iota((n_blocks, rows), 1) // BLK, 1.0, 0.0).astype(BF16)
    row_owner = iota((n_z, n_blocks), 0) * N_Y
    owner_lane = iota((n_z, n_blocks), 1) // nb
    for which, (slot, col) in enumerate(((0, y), (1, y), (2, y), (1, left_col))):
        mine = jnp.where(owner_lane == row_owner + col, place_recv[slot], 0.0)
        code_s[which] = dot(mine.astype(BF16), spread)

    lane_entry = iota((nb, entries), 1)
    rank = jnp.zeros((nb, entries), jnp.int32)
    for e in range(entries):
        found = jnp.max(jnp.where(hits[e], rank_of, 0), axis=1, keepdims=True)
        rank = jnp.where(lane_entry == e, found, rank)
    owner = lists // nb
    owner_row = owner // N_Y
    col = lax.rem(owner, N_Y)
    ranked = 1 + owner * nb + rank
    for tile in range(2):
        full = col == y
        if tile == 0:
            full = full | ((col == left_col) & (owner_row != last))
        index_v[tile] = jnp.where(lists < 0, 0, jnp.where(full, 1 + lists, ranked))
    index_copy = pltpu.make_async_copy(index_v, index_s, load_sem.at[INDEX])
    index_copy.start()

    lane = iota((nb, keys), 1)
    block = jnp.full((nb, keys), -1, jnp.int32)
    for e in range(entries):
        block = jnp.where(lane // BLK == e, lists[:, e:e + 1], block)
    away = (block - (me * nb + iota((nb, keys), 0))) * BLK + lane % BLK
    kp_s[...] = jnp.where(block < 0, 1 << 24, away).astype(F32)

    arrive(2, z, left_col, lambda z, y, hop: z < last)
    send_whole(UP, 2, z, left_col, lambda z, y, hop: z < last)
    send_whole(DOWN, 2, z, left_col, lambda z, y, hop: z < back_b)
    choose_1(z, lambda z, y, hop: y == 0, lambda z, y, hop: y < N_Y - 1, lambda z, y, hop: y < N_Y - 2)
    choose_0(z, lambda z, y, hop: y == 0)
    choose_last(
        lambda z, y, hop: (z == last) & (y < N_Y - 1), lambda z, y, hop: (z == last) & (y < N_Y - 2))
    choose_2(z, lambda z, y, hop: (z < last) & ((y == 1) | (y == 2)))

    routes = ((1, y, reach_a, back_a), (0, y, reach_a, back_a), (2, left_col, reach_b, back_b))
    hops = range(1, n_z // 2 + 1)

    def one_hop(hop, carry):
        above = lax.max(z - hop, 0)
        below = lax.rem(z + hop, n_z)
        for kind, col, reach, back in routes:

            def from_above(z, y, hop, reach=reach):
                return (z >= hop) & (hop <= reach)

            def go_up(z, y, hop, reach=reach):
                return (z >= hop) & (hop < reach) & (z < last)

            def from_below(z, y, hop, back=back):
                return ((z + hop) % n_z < back) & (hop <= back)

            def go_down(z, y, hop, back=back):
                return ((z + hop) % n_z < back) & (hop < back)

            def use_below(z, y, hop, back=back):
                return ((z + hop) % n_z < back) & (hop <= back) & ((z + hop) % n_z < z)

            arrive(kind, above, col, from_above, hop)
            send_whole(UP, kind, above, col, go_up, hop)
            arrive(kind, below, col, from_below, hop)
            send_whole(DOWN, kind, below, col, go_down, hop)
            for row, use in ((above, from_above), (below, use_below)):
                if kind == 1:
                    choose_1(row, use, use, use, hop)
                elif kind == 0:
                    choose_0(row, use, hop)
                else:
                    choose_2(row, use, hop)
        return carry

    lax.fori_loop(hops.start, hops.stop, one_hop, 0)

    def settle(count, sem):
        for k in range(n_z):
            @pl.when(z == k)
            def _():
                for j in range(N_Y):
                    units = count(k, j)
                    if units:
                        @pl.when(y == j)
                        def _():
                            part = kv0.at[0:units * MOST]
                            pltpu.make_async_copy(part, part, sem).wait()

    def due(tile):
        def count(z, y):
            if tile == 1:
                return (z + (y == N_Y - 1)) + (z + (y >= 1)) + (z + (y >= 2))
            if z == last:
                return (z + (y == N_Y - 1)) + z + (y >= 1) + (y >= 2)
            return (z + (y == N_Y - 1)) + (z + (y >= 2))
        return count

    query_row = iota((BLK, keys), 0).astype(F32)
    ones = jnp.ones((keys, LANES), BF16)
    tile_low = iota((BLK, LANES), 1) < HD
    tile_lane = iota((BLK, LANES), 1)
    core_slope = jnp.where(tp == 0, 1.0, 2.0 ** (-8.0 * heads / n_heads)).astype(F32)

    def slope_of(head):
        return core_slope * (2.0 ** (-8.0 * (head + 1) / n_heads))

    def attend(r, side):
        key_pos = kp_s[pl.ds(r, 1), :]
        allowed = key_pos <= query_row
        both = jnp.concatenate([kv[side][index_s[side, r, e]] for e in range(entries)], axis=0)
        scores = dot_nt(q_s[r, side * group * BLK:(side + 1) * group * BLK], both)
        weights = []
        for t in range(group):
            bias = key_pos * (slope_of(side * group + t) * (alibi * LOG2E))
            part = jnp.exp2(scores[t * BLK:(t + 1) * BLK] + bias)
            weights.append(jnp.where(allowed, part, 0.0).astype(BF16))
        return dot(jnp.concatenate(weights, axis=0), jnp.concatenate([both, ones], axis=1))

    def combine(r, outs):
        sums = jnp.ones((BLK, LANES), F32)
        at = pl.ds(r * BLK, BLK)
        for t in range(group):
            first, second = (o[t * BLK:(t + 1) * BLK] for o in outs)
            top = jnp.where(tile_low, first[:, 0:LANES], second[:, 0:LANES])
            total = jnp.where(tile_low, first[:, LANES:], second[:, LANES:])
            att_s[at, t * LANES:(t + 1) * LANES] = (top / total).astype(BF16)
            sums = jnp.where(tile_lane == t, first[:, LANES:], sums)
            sums = jnp.where(tile_lane == t + group, second[:, LANES:], sums)
        sum_s[at] = sums

    loaded(OUT, wo_buf)
    part_rows = rows // PARTS

    def part_at(part):
        return pl.ds(part * part_rows, part_rows)

    def part_copy(part):
        at = part_at(part)
        return pltpu.make_async_remote_copy(
            part_send.at[at], part_recv.at[at], part_sem.at[0, part], part_sem.at[1, part],
            device_id={"tp": partner}, device_id_type=MESH)

    def one_part(part):
        for i in range(nb // PARTS):
            r = part * (nb // PARTS) + i
            combine(r, (attend(r, 0), found_s[r]))
        at = part_at(part)
        part_send[at] = dot(att_s[at], wo_buf[1]).astype(BF16)
        part_copy(part).start()

    index_copy.wait()
    settle(due(1), end_sem.at[1])
    for r in range(nb):
        found_s[r] = attend(r, 1)
    settle(due(0), end_sem.at[0])
    for part in range(PARTS):
        one_part(part)

    own = dot(att_s[...], wo_buf[0])
    row_in = (iota((rows, LANES), 0) % BLK).astype(F32)
    slopes = jnp.exp2(-8.0 / n_heads * (tp * heads + iota((rows, LANES), 1) + 1).astype(F32))
    logs = jnp.log(sum_s[...]) - slopes * alibi * row_in
    lt_ref[...] = logs.T[0:heads]

    def all_sent(size):
        return lambda z, y: sum(
            units for units, when, looped in sent if units == size
            for hop in (hops if looped else (0,)) if when(z, y, hop))

    for chain in range(2):
        settle(all_sent(2 - chain), send_sem.at[chain])

    for part in range(PARTS):
        at = slice(part * part_rows, (part + 1) * part_rows)
        part_copy(part).wait()
        out_ref[at] = (own[at] + part_recv[at].astype(F32)).astype(BF16)


def write_out(mixed, log_total, mixed_out, log_out, sems):
    copies = [
        pltpu.make_async_copy(mixed, mixed_out, sems.at[0]),
        pltpu.make_async_copy(log_total, log_out, sems.at[1]),
    ]
    for copy in copies:
        copy.start()
    for copy in copies:
        copy.wait()


def shards(n_kv, tokens, norm_gain, w_query, w_key, w_value, q_gain, k_gain, w_out, chosen):
    seqs, rows, half = tokens.shape
    nb, entries = chosen.shape[1:]
    q_cols, k_cols = w_query.shape[1], w_key.shape[1]
    heads = q_cols // HD
    n_z = n_kv // N_Y
    vmem = pltpu.VMEM
    dma = pltpu.SemaphoreType.DMA
    mixed, log_total = pl.pallas_call(
        functools.partial(kernel, n_kv),
        out_shape=(vmem((rows, half), BF16), vmem((heads, rows), F32)),
        in_specs=[pl.BlockSpec(memory_space=pltpu.HBM)] * 9,
        out_specs=(pl.BlockSpec(memory_space=vmem), pl.BlockSpec(memory_space=vmem)),
        scratch_shapes=[
            vmem((2, rows, half), BF16),
            vmem((nb, entries), jnp.int32),
            vmem((rows, q_cols + 2 * k_cols), F32),
            vmem((2, half, q_cols + 2 * k_cols), BF16),
            vmem((2, q_cols, half), BF16),
            vmem((2, 1, half), F32),
            vmem((2, 1, HD), F32),
            vmem((nb, n_kv * nb), F32),
            vmem((3, nb, n_kv * nb), F32),
            vmem((4, n_z, rows), F32),
            vmem((2, nb, entries), jnp.int32),
            pltpu.SMEM((2, nb, entries), jnp.int32),
            vmem((n_z, 2, MOST, BLK, LANES), BF16),
            vmem((n_z, 2, MOST, BLK, LANES), BF16),
            vmem((n_z, 2, MOST, BLK, LANES), BF16),
            vmem((nb, heads * BLK, LANES), BF16),
            vmem((1 + n_kv * nb, BLK, LANES), BF16),
            vmem((1 + n_kv * nb, BLK, LANES), BF16),
            vmem((nb, entries * BLK), F32),
            vmem((nb, heads // 2 * BLK, 2 * LANES), F32),
            vmem((rows, q_cols), BF16),
            vmem((rows, LANES), F32),
            vmem((rows, half), BF16),
            vmem((rows, half), BF16),
            dma((8,)),
            dma((2,)),
            dma((2, 3)),
            dma((2,)),
            dma((3, n_z)),
            dma((2,)),
            dma((2, PARTS)),
        ],
        compiler_params=pltpu.CompilerParams(
            collective_id=0, has_side_effects=True, vmem_limit_bytes=66_700_000
        ),
    )(
        tokens.reshape(rows, half), norm_gain.reshape(1, -1), w_query, w_key, w_value,
        q_gain.reshape(1, -1), k_gain.reshape(1, -1), w_out, chosen.reshape(nb, entries),
    )
    mixed, log_total = pl.pallas_call(
        write_out,
        out_shape=(
            jax.ShapeDtypeStruct((rows, half), BF16),
            jax.ShapeDtypeStruct((heads, rows), F32),
        ),
        in_specs=[pl.BlockSpec(memory_space=pl.ANY)] * 2,
        out_specs=(pl.BlockSpec(memory_space=pltpu.HBM),) * 2,
        scratch_shapes=[dma((2,))],
        compiler_params=pltpu.CompilerParams(vmem_limit_bytes=1_000_000),
    )(mixed, log_total)
    return mixed.reshape(seqs, rows, half), log_total.reshape(seqs, heads, rows)


def solution(mesh):
    in_specs = (
        P("dp", "kv", "tp"),
        P(),
        P(None, "tp"),
        P(None, "tp"),
        P(None, "tp"),
        P(),
        P(),
        P("tp", None),
        P("dp", "kv", None),
    )
    out_specs = (P("dp", "kv", "tp"), P("dp", "tp", "kv"))
    return jax.shard_map(
        functools.partial(shards, mesh.shape["kv"]),
        mesh=mesh, in_specs=in_specs, out_specs=out_specs, check_vma=False)
```

```python
import functools
import math

import jax
import jax.numpy as jnp
from jax import lax
from jax.experimental import pallas as pl
from jax.experimental.pallas import tpu as pltpu
from jax.sharding import PartitionSpec as P

HD = 64
BLK = 32
LANES = 128
MOST = 4
PARTS = 2
N_Y = 4
UP, DOWN, LEFT, RIGHT, FAR = range(5)

epsilon = 1e-06
alibi_reach = 4.0
LOG2E = math.log2(math.e)
F32 = jnp.float32
BF16 = jnp.bfloat16
NT = (((1,), (1,)), ((), ()))
MESH = pl.DeviceIdType.MESH


def iota(shape, dim):
    return lax.broadcasted_iota(jnp.int32, shape, dim)


def dot(a, b):
    return jnp.dot(a, b, preferred_element_type=F32)


def dot_nt(a, b):
    return lax.dot_general(a, b, NT, preferred_element_type=F32)


def kernel(
    n_kv,
    tok, gain, wq, wk, wv, qg, kg, wo, ch,
    out_ref, lt_ref,
    x_buf, ch_buf, raw_s, w_buf, wo_buf, g_buf, hg_buf,
    place_send, place_recv, code_s, index_v, index_s, left_s, right_s, far_s,
    q_s, kv0, kv1, kp_s, found_s, att_s, sum_s, part_send, part_recv,
    load_sem, x_sem, place_sem, send_sem, stage_sem, end_sem, part_sem,
):
    me = lax.axis_index("kv")
    tp = lax.axis_index("tp")
    partner = 1 - tp
    n_z = n_kv // N_Y
    z = me // N_Y
    y = me % N_Y
    rows, half = tok.shape
    q_cols = wq.shape[1]
    k_cols = wk.shape[1]
    heads = q_cols // HD
    kv_heads = k_cols // HD
    group = heads // kv_heads
    n_heads = heads * lax.axis_size("tp")
    nb, entries = ch.shape
    n_blocks = n_kv * nb
    width = half * 2
    seq_len = rows * n_kv
    alibi = alibi_reach / seq_len
    keys = entries * BLK
    picked = MOST * BLK
    kv = (kv0, kv1)

    def device(row, col):
        return lax.rem(row + n_z, n_z) * N_Y + lax.rem(col + N_Y, N_Y)

    neighbour = {
        UP: device(z + 1, y), DOWN: device(z - 1, y),
        LEFT: device(z, y - 1), RIGHT: device(z, y + 1), FAR: device(z, y + 2),
    }
    barrier = pltpu.get_barrier_semaphore()
    pl.semaphore_signal(barrier, inc=1, device_id={"tp": partner}, device_id_type=MESH)
    for target in neighbour.values():
        pl.semaphore_signal(barrier, inc=1, device_id={"kv": target}, device_id_type=MESH)

    def span(start):
        return pl.ds(pl.multiple_of(start * half, LANES), half)

    def load(sem, *pairs):
        for src, dst in pairs:
            pltpu.make_async_copy(src, dst, load_sem.at[sem]).start()

    def loaded(sem, whole):
        pltpu.make_async_copy(whole, whole, load_sem.at[sem]).wait()

    def weights(side, which):
        return (
            (wk.at[span(which), :], w_buf.at[side, :, q_cols:q_cols + k_cols]),
            (wv.at[span(which), :], w_buf.at[side, :, q_cols + k_cols:q_cols + 2 * k_cols]),
            (wq.at[span(which), :], w_buf.at[side, :, 0:q_cols]),
        )

    TABLE, TOK, GAIN, W0, W1, HEAD_GAIN, OUT, INDEX = range(8)
    load(TOK, (tok, x_buf.at[0]))
    load(TABLE, (ch, ch_buf))
    load(GAIN, (gain.at[:, span(tp)], g_buf.at[0]), (gain.at[:, span(partner)], g_buf.at[1]))
    load(W0, *weights(0, tp))
    load(W1, *weights(1, partner))
    load(HEAD_GAIN, (qg, hg_buf.at[0]), (kg, hg_buf.at[1]))

    def scaled(side):
        x = x_buf[side].astype(F32)
        return (x * g_buf[side]).astype(BF16), jnp.sum(x * x, axis=1, keepdims=True)

    loaded(TOK, x_buf.at[0])
    pl.semaphore_wait(barrier, 1 + len(neighbour))
    x_copy = pltpu.make_async_remote_copy(
        x_buf.at[0], x_buf.at[1], x_sem.at[0], x_sem.at[1],
        device_id={"tp": partner}, device_id_type=MESH)
    x_copy.start()

    loaded(TABLE, ch_buf)
    lists = ch_buf[...]
    lane_block = iota((nb, n_blocks), 1)
    hits = [lists[:, e:e + 1] == lane_block for e in range(entries)]
    hit = hits[0]
    for e in range(1, entries):
        hit = hit | hits[e]
    need = jnp.broadcast_to(jnp.max(jnp.where(hit, 1, 0), axis=0, keepdims=True), (nb, n_blocks))
    rank_of = jnp.zeros((nb, n_blocks), jnp.int32)
    for k in range(1, nb):
        rank_of = rank_of + jnp.where(lane_block % nb >= k, pltpu.roll(need, k, 1), 0)
    place_send[...] = jnp.where(need > 0, rank_of, -1).astype(F32)

    def place_copy(direction, slot):
        return pltpu.make_async_remote_copy(
            place_send, place_recv.at[slot], place_sem.at[0, slot], place_sem.at[1, slot],
            device_id={"kv": neighbour[direction]}, device_id_type=MESH)

    place_copies = [place_copy(RIGHT, 0), place_copy(LEFT, 1), place_copy(FAR, 2)]
    for copy in place_copies:
        copy.start()

    for side, which in ((0, tp), (1, partner)):
        for head in range(heads):
            to = head % group * LANES + head // group * HD
            load(OUT, (wo.at[head * HD:(head + 1) * HD, span(which)], wo_buf.at[side, to:to + HD]))

    loaded(GAIN, g_buf)
    loaded(W0, w_buf.at[0])
    y0, sq0 = scaled(0)
    raw_s[...] = dot(y0, w_buf[0])

    same_head = jnp.where(
        iota((LANES, LANES), 0) // HD == iota((LANES, LANES), 1) // HD, 1.0, 0.0).astype(BF16)

    def head_norm(v, gain_row):
        sq = v * v
        hi = sq.astype(BF16)
        lo = (sq - hi.astype(F32)).astype(BF16)
        total = dot(hi, same_head) + dot(lo, same_head)
        return v * lax.rsqrt(total / HD + epsilon) * gain_row

    loaded(HEAD_GAIN, hg_buf)
    loaded(W1, w_buf.at[1])
    qg_row = jnp.concatenate([hg_buf[0], hg_buf[0]], axis=1) * (HD ** -0.5 * LOG2E)
    kg_row = jnp.concatenate([hg_buf[1], hg_buf[1]], axis=1)
    low = iota((rows, LANES), 1) < HD
    x_copy.wait()
    y1, sq1 = scaled(1)
    row_scale = lax.rsqrt((sq0 + sq1) / width + epsilon)
    raw_kv = (raw_s[:, q_cols:] + dot(y1, w_buf[1, :, q_cols:])) * row_scale
    key_part = pltpu.roll(head_norm(raw_kv[:, 0:k_cols], kg_row), HD, 1)
    value_part = raw_kv[:, k_cols:]

    def base(row, col):
        return 1 + (row * N_Y + col) * nb

    own_tiles = (jnp.where(low, value_part, key_part), jnp.where(low, key_part, value_part))
    for tile in range(2):
        kv[tile][0] = jnp.zeros((BLK, LANES), BF16)
        kv[tile][pl.ds(base(z, y), nb)] = own_tiles[tile].astype(BF16).reshape(nb, BLK, LANES)

    last = n_z - 1
    reach_a, reach_b = n_z // 2, n_z // 2 - 1
    back_a, back_b = last - reach_a, last - reach_b
    sent = []

    def send(direction, src, dst, chain, units, arrival, when, hop=None):
        sent.append((chain, units, when, hop is not None))

        @pl.when(when(z, y, hop))
        def _():
            pltpu.make_async_remote_copy(
                src, dst, send_sem.at[chain], arrival,
                device_id={"kv": neighbour[direction]}, device_id_type=MESH).start()

    def stage(kind, row):
        return stage_sem.at[kind, row]

    def whole(kind, row, col):
        if kind < 2:
            return kv[kind].at[pl.ds(base(row, col), nb)]
        return kv0.at[pl.ds(base(row, col) + (kind - 2) * (nb // 2), nb // 2)]

    def send_whole(direction, kind, row, col, when, hop=None):
        part = whole(kind, row, col)
        send(direction, part, part, 0, 2 if kind < 2 else 1, stage(kind, row), when, hop)

    def arrive(kind, row, col, when, hop=None):
        @pl.when(when(z, y, hop))
        def _():
            part = whole(kind, row, col)
            pltpu.make_async_remote_copy(
                part, part, send_sem.at[0], stage(kind, row),
                device_id={"kv": neighbour[UP]}, device_id_type=MESH).wait_recv()

    same_row = iota((picked, rows), 0) % BLK == iota((picked, rows), 1) % BLK
    row_slot = (iota((picked, rows), 0) // BLK).astype(F32)

    def chooser(which, row):
        code = code_s[which, pl.ds(row, 1), :]
        return jnp.where(same_row & (code == row_slot), 1.0, 0.0).astype(BF16)

    def item(tile, row, col):
        return kv[tile][pl.ds(base(row, col), nb)].reshape(rows, LANES)

    def blocks(x):
        return x.astype(BF16).reshape(-1, BLK, LANES)

    def send_chosen(direction, buf, tile, row, col, when, hop=None):
        send(direction, buf, kv[tile].at[pl.ds(base(row, col), MOST)], 1, 1, end_sem.at[tile], when, hop)

    def choose_1(row, to_left, to_right, to_far, hop=None):
        @pl.when(to_left(z, y, hop) | to_right(z, y, hop) | to_far(z, y, hop))
        def _():
            code = jnp.concatenate([chooser(i, row) for i in (2, 0, 1)], axis=0)
            found = blocks(dot(code, item(1, row, y)))
            far_s[row, 1] = found[0:MOST]
            left_s[row, 1] = found[MOST:2 * MOST]
            right_s[row, 1] = found[2 * MOST:]

        send_chosen(FAR, far_s.at[row, 1], 1, row, y, to_far, hop)
        send_chosen(LEFT, left_s.at[row, 1], 1, row, y, to_left, hop)
        send_chosen(RIGHT, right_s.at[row, 1], 1, row, y, to_right, hop)

    def choose_0(row, to_left, hop=None):
        @pl.when(to_left(z, y, hop))
        def _():
            left_s[row, 0] = blocks(dot(chooser(0, row), item(0, row, y)))

        send_chosen(LEFT, left_s.at[row, 0], 0, row, y, to_left, hop)

    def choose_2(row, to_right, hop=None):
        @pl.when(to_right(z, y, hop))
        def _():
            right_s[row, 0] = blocks(dot(chooser(3, row), item(0, row, left_col)))

        send_chosen(RIGHT, right_s.at[row, 0], 0, row, left_col, to_right, hop)

    def choose_last(to_right, to_far):
        @pl.when(to_right(z, y, None))
        def _():
            code = jnp.concatenate([chooser(i, z) for i in (2, 1)], axis=0)
            found = blocks(dot(code, item(0, z, y)))
            far_s[z, 0] = found[0:MOST]
            right_s[z, 0] = found[MOST:]

        send_chosen(FAR, far_s.at[z, 0], 0, z, y, to_far)
        send_chosen(RIGHT, right_s.at[z, 0], 0, z, y, to_right)

    left_col = lax.rem(y + N_Y - 1, N_Y)
    for kind in (2, 3):
        send_whole(RIGHT, kind, z, y, lambda z, y, hop: z < last)
    for kind in (1, 0):
        send_whole(UP, kind, z, y, lambda z, y, hop: z < last)
        send_whole(DOWN, kind, z, y, lambda z, y, hop: z < back_a)

    for copy in place_copies:
        copy.wait()
    spread = jnp.where(
        iota((n_blocks, rows), 0) % nb == iota((n_blocks, rows), 1) // BLK, 1.0, 0.0).astype(BF16)
    row_owner = iota((n_z, n_blocks), 0) * N_Y
    owner_lane = iota((n_z, n_blocks), 1) // nb
    for which, (slot, col) in enumerate(((0, y), (1, y), (2, y), (1, left_col))):
        mine = jnp.where(owner_lane == row_owner + col, place_recv[slot], 0.0)
        code_s[which] = dot(mine.astype(BF16), spread)

    choose_1(z, lambda z, y, hop: y == 0, lambda z, y, hop: y < N_Y - 1, lambda z, y, hop: y < N_Y - 2)
    choose_0(z, lambda z, y, hop: y == 0)
    choose_last(
        lambda z, y, hop: (z == last) & (y < N_Y - 1), lambda z, y, hop: (z == last) & (y < N_Y - 2))

    raw = (raw_s[:, 0:q_cols] + dot(y1, w_buf[1, :, 0:q_cols])) * row_scale
    for tile in range(q_cols // LANES):
        q = head_norm(raw[:, tile * LANES:(tile + 1) * LANES], qg_row)
        turned = pltpu.roll(q, HD, 1)
        for odd in range(2):
            head = 2 * tile + odd
            side = head // group
            here = turned if odd == side else q
            here = jnp.where(low if side == 1 else ~low, here, 0.0).astype(BF16)
            for r in range(nb):
                q_s[r, head * BLK:(head + 1) * BLK] = here[r * BLK:(r + 1) * BLK]

    lane_entry = iota((nb, entries), 1)
    rank = jnp.zeros((nb, entries), jnp.int32)
    for e in range(entries):
        found = jnp.max(jnp.where(hits[e], rank_of, 0), axis=1, keepdims=True)
        rank = jnp.where(lane_entry == e, found, rank)
    owner = lists // nb
    owner_row = owner // N_Y
    col = lax.rem(owner, N_Y)
    ranked = 1 + owner * nb + rank
    for tile in range(2):
        full = col == y
        if tile == 0:
            full = full | ((col == left_col) & (owner_row != last))
        index_v[tile] = jnp.where(lists < 0, 0, jnp.where(full, 1 + lists, ranked))
    index_copy = pltpu.make_async_copy(index_v, index_s, load_sem.at[INDEX])
    index_copy.start()

    lane = iota((nb, keys), 1)
    block = jnp.full((nb, keys), -1, jnp.int32)
    for e in range(entries):
        block = jnp.where(lane // BLK == e, lists[:, e:e + 1], block)
    away = (block - (me * nb + iota((nb, keys), 0))) * BLK + lane % BLK
    kp_s[...] = jnp.where(block < 0, 1 << 24, away).astype(F32)

    for kind in (2, 3):
        arrive(kind, z, left_col, lambda z, y, hop: z < last)
        send_whole(UP, kind, z, left_col, lambda z, y, hop: z < last)
        send_whole(DOWN, kind, z, left_col, lambda z, y, hop: z < back_b)
    choose_2(z, lambda z, y, hop: (z < last) & ((y == 1) | (y == 2)))

    routes = (((1,), y, reach_a, back_a), ((0,), y, reach_a, back_a), ((2, 3), left_col, reach_b, back_b))
    hops = range(1, n_z // 2 + 1)

    def one_hop(hop, carry):
        above = lax.max(z - hop, 0)
        below = lax.rem(z + hop, n_z)
        for kinds, col, reach, back in routes:

            def from_above(z, y, hop, reach=reach):
                return (z >= hop) & (hop <= reach)

            def go_up(z, y, hop, reach=reach):
                return (z >= hop) & (hop < reach) & (z < last)

            def from_below(z, y, hop, back=back):
                return ((z + hop) % n_z < back) & (hop <= back)

            def go_down(z, y, hop, back=back):
                return ((z + hop) % n_z < back) & (hop < back)

            def use_below(z, y, hop, back=back):
                return ((z + hop) % n_z < back) & (hop <= back) & ((z + hop) % n_z < z)

            for kind in kinds:
                arrive(kind, above, col, from_above, hop)
                send_whole(UP, kind, above, col, go_up, hop)
                arrive(kind, below, col, from_below, hop)
                send_whole(DOWN, kind, below, col, go_down, hop)
            for row, use in ((above, from_above), (below, use_below)):
                if kinds == (1,):
                    choose_1(row, use, use, use, hop)
                elif kinds == (0,):
                    choose_0(row, use, hop)
                else:
                    choose_2(row, use, hop)
        return carry

    lax.fori_loop(hops.start, hops.stop, one_hop, 0)

    def settle(count, sem):
        for k in range(n_z):
            @pl.when(z == k)
            def _():
                for j in range(N_Y):
                    units = count(k, j)
                    if units:
                        @pl.when(y == j)
                        def _():
                            part = kv0.at[0:units * MOST]
                            pltpu.make_async_copy(part, part, sem).wait()

    def due(tile):
        def count(z, y):
            if tile == 1:
                return (z + (y == N_Y - 1)) + (z + (y >= 1)) + (z + (y >= 2))
            if z == last:
                return (z + (y == N_Y - 1)) + z + (y >= 1) + (y >= 2)
            return (z + (y == N_Y - 1)) + (z + (y >= 2))
        return count

    query_row = iota((BLK, keys), 0).astype(F32)
    ones = jnp.ones((keys, LANES), BF16)
    tile_low = iota((BLK, LANES), 1) < HD
    tile_lane = iota((BLK, LANES), 1)
    core_slope = jnp.where(tp == 0, 1.0, 2.0 ** (-8.0 * heads / n_heads)).astype(F32)

    def slope_of(head):
        return core_slope * (2.0 ** (-8.0 * (head + 1) / n_heads))

    def attend(r, side):
        key_pos = kp_s[pl.ds(r, 1), :]
        allowed = key_pos <= query_row
        both = jnp.concatenate([kv[side][index_s[side, r, e]] for e in range(entries)], axis=0)
        scores = dot_nt(q_s[r, side * group * BLK:(side + 1) * group * BLK], both)
        weights = []
        for t in range(group):
            bias = key_pos * (slope_of(side * group + t) * (alibi * LOG2E))
            part = jnp.exp2(scores[t * BLK:(t + 1) * BLK] + bias)
            weights.append(jnp.where(allowed, part, 0.0).astype(BF16))
        return dot(jnp.concatenate(weights, axis=0), jnp.concatenate([both, ones], axis=1))

    def combine(r, outs):
        sums = jnp.ones((BLK, LANES), F32)
        at = pl.ds(r * BLK, BLK)
        for t in range(group):
            first, second = (o[t * BLK:(t + 1) * BLK] for o in outs)
            top = jnp.where(tile_low, first[:, 0:LANES], second[:, 0:LANES])
            total = jnp.where(tile_low, first[:, LANES:], second[:, LANES:])
            att_s[at, t * LANES:(t + 1) * LANES] = (top / total).astype(BF16)
            sums = jnp.where(tile_lane == t, first[:, LANES:], sums)
            sums = jnp.where(tile_lane == t + group, second[:, LANES:], sums)
        sum_s[at] = sums

    loaded(OUT, wo_buf)
    part_rows = rows // PARTS

    def part_at(part):
        return pl.ds(part * part_rows, part_rows)

    def part_copy(part):
        at = part_at(part)
        return pltpu.make_async_remote_copy(
            part_send.at[at], part_recv.at[at], part_sem.at[0, part], part_sem.at[1, part],
            device_id={"tp": partner}, device_id_type=MESH)

    def one_part(part):
        each = nb // PARTS
        first = [attend(part * each + i, 0) for i in range(each)]
        for i in range(each):
            combine(part * each + i, (first[i], found_s[part * each + i]))
        at = part_at(part)
        part_send[at] = dot(att_s[at], wo_buf[1]).astype(BF16)
        part_copy(part).start()

    index_copy.wait()
    settle(due(1), end_sem.at[1])
    for start in range(0, nb, 4):
        second = [attend(start + i, 1) for i in range(4)]
        for i in range(4):
            found_s[start + i] = second[i]
    settle(due(0), end_sem.at[0])
    for part in range(PARTS):
        one_part(part)

    own = dot(att_s[...], wo_buf[0])
    row_in = (iota((rows, LANES), 0) % BLK).astype(F32)
    slopes = jnp.exp2(-8.0 / n_heads * (tp * heads + iota((rows, LANES), 1) + 1).astype(F32))
    logs = jnp.log(sum_s[...]) - slopes * alibi * row_in
    lt_ref[...] = logs.T[0:heads]

    def all_sent(which):
        return lambda z, y: sum(
            units for chain, units, when, looped in sent if chain == which
            for hop in (hops if looped else (0,)) if when(z, y, hop))

    for chain in range(2):
        settle(all_sent(chain), send_sem.at[chain])

    for part in range(PARTS):
        at = slice(part * part_rows, (part + 1) * part_rows)
        part_copy(part).wait()
        out_ref[at] = (own[at] + part_recv[at].astype(F32)).astype(BF16)


def write_out(mixed, log_total, mixed_out, log_out, sems):
    copies = [
        pltpu.make_async_copy(mixed, mixed_out, sems.at[0]),
        pltpu.make_async_copy(log_total, log_out, sems.at[1]),
    ]
    for copy in copies:
        copy.start()
    for copy in copies:
        copy.wait()


def shards(n_kv, tokens, norm_gain, w_query, w_key, w_value, q_gain, k_gain, w_out, chosen):
    seqs, rows, half = tokens.shape
    nb, entries = chosen.shape[1:]
    q_cols, k_cols = w_query.shape[1], w_key.shape[1]
    heads = q_cols // HD
    n_z = n_kv // N_Y
    vmem = pltpu.VMEM
    dma = pltpu.SemaphoreType.DMA
    mixed, log_total = pl.pallas_call(
        functools.partial(kernel, n_kv),
        out_shape=(vmem((rows, half), BF16), vmem((heads, rows), F32)),
        in_specs=[pl.BlockSpec(memory_space=pltpu.HBM)] * 9,
        out_specs=(pl.BlockSpec(memory_space=vmem), pl.BlockSpec(memory_space=vmem)),
        scratch_shapes=[
            vmem((2, rows, half), BF16),
            vmem((nb, entries), jnp.int32),
            vmem((rows, q_cols + 2 * k_cols), F32),
            vmem((2, half, q_cols + 2 * k_cols), BF16),
            vmem((2, q_cols, half), BF16),
            vmem((2, 1, half), F32),
            vmem((2, 1, HD), F32),
            vmem((nb, n_kv * nb), F32),
            vmem((3, nb, n_kv * nb), F32),
            vmem((4, n_z, rows), F32),
            vmem((2, nb, entries), jnp.int32),
            pltpu.SMEM((2, nb, entries), jnp.int32),
            vmem((n_z, 2, MOST, BLK, LANES), BF16),
            vmem((n_z, 2, MOST, BLK, LANES), BF16),
            vmem((n_z, 2, MOST, BLK, LANES), BF16),
            vmem((nb, heads * BLK, LANES), BF16),
            vmem((1 + n_kv * nb, BLK, LANES), BF16),
            vmem((1 + n_kv * nb, BLK, LANES), BF16),
            vmem((nb, entries * BLK), F32),
            vmem((nb, heads // 2 * BLK, 2 * LANES), F32),
            vmem((rows, q_cols), BF16),
            vmem((rows, LANES), F32),
            vmem((rows, half), BF16),
            vmem((rows, half), BF16),
            dma((8,)),
            dma((2,)),
            dma((2, 3)),
            dma((2,)),
            dma((4, n_z)),
            dma((2,)),
            dma((2, PARTS)),
        ],
        compiler_params=pltpu.CompilerParams(
            collective_id=0, has_side_effects=True, vmem_limit_bytes=66_700_000
        ),
    )(
        tokens.reshape(rows, half), norm_gain.reshape(1, -1), w_query, w_key, w_value,
        q_gain.reshape(1, -1), k_gain.reshape(1, -1), w_out, chosen.reshape(nb, entries),
    )
    mixed, log_total = pl.pallas_call(
        write_out,
        out_shape=(
            jax.ShapeDtypeStruct((rows, half), BF16),
            jax.ShapeDtypeStruct((heads, rows), F32),
        ),
        in_specs=[pl.BlockSpec(memory_space=pl.ANY)] * 2,
        out_specs=(pl.BlockSpec(memory_space=pltpu.HBM),) * 2,
        scratch_shapes=[dma((2,))],
        compiler_params=pltpu.CompilerParams(vmem_limit_bytes=1_000_000),
    )(mixed, log_total)
    return mixed.reshape(seqs, rows, half), log_total.reshape(seqs, heads, rows)


def solution(mesh):
    in_specs = (
        P("dp", "kv", "tp"),
        P(),
        P(None, "tp"),
        P(None, "tp"),
        P(None, "tp"),
        P(),
        P(),
        P("tp", None),
        P("dp", "kv", None),
    )
    out_specs = (P("dp", "kv", "tp"), P("dp", "tp", "kv"))
    return jax.shard_map(
        functools.partial(shards, mesh.shape["kv"]),
        mesh=mesh, in_specs=in_specs, out_specs=out_specs, check_vma=False)
```

```python
import functools
import math

import jax
import jax.numpy as jnp
from jax import lax
from jax.experimental import pallas as pl
from jax.experimental.pallas import tpu as pltpu
from jax.sharding import PartitionSpec as P

HD = 64
BLK = 32
LANES = 128
MOST = 4
LATE = 4
PARTS = 2
N_Y = 4
UP, DOWN, LEFT, RIGHT, FAR = range(5)

epsilon = 1e-06
alibi_reach = 4.0
LOG2E = math.log2(math.e)
F32 = jnp.float32
BF16 = jnp.bfloat16
NT = (((1,), (1,)), ((), ()))
MESH = pl.DeviceIdType.MESH


def iota(shape, dim):
    return lax.broadcasted_iota(jnp.int32, shape, dim)


def dot(a, b):
    return jnp.dot(a, b, preferred_element_type=F32)


def dot_nt(a, b):
    return lax.dot_general(a, b, NT, preferred_element_type=F32)


def kernel(
    n_kv,
    tok, gain, wq, wk, wv, qg, kg, wo, ch,
    out_ref, lt_ref,
    x_buf, ch_buf, raw_s, w_buf, wo_buf, g_buf, hg_buf,
    place_send, place_recv, code_s, index_v, index_s, left_s, right_s, far_s,
    q_s, kv0, kv1, late_s, kp_s, late_kp, found_s, att_s, sum_s, part_send, part_recv,
    load_sem, x_sem, place_sem, send_sem, stage_sem, end_sem, part_sem,
):
    me = lax.axis_index("kv")
    tp = lax.axis_index("tp")
    partner = 1 - tp
    n_z = n_kv // N_Y
    z = me // N_Y
    y = me % N_Y
    rows, half = tok.shape
    q_cols = wq.shape[1]
    k_cols = wk.shape[1]
    heads = q_cols // HD
    kv_heads = k_cols // HD
    group = heads // kv_heads
    n_heads = heads * lax.axis_size("tp")
    nb, entries = ch.shape
    n_blocks = n_kv * nb
    width = half * 2
    seq_len = rows * n_kv
    alibi = alibi_reach / seq_len
    keys = entries * BLK
    picked = MOST * BLK
    kv = (kv0, kv1)

    def device(row, col):
        return lax.rem(row + n_z, n_z) * N_Y + lax.rem(col + N_Y, N_Y)

    neighbour = {
        UP: device(z + 1, y), DOWN: device(z - 1, y),
        LEFT: device(z, y - 1), RIGHT: device(z, y + 1), FAR: device(z, y + 2),
    }
    barrier = pltpu.get_barrier_semaphore()
    pl.semaphore_signal(barrier, inc=1, device_id={"tp": partner}, device_id_type=MESH)
    for target in neighbour.values():
        pl.semaphore_signal(barrier, inc=1, device_id={"kv": target}, device_id_type=MESH)

    def span(start):
        return pl.ds(pl.multiple_of(start * half, LANES), half)

    def load(sem, *pairs):
        for src, dst in pairs:
            pltpu.make_async_copy(src, dst, load_sem.at[sem]).start()

    def loaded(sem, whole):
        pltpu.make_async_copy(whole, whole, load_sem.at[sem]).wait()

    def weights(side, which):
        return (
            (wk.at[span(which), :], w_buf.at[side, :, q_cols:q_cols + k_cols]),
            (wv.at[span(which), :], w_buf.at[side, :, q_cols + k_cols:q_cols + 2 * k_cols]),
            (wq.at[span(which), :], w_buf.at[side, :, 0:q_cols]),
        )

    TABLE, TOK, GAIN, W0, W1, HEAD_GAIN, OUT, INDEX = range(8)
    load(TOK, (tok, x_buf.at[0]))
    load(TABLE, (ch, ch_buf))
    load(GAIN, (gain.at[:, span(tp)], g_buf.at[0]), (gain.at[:, span(partner)], g_buf.at[1]))
    load(W0, *weights(0, tp))
    load(W1, *weights(1, partner))
    load(HEAD_GAIN, (qg, hg_buf.at[0]), (kg, hg_buf.at[1]))

    def scaled(side):
        x = x_buf[side].astype(F32)
        return (x * g_buf[side]).astype(BF16), jnp.sum(x * x, axis=1, keepdims=True)

    loaded(TOK, x_buf.at[0])
    pl.semaphore_wait(barrier, 1 + len(neighbour))
    x_copy = pltpu.make_async_remote_copy(
        x_buf.at[0], x_buf.at[1], x_sem.at[0], x_sem.at[1],
        device_id={"tp": partner}, device_id_type=MESH)
    x_copy.start()

    loaded(TABLE, ch_buf)
    lists = ch_buf[...]
    lane_block = iota((nb, n_blocks), 1)
    hits = [lists[:, e:e + 1] == lane_block for e in range(entries)]
    hit = hits[0]
    for e in range(1, entries):
        hit = hit | hits[e]
    need = jnp.broadcast_to(jnp.max(jnp.where(hit, 1, 0), axis=0, keepdims=True), (nb, n_blocks))
    rank_of = jnp.zeros((nb, n_blocks), jnp.int32)
    for k in range(1, nb):
        rank_of = rank_of + jnp.where(lane_block % nb >= k, pltpu.roll(need, k, 1), 0)
    place_send[...] = jnp.where(need > 0, rank_of, -1).astype(F32)

    def place_copy(direction, slot):
        return pltpu.make_async_remote_copy(
            place_send, place_recv.at[slot], place_sem.at[0, slot], place_sem.at[1, slot],
            device_id={"kv": neighbour[direction]}, device_id_type=MESH)

    place_copies = [place_copy(RIGHT, 0), place_copy(LEFT, 1), place_copy(FAR, 2)]
    for copy in place_copies:
        copy.start()

    for side, which in ((0, tp), (1, partner)):
        for head in range(heads):
            to = head % group * LANES + head // group * HD
            load(OUT, (wo.at[head * HD:(head + 1) * HD, span(which)], wo_buf.at[side, to:to + HD]))

    loaded(GAIN, g_buf)
    loaded(W0, w_buf.at[0])
    y0, sq0 = scaled(0)
    raw_s[...] = dot(y0, w_buf[0])

    same_head = jnp.where(
        iota((LANES, LANES), 0) // HD == iota((LANES, LANES), 1) // HD, 1.0, 0.0).astype(BF16)

    def head_norm(v, gain_row):
        sq = v * v
        hi = sq.astype(BF16)
        lo = (sq - hi.astype(F32)).astype(BF16)
        total = dot(hi, same_head) + dot(lo, same_head)
        return v * lax.rsqrt(total / HD + epsilon) * gain_row

    loaded(HEAD_GAIN, hg_buf)
    loaded(W1, w_buf.at[1])
    qg_row = jnp.concatenate([hg_buf[0], hg_buf[0]], axis=1) * (HD ** -0.5 * LOG2E)
    kg_row = jnp.concatenate([hg_buf[1], hg_buf[1]], axis=1)
    low = iota((rows, LANES), 1) < HD
    x_copy.wait()
    y1, sq1 = scaled(1)
    row_scale = lax.rsqrt((sq0 + sq1) / width + epsilon)
    raw_kv = (raw_s[:, q_cols:] + dot(y1, w_buf[1, :, q_cols:])) * row_scale
    key_part = pltpu.roll(head_norm(raw_kv[:, 0:k_cols], kg_row), HD, 1)
    value_part = raw_kv[:, k_cols:]

    def base(row, col):
        return 1 + (row * N_Y + col) * nb

    own_tiles = (jnp.where(low, value_part, key_part), jnp.where(low, key_part, value_part))
    for tile in range(2):
        kv[tile][0] = jnp.zeros((BLK, LANES), BF16)
        kv[tile][pl.ds(base(z, y), nb)] = own_tiles[tile].astype(BF16).reshape(nb, BLK, LANES)

    last = n_z - 1
    reach_a, reach_b = n_z // 2, n_z // 2 - 1
    back_a, back_b = last - reach_a, last - reach_b
    assert LATE == reach_a == back_b

    @pl.when(z < LATE)
    def _():
        late_s[...] = jnp.zeros(late_s.shape, BF16)

    sent = []

    def send(direction, src, dst, chain, units, arrival, when, hop=None):
        sent.append((chain, units, when, hop is not None))

        @pl.when(when(z, y, hop))
        def _():
            pltpu.make_async_remote_copy(
                src, dst, send_sem.at[chain], arrival,
                device_id={"kv": neighbour[direction]}, device_id_type=MESH).start()

    def stage(kind, row):
        return stage_sem.at[kind, row]

    def whole(kind, row, col):
        if kind < 2:
            return kv[kind].at[pl.ds(base(row, col), nb)]
        return kv0.at[pl.ds(base(row, col) + (kind - 2) * (nb // 2), nb // 2)]

    def send_whole(direction, kind, row, col, when, hop=None):
        part = whole(kind, row, col)
        send(direction, part, part, 0, 2 if kind < 2 else 1, stage(kind, row), when, hop)

    def arrive(kind, row, col, when, hop=None):
        @pl.when(when(z, y, hop))
        def _():
            part = whole(kind, row, col)
            pltpu.make_async_remote_copy(
                part, part, send_sem.at[0], stage(kind, row),
                device_id={"kv": neighbour[UP]}, device_id_type=MESH).wait_recv()

    same_row = iota((picked, rows), 0) % BLK == iota((picked, rows), 1) % BLK
    row_slot = (iota((picked, rows), 0) // BLK).astype(F32)

    def chooser(which, row):
        code = code_s[which, pl.ds(row, 1), :]
        return jnp.where(same_row & (code == row_slot), 1.0, 0.0).astype(BF16)

    def item(tile, row, col):
        return kv[tile][pl.ds(base(row, col), nb)].reshape(rows, LANES)

    def blocks(x):
        return x.astype(BF16).reshape(-1, BLK, LANES)

    def send_chosen(direction, buf, tile, row, col, when, hop=None):
        send(direction, buf, kv[tile].at[pl.ds(base(row, col), MOST)], 1, 1, end_sem.at[tile], when, hop)

    def choose_1(row, to_left, to_right, to_far, hop=None):
        @pl.when(to_left(z, y, hop) | to_right(z, y, hop) | to_far(z, y, hop))
        def _():
            code = jnp.concatenate([chooser(i, row) for i in (2, 0, 1)], axis=0)
            found = blocks(dot(code, item(1, row, y)))
            far_s[row, 1] = found[0:MOST]
            left_s[row, 1] = found[MOST:2 * MOST]
            right_s[row, 1] = found[2 * MOST:]

        send_chosen(FAR, far_s.at[row, 1], 1, row, y, to_far, hop)
        send_chosen(LEFT, left_s.at[row, 1], 1, row, y, to_left, hop)
        send_chosen(RIGHT, right_s.at[row, 1], 1, row, y, to_right, hop)

    def send_tile_0(direction, buf, slot, row, col, when, hop):
        if hop is None:
            send_chosen(direction, buf, 0, row, col, when)
            return
        send_chosen(direction, buf, 0, row, col, lambda z, y, hop: when(z, y, hop) & (hop < LATE), hop)
        send(direction, buf, late_s.at[slot], 1, 1, end_sem.at[2],
             lambda z, y, hop: when(z, y, hop) & (hop == LATE), hop)

    def choose_0(row, to_left, hop=None):
        @pl.when(to_left(z, y, hop))
        def _():
            left_s[row, 0] = blocks(dot(chooser(0, row), item(0, row, y)))

        send_tile_0(LEFT, left_s.at[row, 0], 0, row, y, to_left, hop)

    def choose_2(row, to_right, hop=None):
        @pl.when(to_right(z, y, hop))
        def _():
            right_s[row, 0] = blocks(dot(chooser(3, row), item(0, row, left_col)))

        send_tile_0(RIGHT, right_s.at[row, 0], 1, row, left_col, to_right, hop)

    def choose_last(to_right, to_far):
        @pl.when(to_right(z, y, None))
        def _():
            code = jnp.concatenate([chooser(i, z) for i in (2, 1)], axis=0)
            found = blocks(dot(code, item(0, z, y)))
            far_s[z, 0] = found[0:MOST]
            right_s[z, 0] = found[MOST:]

        send_chosen(FAR, far_s.at[z, 0], 0, z, y, to_far)
        send_chosen(RIGHT, right_s.at[z, 0], 0, z, y, to_right)

    left_col = lax.rem(y + N_Y - 1, N_Y)
    for kind in (2, 3):
        send_whole(RIGHT, kind, z, y, lambda z, y, hop: z < last)
    for kind in (1, 0):
        send_whole(UP, kind, z, y, lambda z, y, hop: z < last)
        send_whole(DOWN, kind, z, y, lambda z, y, hop: z < back_a)

    for copy in place_copies:
        copy.wait()
    spread = jnp.where(
        iota((n_blocks, rows), 0) % nb == iota((n_blocks, rows), 1) // BLK, 1.0, 0.0).astype(BF16)
    row_owner = iota((n_z, n_blocks), 0) * N_Y
    owner_lane = iota((n_z, n_blocks), 1) // nb
    for which, (slot, col) in enumerate(((0, y), (1, y), (2, y), (1, left_col))):
        mine = jnp.where(owner_lane == row_owner + col, place_recv[slot], 0.0)
        code_s[which] = dot(mine.astype(BF16), spread)

    choose_1(z, lambda z, y, hop: y == 0, lambda z, y, hop: y < N_Y - 1, lambda z, y, hop: y < N_Y - 2)
    choose_0(z, lambda z, y, hop: y == 0)
    choose_last(
        lambda z, y, hop: (z == last) & (y < N_Y - 1), lambda z, y, hop: (z == last) & (y < N_Y - 2))

    raw = (raw_s[:, 0:q_cols] + dot(y1, w_buf[1, :, 0:q_cols])) * row_scale
    for tile in range(q_cols // LANES):
        q = head_norm(raw[:, tile * LANES:(tile + 1) * LANES], qg_row)
        turned = pltpu.roll(q, HD, 1)
        for odd in range(2):
            head = 2 * tile + odd
            side = head // group
            here = turned if odd == side else q
            here = jnp.where(low if side == 1 else ~low, here, 0.0).astype(BF16)
            for r in range(nb):
                q_s[r, head * BLK:(head + 1) * BLK] = here[r * BLK:(r + 1) * BLK]

    lane_entry = iota((nb, entries), 1)
    rank = jnp.zeros((nb, entries), jnp.int32)
    for e in range(entries):
        found = jnp.max(jnp.where(hits[e], rank_of, 0), axis=1, keepdims=True)
        rank = jnp.where(lane_entry == e, found, rank)
    owner = lists // nb
    owner_row = owner // N_Y
    col = lax.rem(owner, N_Y)
    ranked = 1 + owner * nb + rank
    late_owners = [
        jnp.where(z >= LATE, (z - LATE) * N_Y + lax.rem(y + step, N_Y), -2) for step in (1, 2)]
    for tile in range(2):
        full = col == y
        if tile == 0:
            full = full | ((col == left_col) & (owner_row != last))
        empty = lists < 0
        if tile == 0:
            empty = empty | (owner == late_owners[0]) | (owner == late_owners[1])
        index_v[tile] = jnp.where(empty, 0, jnp.where(full, 1 + lists, ranked))
    index_copy = pltpu.make_async_copy(index_v, index_s, load_sem.at[INDEX])
    index_copy.start()

    lane = iota((nb, keys), 1)
    block = jnp.full((nb, keys), -1, jnp.int32)
    for e in range(entries):
        block = jnp.where(lane // BLK == e, lists[:, e:e + 1], block)
    block_owner = block // nb
    late = (block_owner == late_owners[0]) | (block_owner == late_owners[1])

    def positions(block, lane, hide):
        away = (block - (me * nb + iota(block.shape, 0))) * BLK + lane % BLK
        return jnp.where(hide, 1 << 24, away).astype(F32)

    kp_s[0] = positions(block, lane, (block < 0) | late)
    kp_s[1] = positions(block, lane, block < 0)
    lane = iota((nb, 2 * picked), 1)
    late_owner = jnp.where(lane < picked, late_owners[0], late_owners[1])
    block = jnp.full((nb, 2 * picked), -1, jnp.int32)
    for e in range(entries):
        here = (owner[:, e:e + 1] == late_owner) & (rank[:, e:e + 1] == lane // BLK % MOST)
        block = jnp.where(here, lists[:, e:e + 1], block)
    late_kp[...] = positions(block, lane, block < 0)

    for kind in (2, 3):
        arrive(kind, z, left_col, lambda z, y, hop: z < last)
        send_whole(UP, kind, z, left_col, lambda z, y, hop: z < last)
        send_whole(DOWN, kind, z, left_col, lambda z, y, hop: z < back_b)
    choose_2(z, lambda z, y, hop: (z < last) & ((y == 1) | (y == 2)))

    routes = (((1,), y, reach_a, back_a), ((0,), y, reach_a, back_a), ((2, 3), left_col, reach_b, back_b))
    hops = range(1, n_z // 2 + 1)

    def one_hop(hop, carry):
        above = lax.max(z - hop, 0)
        below = lax.rem(z + hop, n_z)
        for kinds, col, reach, back in routes:

            def from_above(z, y, hop, reach=reach):
                return (z >= hop) & (hop <= reach)

            def go_up(z, y, hop, reach=reach):
                return (z >= hop) & (hop < reach) & (z < last)

            def from_below(z, y, hop, back=back):
                return ((z + hop) % n_z < back) & (hop <= back)

            def go_down(z, y, hop, back=back):
                return ((z + hop) % n_z < back) & (hop < back)

            def use_below(z, y, hop, back=back):
                return ((z + hop) % n_z < back) & (hop <= back) & ((z + hop) % n_z < z)

            for kind in kinds:
                arrive(kind, above, col, from_above, hop)
                send_whole(UP, kind, above, col, go_up, hop)
                arrive(kind, below, col, from_below, hop)
                send_whole(DOWN, kind, below, col, go_down, hop)
            for row, use in ((above, from_above), (below, use_below)):
                if kinds == (1,):
                    choose_1(row, use, use, use, hop)
                elif kinds == (0,):
                    choose_0(row, use, hop)
                else:
                    choose_2(row, use, hop)
        return carry

    lax.fori_loop(hops.start, hops.stop, one_hop, 0)

    def settle(count, sem):
        for k in range(n_z):
            @pl.when(z == k)
            def _():
                for j in range(N_Y):
                    units = count(k, j)
                    if units:
                        @pl.when(y == j)
                        def _():
                            part = kv0.at[0:units * MOST]
                            pltpu.make_async_copy(part, part, sem).wait()

    def due(tile):
        def count(z, y):
            if tile == 1:
                return (z + (y == N_Y - 1)) + (z + (y >= 1)) + (z + (y >= 2))
            later = 2 if z >= LATE else 0
            if tile == 2:
                return later
            if z == last:
                return (z + (y == N_Y - 1)) + z + (y >= 1) + (y >= 2) - later
            return (z + (y == N_Y - 1)) + (z + (y >= 2)) - later
        return count

    tile_low = iota((BLK, LANES), 1) < HD
    tile_lane = iota((BLK, LANES), 1)
    core_slope = jnp.where(tp == 0, 1.0, 2.0 ** (-8.0 * heads / n_heads)).astype(F32)

    def slope_of(head):
        return core_slope * (2.0 ** (-8.0 * (head + 1) / n_heads))

    def attend(r, side, both, key_pos):
        count = both.shape[0]
        allowed = key_pos <= iota((BLK, count), 0).astype(F32)
        scores = dot_nt(q_s[r, side * group * BLK:(side + 1) * group * BLK], both)
        weights = []
        for t in range(group):
            bias = key_pos * (slope_of(side * group + t) * (alibi * LOG2E))
            part = jnp.exp2(scores[t * BLK:(t + 1) * BLK] + bias)
            weights.append(jnp.where(allowed, part, 0.0).astype(BF16))
        ones = jnp.ones((count, LANES), BF16)
        return dot(jnp.concatenate(weights, axis=0), jnp.concatenate([both, ones], axis=1))

    def attend_chosen(side):
        for start in range(0, nb, 4):
            found = []
            for r in range(start, start + 4):
                both = jnp.concatenate([kv[side][index_s[side, r, e]] for e in range(entries)], axis=0)
                found.append(attend(r, side, both, kp_s[side, r:r + 1, :]))
            for i in range(4):
                found_s[side, start + i] = found[i]

    def attend_late(r):
        return attend(r, 0, late_s[...].reshape(2 * picked, LANES), late_kp[r:r + 1, :])

    def combine(r, outs):
        sums = jnp.ones((BLK, LANES), F32)
        at = pl.ds(r * BLK, BLK)
        for t in range(group):
            first, second = (o[t * BLK:(t + 1) * BLK] for o in outs)
            top = jnp.where(tile_low, first[:, 0:LANES], second[:, 0:LANES])
            total = jnp.where(tile_low, first[:, LANES:], second[:, LANES:])
            att_s[at, t * LANES:(t + 1) * LANES] = (top / total).astype(BF16)
            sums = jnp.where(tile_lane == t, first[:, LANES:], sums)
            sums = jnp.where(tile_lane == t + group, second[:, LANES:], sums)
        sum_s[at] = sums

    loaded(OUT, wo_buf)
    part_rows = rows // PARTS

    def part_at(part):
        return pl.ds(part * part_rows, part_rows)

    def part_copy(part):
        at = part_at(part)
        return pltpu.make_async_remote_copy(
            part_send.at[at], part_recv.at[at], part_sem.at[0, part], part_sem.at[1, part],
            device_id={"tp": partner}, device_id_type=MESH)

    def one_part(part):
        each = nb // PARTS
        rest = [attend_late(part * each + i) for i in range(each)]
        for i in range(each):
            r = part * each + i
            combine(r, (found_s[0, r] + rest[i], found_s[1, r]))
        at = part_at(part)
        part_send[at] = dot(att_s[at], wo_buf[1]).astype(BF16)
        part_copy(part).start()

    index_copy.wait()
    settle(due(0), end_sem.at[0])
    attend_chosen(0)
    settle(due(1), end_sem.at[1])
    attend_chosen(1)
    settle(due(2), end_sem.at[2])
    for part in range(PARTS):
        one_part(part)

    own = dot(att_s[...], wo_buf[0])
    row_in = (iota((rows, LANES), 0) % BLK).astype(F32)
    slopes = jnp.exp2(-8.0 / n_heads * (tp * heads + iota((rows, LANES), 1) + 1).astype(F32))
    logs = jnp.log(sum_s[...]) - slopes * alibi * row_in
    lt_ref[...] = logs.T[0:heads]

    def all_sent(which):
        return lambda z, y: sum(
            units for chain, units, when, looped in sent if chain == which
            for hop in (hops if looped else (0,)) if when(z, y, hop))

    for chain in range(2):
        settle(all_sent(chain), send_sem.at[chain])

    for part in range(PARTS):
        at = slice(part * part_rows, (part + 1) * part_rows)
        part_copy(part).wait()
        out_ref[at] = (own[at] + part_recv[at].astype(F32)).astype(BF16)


def write_out(mixed, log_total, mixed_out, log_out, sems):
    copies = [
        pltpu.make_async_copy(mixed, mixed_out, sems.at[0]),
        pltpu.make_async_copy(log_total, log_out, sems.at[1]),
    ]
    for copy in copies:
        copy.start()
    for copy in copies:
        copy.wait()


def shards(n_kv, tokens, norm_gain, w_query, w_key, w_value, q_gain, k_gain, w_out, chosen):
    seqs, rows, half = tokens.shape
    nb, entries = chosen.shape[1:]
    q_cols, k_cols = w_query.shape[1], w_key.shape[1]
    heads = q_cols // HD
    n_z = n_kv // N_Y
    vmem = pltpu.VMEM
    dma = pltpu.SemaphoreType.DMA
    mixed, log_total = pl.pallas_call(
        functools.partial(kernel, n_kv),
        out_shape=(vmem((rows, half), BF16), vmem((heads, rows), F32)),
        in_specs=[pl.BlockSpec(memory_space=pltpu.HBM)] * 9,
        out_specs=(pl.BlockSpec(memory_space=vmem), pl.BlockSpec(memory_space=vmem)),
        scratch_shapes=[
            vmem((2, rows, half), BF16),
            vmem((nb, entries), jnp.int32),
            vmem((rows, q_cols + 2 * k_cols), F32),
            vmem((2, half, q_cols + 2 * k_cols), BF16),
            vmem((2, q_cols, half), BF16),
            vmem((2, 1, half), F32),
            vmem((2, 1, HD), F32),
            vmem((nb, n_kv * nb), F32),
            vmem((3, nb, n_kv * nb), F32),
            vmem((4, n_z, rows), F32),
            vmem((2, nb, entries), jnp.int32),
            pltpu.SMEM((2, nb, entries), jnp.int32),
            vmem((n_z, 2, MOST, BLK, LANES), BF16),
            vmem((n_z, 2, MOST, BLK, LANES), BF16),
            vmem((n_z, 2, MOST, BLK, LANES), BF16),
            vmem((nb, heads * BLK, LANES), BF16),
            vmem((1 + n_kv * nb, BLK, LANES), BF16),
            vmem((1 + n_kv * nb, BLK, LANES), BF16),
            vmem((2, MOST, BLK, LANES), BF16),
            vmem((2, nb, entries * BLK), F32),
            vmem((nb, 2 * MOST * BLK), F32),
            vmem((2, nb, heads // 2 * BLK, 2 * LANES), F32),
            vmem((rows, q_cols), BF16),
            vmem((rows, LANES), F32),
            vmem((rows, half), BF16),
            vmem((rows, half), BF16),
            dma((8,)),
            dma((2,)),
            dma((2, 3)),
            dma((2,)),
            dma((4, n_z)),
            dma((3,)),
            dma((2, PARTS)),
        ],
        compiler_params=pltpu.CompilerParams(
            collective_id=0, has_side_effects=True, vmem_limit_bytes=66_700_000
        ),
    )(
        tokens.reshape(rows, half), norm_gain.reshape(1, -1), w_query, w_key, w_value,
        q_gain.reshape(1, -1), k_gain.reshape(1, -1), w_out, chosen.reshape(nb, entries),
    )
    mixed, log_total = pl.pallas_call(
        write_out,
        out_shape=(
            jax.ShapeDtypeStruct((rows, half), BF16),
            jax.ShapeDtypeStruct((heads, rows), F32),
        ),
        in_specs=[pl.BlockSpec(memory_space=pl.ANY)] * 2,
        out_specs=(pl.BlockSpec(memory_space=pltpu.HBM),) * 2,
        scratch_shapes=[dma((2,))],
        compiler_params=pltpu.CompilerParams(vmem_limit_bytes=1_000_000),
    )(mixed, log_total)
    return mixed.reshape(seqs, rows, half), log_total.reshape(seqs, heads, rows)


def solution(mesh):
    in_specs = (
        P("dp", "kv", "tp"),
        P(),
        P(None, "tp"),
        P(None, "tp"),
        P(None, "tp"),
        P(),
        P(),
        P("tp", None),
        P("dp", "kv", None),
    )
    out_specs = (P("dp", "kv", "tp"), P("dp", "tp", "kv"))
    return jax.shard_map(
        functools.partial(shards, mesh.shape["kv"]),
        mesh=mesh, in_specs=in_specs, out_specs=out_specs, check_vma=False)
```

```python
import functools
import math

import jax
import jax.numpy as jnp
from jax import lax
from jax.experimental import pallas as pl
from jax.experimental.pallas import tpu as pltpu
from jax.sharding import PartitionSpec as P

HD = 64
BLK = 32
LANES = 128
MOST = 4
PARTS = 2
N_Y = 4
UP, DOWN, LEFT, RIGHT, FAR = range(5)

epsilon = 1e-06
alibi_reach = 4.0
LOG2E = math.log2(math.e)
F32 = jnp.float32
BF16 = jnp.bfloat16
NT = (((1,), (1,)), ((), ()))
MESH = pl.DeviceIdType.MESH


def iota(shape, dim):
    return lax.broadcasted_iota(jnp.int32, shape, dim)


def dot(a, b):
    return jnp.dot(a, b, preferred_element_type=F32)


def dot_nt(a, b):
    return lax.dot_general(a, b, NT, preferred_element_type=F32)


def kernel(
    n_kv,
    tok, gain, wq, wk, wv, qg, kg, wo, ch,
    out_ref, lt_ref,
    x_buf, ch_buf, raw_s, w_buf, wo_buf, g_buf, hg_buf,
    place_send, place_recv, code_s, hot_s, index_v, index_s, left_s, right_s, far_s,
    q_s, kv0, kv1, kp_s, found_s, att_s, sum_s, part_send, part_recv,
    load_sem, x_sem, place_sem, send_sem, stage_sem, end_sem, part_sem,
):
    me = lax.axis_index("kv")
    tp = lax.axis_index("tp")
    partner = 1 - tp
    n_z = n_kv // N_Y
    z = me // N_Y
    y = me % N_Y
    rows, half = tok.shape
    q_cols = wq.shape[1]
    k_cols = wk.shape[1]
    heads = q_cols // HD
    kv_heads = k_cols // HD
    group = heads // kv_heads
    n_heads = heads * lax.axis_size("tp")
    nb, entries = ch.shape
    n_blocks = n_kv * nb
    width = half * 2
    seq_len = rows * n_kv
    alibi = alibi_reach / seq_len
    keys = entries * BLK
    picked = MOST * BLK
    kv = (kv0, kv1)

    def device(row, col):
        return lax.rem(row + n_z, n_z) * N_Y + lax.rem(col + N_Y, N_Y)

    neighbour = {
        UP: device(z + 1, y), DOWN: device(z - 1, y),
        LEFT: device(z, y - 1), RIGHT: device(z, y + 1), FAR: device(z, y + 2),
    }
    barrier = pltpu.get_barrier_semaphore()
    pl.semaphore_signal(barrier, inc=1, device_id={"tp": partner}, device_id_type=MESH)
    for target in neighbour.values():
        pl.semaphore_signal(barrier, inc=1, device_id={"kv": target}, device_id_type=MESH)

    def span(start):
        return pl.ds(pl.multiple_of(start * half, LANES), half)

    def load(sem, *pairs):
        for src, dst in pairs:
            pltpu.make_async_copy(src, dst, load_sem.at[sem]).start()

    def loaded(sem, whole):
        pltpu.make_async_copy(whole, whole, load_sem.at[sem]).wait()

    def weights(side, which):
        return (
            (wk.at[span(which), :], w_buf.at[side, :, q_cols:q_cols + k_cols]),
            (wv.at[span(which), :], w_buf.at[side, :, q_cols + k_cols:q_cols + 2 * k_cols]),
            (wq.at[span(which), :], w_buf.at[side, :, 0:q_cols]),
        )

    TABLE, TOK, GAIN, W0, W1, HEAD_GAIN, OUT, INDEX = range(8)
    load(TOK, (tok, x_buf.at[0]))
    load(TABLE, (ch, ch_buf))
    load(GAIN, (gain.at[:, span(tp)], g_buf.at[0]), (gain.at[:, span(partner)], g_buf.at[1]))
    load(W0, *weights(0, tp))
    load(W1, *weights(1, partner))
    load(HEAD_GAIN, (qg, hg_buf.at[0]), (kg, hg_buf.at[1]))

    def scaled(side):
        x = x_buf[side].astype(F32)
        return (x * g_buf[side]).astype(BF16), jnp.sum(x * x, axis=1, keepdims=True)

    loaded(TOK, x_buf.at[0])
    pl.semaphore_wait(barrier, 1 + len(neighbour))
    x_copy = pltpu.make_async_remote_copy(
        x_buf.at[0], x_buf.at[1], x_sem.at[0], x_sem.at[1],
        device_id={"tp": partner}, device_id_type=MESH)
    x_copy.start()

    loaded(TABLE, ch_buf)
    lists = ch_buf[...]
    lane_block = iota((nb, n_blocks), 1)
    hits = [lists[:, e:e + 1] == lane_block for e in range(entries)]
    hit = hits[0]
    for e in range(1, entries):
        hit = hit | hits[e]
    need = jnp.broadcast_to(jnp.max(jnp.where(hit, 1, 0), axis=0, keepdims=True), (nb, n_blocks))
    rank_of = jnp.zeros((nb, n_blocks), jnp.int32)
    for k in range(1, nb):
        rank_of = rank_of + jnp.where(lane_block % nb >= k, pltpu.roll(need, k, 1), 0)
    place_send[...] = jnp.where(need > 0, rank_of, -1).astype(F32)

    def place_copy(direction, slot):
        return pltpu.make_async_remote_copy(
            place_send, place_recv.at[slot], place_sem.at[0], place_sem.at[1],
            device_id={"kv": neighbour[direction]}, device_id_type=MESH)

    place_copies = [place_copy(RIGHT, 0), place_copy(LEFT, 1), place_copy(FAR, 2)]
    for copy in place_copies:
        copy.start()


    loaded(GAIN, g_buf)
    loaded(W0, w_buf.at[0])
    y0, sq0 = scaled(0)
    raw_s[...] = dot(y0, w_buf[0])

    same_head = jnp.where(
        iota((LANES, LANES), 0) // HD == iota((LANES, LANES), 1) // HD, 1.0, 0.0).astype(BF16)

    def head_norm(v, gain_row):
        sq = v * v
        hi = sq.astype(BF16)
        lo = (sq - hi.astype(F32)).astype(BF16)
        total = dot(hi, same_head) + dot(lo, same_head)
        return v * lax.rsqrt(total / HD + epsilon) * gain_row

    loaded(HEAD_GAIN, hg_buf)
    loaded(W1, w_buf.at[1])
    qg_row = jnp.concatenate([hg_buf[0], hg_buf[0]], axis=1) * (HD ** -0.5 * LOG2E)
    kg_row = jnp.concatenate([hg_buf[1], hg_buf[1]], axis=1)
    low = iota((rows, LANES), 1) < HD
    x_copy.wait()
    y1, sq1 = scaled(1)
    row_scale = lax.rsqrt((sq0 + sq1) / width + epsilon)
    raw_kv = (raw_s[:, q_cols:] + dot(y1, w_buf[1, :, q_cols:])) * row_scale
    key_part = pltpu.roll(head_norm(raw_kv[:, 0:k_cols], kg_row), HD, 1)
    value_part = raw_kv[:, k_cols:]

    def base(row, col):
        return 1 + (row * N_Y + col) * nb

    own_tiles = (jnp.where(low, value_part, key_part), jnp.where(low, key_part, value_part))
    for tile in range(2):
        kv[tile][0] = jnp.zeros((BLK, LANES), BF16)
        kv[tile][pl.ds(base(z, y), nb)] = own_tiles[tile].astype(BF16).reshape(nb, BLK, LANES)

    last = n_z - 1
    reach_a, reach_b = n_z // 2, n_z // 2 - 1
    back_a, back_b = last - reach_a, last - reach_b
    sent = []

    def send(direction, src, dst, chain, units, arrival, when, hop=None):
        sent.append((chain, units, when, hop is not None))

        @pl.when(when(z, y, hop))
        def _():
            pltpu.make_async_remote_copy(
                src, dst, send_sem.at[chain], arrival,
                device_id={"kv": neighbour[direction]}, device_id_type=MESH).start()

    def stage(kind, row):
        return stage_sem.at[kind, row]

    def whole(kind, row, col):
        if kind < 2:
            return kv[kind].at[pl.ds(base(row, col), nb)]
        return kv0.at[pl.ds(base(row, col) + (kind - 2) * (nb // 2), nb // 2)]

    def send_whole(direction, kind, row, col, when, hop=None):
        part = whole(kind, row, col)
        send(direction, part, part, 0, 2 if kind < 2 else 1, stage(kind, row), when, hop)

    def arrive(kind, row, col, when, hop=None):
        @pl.when(when(z, y, hop))
        def _():
            part = whole(kind, row, col)
            pltpu.make_async_remote_copy(
                part, part, send_sem.at[0], stage(kind, row),
                device_id={"kv": neighbour[UP]}, device_id_type=MESH).wait_recv()

    same_row = iota((picked, rows), 0) % BLK == iota((picked, rows), 1) % BLK
    row_slot = (iota((picked, rows), 0) // BLK).astype(F32)

    def chooser(which, row):
        code = code_s[which, pl.ds(row, 1), :]
        return jnp.where(same_row & (code == row_slot), 1.0, 0.0).astype(BF16)

    def item(tile, row, col):
        return kv[tile][pl.ds(base(row, col), nb)].reshape(rows, LANES)

    def blocks(x):
        return x.astype(BF16).reshape(-1, BLK, LANES)

    def send_chosen(direction, buf, tile, row, col, when, hop=None):
        send(direction, buf, kv[tile].at[pl.ds(base(row, col), MOST)], 1, 1, end_sem.at[tile], when, hop)

    def prepare(side, row):
        for i in range(4):
            hot_s[side, i] = chooser((2, 0, 1, 3)[i], row)

    def choose_1(row, to_left, to_right, to_far, hop=None, side=None):
        @pl.when(to_left(z, y, hop) | to_right(z, y, hop) | to_far(z, y, hop))
        def _():
            if side is None:
                code = jnp.concatenate([chooser(i, row) for i in (2, 0, 1)], axis=0)
            else:
                code = hot_s[side, 0:3].reshape(3 * picked, rows)
            found = blocks(dot(code, item(1, row, y)))
            far_s[row, 1] = found[0:MOST]
            left_s[row, 1] = found[MOST:2 * MOST]
            right_s[row, 1] = found[2 * MOST:]

        send_chosen(LEFT, left_s.at[row, 1], 1, row, y, to_left, hop)
        send_chosen(RIGHT, right_s.at[row, 1], 1, row, y, to_right, hop)
        send_chosen(FAR, far_s.at[row, 1], 1, row, y, to_far, hop)

    def choose_0(row, to_left, hop=None, side=None):
        @pl.when(to_left(z, y, hop))
        def _():
            left_s[row, 0] = blocks(dot(chooser(0, row) if side is None else hot_s[side, 1], item(0, row, y)))

        send_chosen(LEFT, left_s.at[row, 0], 0, row, y, to_left, hop)

    def choose_2(row, to_right, hop=None, side=None):
        @pl.when(to_right(z, y, hop))
        def _():
            right_s[row, 0] = blocks(dot(chooser(3, row) if side is None else hot_s[side, 3], item(0, row, left_col)))

        send_chosen(RIGHT, right_s.at[row, 0], 0, row, left_col, to_right, hop)

    def choose_last(to_right, to_far):
        @pl.when(to_right(z, y, None))
        def _():
            code = jnp.concatenate([chooser(i, z) for i in (2, 1)], axis=0)
            found = blocks(dot(code, item(0, z, y)))
            far_s[z, 0] = found[0:MOST]
            right_s[z, 0] = found[MOST:]

        send_chosen(FAR, far_s.at[z, 0], 0, z, y, to_far)
        send_chosen(RIGHT, right_s.at[z, 0], 0, z, y, to_right)

    left_col = lax.rem(y + N_Y - 1, N_Y)
    for kind in (2, 3):
        send_whole(RIGHT, kind, z, y, lambda z, y, hop: z < last)
    for kind in (1, 0):
        send_whole(UP, kind, z, y, lambda z, y, hop: z < last)
        send_whole(DOWN, kind, z, y, lambda z, y, hop: z < back_a)

    for side, which in ((0, tp), (1, partner)):
        for head in range(heads):
            to = head % group * LANES + head // group * HD
            load(OUT, (wo.at[head * HD:(head + 1) * HD, span(which)], wo_buf.at[side, to:to + HD]))

    for sem in range(2):
        pltpu.make_async_copy(place_recv, place_recv, place_sem.at[sem]).wait()
    spread = jnp.where(
        iota((n_blocks, rows), 0) % nb == iota((n_blocks, rows), 1) // BLK, 1.0, 0.0).astype(BF16)
    row_owner = iota((n_z, n_blocks), 0) * N_Y
    owner_lane = iota((n_z, n_blocks), 1) // nb
    for which, (slot, col) in enumerate(((0, y), (1, y), (2, y), (1, left_col))):
        mine = jnp.where(owner_lane == row_owner + col, place_recv[slot], 0.0)
        code_s[which] = dot(mine.astype(BF16), spread)

    choose_1(z, lambda z, y, hop: y == 0, lambda z, y, hop: y < N_Y - 1, lambda z, y, hop: y < N_Y - 2)
    choose_0(z, lambda z, y, hop: y == 0)
    choose_last(
        lambda z, y, hop: (z == last) & (y < N_Y - 1), lambda z, y, hop: (z == last) & (y < N_Y - 2))

    raw = (raw_s[:, 0:q_cols] + dot(y1, w_buf[1, :, 0:q_cols])) * row_scale
    for tile in range(q_cols // LANES):
        q = head_norm(raw[:, tile * LANES:(tile + 1) * LANES], qg_row)
        turned = pltpu.roll(q, HD, 1)
        for odd in range(2):
            head = 2 * tile + odd
            side = head // group
            here = turned if odd == side else q
            here = jnp.where(low if side == 1 else ~low, here, 0.0).astype(BF16)
            for r in range(nb):
                q_s[r, head * BLK:(head + 1) * BLK] = here[r * BLK:(r + 1) * BLK]

    lane_entry = iota((nb, entries), 1)
    rank = jnp.zeros((nb, entries), jnp.int32)
    for e in range(entries):
        found = jnp.max(jnp.where(hits[e], rank_of, 0), axis=1, keepdims=True)
        rank = jnp.where(lane_entry == e, found, rank)
    owner = lists // nb
    owner_row = owner // N_Y
    col = lax.rem(owner, N_Y)
    ranked = 1 + owner * nb + rank
    for tile in range(2):
        full = col == y
        if tile == 0:
            full = full | ((col == left_col) & (owner_row != last))
        index_v[tile] = jnp.where(lists < 0, 0, jnp.where(full, 1 + lists, ranked))
    index_copy = pltpu.make_async_copy(index_v, index_s, load_sem.at[INDEX])
    index_copy.start()

    lane = iota((nb, keys), 1)
    block = jnp.full((nb, keys), -1, jnp.int32)
    for e in range(entries):
        block = jnp.where(lane // BLK == e, lists[:, e:e + 1], block)
    away = (block - (me * nb + iota((nb, keys), 0))) * BLK + lane % BLK
    kp_s[...] = jnp.where(block < 0, 1 << 24, away).astype(F32)

    for kind in (2, 3):
        arrive(kind, z, left_col, lambda z, y, hop: z < last)
        send_whole(UP, kind, z, left_col, lambda z, y, hop: z < last)
        send_whole(DOWN, kind, z, left_col, lambda z, y, hop: z < back_b)
    choose_2(z, lambda z, y, hop: (z < last) & ((y == 1) | (y == 2)))

    routes = (((1,), y, reach_a, back_a), ((0,), y, reach_a, back_a), ((2, 3), left_col, reach_b, back_b))
    hops = range(1, n_z // 2 + 1)

    def one_hop(hop, carry):
        above = lax.max(z - hop, 0)
        below = lax.rem(z + hop, n_z)

        @pl.when(z >= hop)
        def _():
            prepare(0, above)

        @pl.when((below < back_b) & (below < z))
        def _():
            prepare(1, below)

        for kinds, col, reach, back in routes:

            def from_above(z, y, hop, reach=reach):
                return (z >= hop) & (hop <= reach)

            def go_up(z, y, hop, reach=reach):
                return (z >= hop) & (hop < reach) & (z < last)

            def from_below(z, y, hop, back=back):
                return ((z + hop) % n_z < back) & (hop <= back)

            def go_down(z, y, hop, back=back):
                return ((z + hop) % n_z < back) & (hop < back)

            def use_below(z, y, hop, back=back):
                return ((z + hop) % n_z < back) & (hop <= back) & ((z + hop) % n_z < z)

            for kind in kinds:
                arrive(kind, above, col, from_above, hop)
                send_whole(UP, kind, above, col, go_up, hop)
                arrive(kind, below, col, from_below, hop)
                send_whole(DOWN, kind, below, col, go_down, hop)
            for side, (row, use) in enumerate(((above, from_above), (below, use_below))):
                if kinds == (1,):
                    choose_1(row, use, use, use, hop, side)
                elif kinds == (0,):
                    choose_0(row, use, hop, side)
                else:
                    choose_2(row, use, hop, side)
        return carry

    lax.fori_loop(hops.start, hops.stop, one_hop, 0)

    def settle(count, sem):
        for k in range(n_z):
            @pl.when(z == k)
            def _():
                for j in range(N_Y):
                    units = count(k, j)
                    if units:
                        @pl.when(y == j)
                        def _():
                            part = kv0.at[0:units * MOST]
                            pltpu.make_async_copy(part, part, sem).wait()

    def due(tile):
        def count(z, y):
            if tile == 1:
                return (z + (y == N_Y - 1)) + (z + (y >= 1)) + (z + (y >= 2))
            if z == last:
                return (z + (y == N_Y - 1)) + z + (y >= 1) + (y >= 2)
            return (z + (y == N_Y - 1)) + (z + (y >= 2))
        return count

    query_row = iota((BLK, keys), 0).astype(F32)
    ones = jnp.ones((keys, LANES), BF16)
    tile_low = iota((BLK, LANES), 1) < HD
    tile_lane = iota((BLK, LANES), 1)
    core_slope = jnp.where(tp == 0, 1.0, 2.0 ** (-8.0 * heads / n_heads)).astype(F32)

    def slope_of(head):
        return core_slope * (2.0 ** (-8.0 * (head + 1) / n_heads))

    def attend(r, side):
        key_pos = kp_s[pl.ds(r, 1), :]
        allowed = key_pos <= query_row
        both = jnp.concatenate([kv[side][index_s[side, r, e]] for e in range(entries)], axis=0)
        scores = dot_nt(q_s[r, side * group * BLK:(side + 1) * group * BLK], both)
        weights = []
        for t in range(group):
            bias = key_pos * (slope_of(side * group + t) * (alibi * LOG2E))
            part = jnp.exp2(scores[t * BLK:(t + 1) * BLK] + bias)
            weights.append(jnp.where(allowed, part, 0.0).astype(BF16))
        return dot(jnp.concatenate(weights, axis=0), jnp.concatenate([both, ones], axis=1))

    def combine(r, outs):
        sums = jnp.ones((BLK, LANES), F32)
        at = pl.ds(r * BLK, BLK)
        for t in range(group):
            first, second = (o[t * BLK:(t + 1) * BLK] for o in outs)
            top = jnp.where(tile_low, first[:, 0:LANES], second[:, 0:LANES])
            total = jnp.where(tile_low, first[:, LANES:], second[:, LANES:])
            att_s[at, t * LANES:(t + 1) * LANES] = (top / total).astype(BF16)
            sums = jnp.where(tile_lane == t, first[:, LANES:], sums)
            sums = jnp.where(tile_lane == t + group, second[:, LANES:], sums)
        sum_s[at] = sums

    loaded(OUT, wo_buf)
    part_rows = rows // PARTS

    def part_at(part):
        return pl.ds(part * part_rows, part_rows)

    def part_copy(part):
        at = part_at(part)
        return pltpu.make_async_remote_copy(
            part_send.at[at], part_recv.at[at], part_sem.at[0, part], part_sem.at[1, part],
            device_id={"tp": partner}, device_id_type=MESH)

    def one_part(part):
        each = nb // PARTS
        first = [attend(part * each + i, 0) for i in range(each)]
        for i in range(each):
            combine(part * each + i, (first[i], found_s[part * each + i]))
        at = part_at(part)
        part_send[at] = dot(att_s[at], wo_buf[1]).astype(BF16)
        part_copy(part).start()

    index_copy.wait()
    settle(due(1), end_sem.at[1])
    for start in range(0, nb, 4):
        second = [attend(start + i, 1) for i in range(4)]
        for i in range(4):
            found_s[start + i] = second[i]
    settle(due(0), end_sem.at[0])
    for part in range(PARTS):
        one_part(part)

    own = dot(att_s[...], wo_buf[0])
    row_in = (iota((rows, LANES), 0) % BLK).astype(F32)
    slopes = jnp.exp2(-8.0 / n_heads * (tp * heads + iota((rows, LANES), 1) + 1).astype(F32))
    logs = jnp.log(sum_s[...]) - slopes * alibi * row_in
    lt_ref[...] = logs.T[0:heads]

    def all_sent(which):
        return lambda z, y: sum(
            units for chain, units, when, looped in sent if chain == which
            for hop in (hops if looped else (0,)) if when(z, y, hop))

    for chain in range(2):
        settle(all_sent(chain), send_sem.at[chain])

    for part in range(PARTS):
        at = slice(part * part_rows, (part + 1) * part_rows)
        part_copy(part).wait()
        out_ref[at] = (own[at] + part_recv[at].astype(F32)).astype(BF16)


def write_out(mixed, log_total, mixed_out, log_out, sems):
    copies = [
        pltpu.make_async_copy(mixed, mixed_out, sems.at[0]),
        pltpu.make_async_copy(log_total, log_out, sems.at[1]),
    ]
    for copy in copies:
        copy.start()
    for copy in copies:
        copy.wait()


def shards(n_kv, tokens, norm_gain, w_query, w_key, w_value, q_gain, k_gain, w_out, chosen):
    seqs, rows, half = tokens.shape
    nb, entries = chosen.shape[1:]
    q_cols, k_cols = w_query.shape[1], w_key.shape[1]
    heads = q_cols // HD
    n_z = n_kv // N_Y
    vmem = pltpu.VMEM
    dma = pltpu.SemaphoreType.DMA
    mixed, log_total = pl.pallas_call(
        functools.partial(kernel, n_kv),
        out_shape=(vmem((rows, half), BF16), vmem((heads, rows), F32)),
        in_specs=[pl.BlockSpec(memory_space=pltpu.HBM)] * 9,
        out_specs=(pl.BlockSpec(memory_space=vmem), pl.BlockSpec(memory_space=vmem)),
        scratch_shapes=[
            vmem((2, rows, half), BF16),
            vmem((nb, entries), jnp.int32),
            vmem((rows, q_cols + 2 * k_cols), F32),
            vmem((2, half, q_cols + 2 * k_cols), BF16),
            vmem((2, q_cols, half), BF16),
            vmem((2, 1, half), F32),
            vmem((2, 1, HD), F32),
            vmem((nb, n_kv * nb), F32),
            vmem((3, nb, n_kv * nb), F32),
            vmem((4, n_z, rows), F32),
            vmem((2, 4, MOST * BLK, rows), BF16),
            vmem((2, nb, entries), jnp.int32),
            pltpu.SMEM((2, nb, entries), jnp.int32),
            vmem((n_z, 2, MOST, BLK, LANES), BF16),
            vmem((n_z, 2, MOST, BLK, LANES), BF16),
            vmem((n_z, 2, MOST, BLK, LANES), BF16),
            vmem((nb, heads * BLK, LANES), BF16),
            vmem((1 + n_kv * nb, BLK, LANES), BF16),
            vmem((1 + n_kv * nb, BLK, LANES), BF16),
            vmem((nb, entries * BLK), F32),
            vmem((nb, heads // 2 * BLK, 2 * LANES), F32),
            vmem((rows, q_cols), BF16),
            vmem((rows, LANES), F32),
            vmem((rows, half), BF16),
            vmem((rows, half), BF16),
            dma((8,)),
            dma((2,)),
            dma((2,)),
            dma((2,)),
            dma((4, n_z)),
            dma((2,)),
            dma((2, PARTS)),
        ],
        compiler_params=pltpu.CompilerParams(
            collective_id=0, has_side_effects=True, vmem_limit_bytes=66_700_000,
        ),
    )(
        tokens.reshape(rows, half), norm_gain.reshape(1, -1), w_query, w_key, w_value,
        q_gain.reshape(1, -1), k_gain.reshape(1, -1), w_out, chosen.reshape(nb, entries),
    )
    mixed, log_total = pl.pallas_call(
        write_out,
        out_shape=(
            jax.ShapeDtypeStruct((rows, half), BF16),
            jax.ShapeDtypeStruct((heads, rows), F32),
        ),
        in_specs=[pl.BlockSpec(memory_space=pl.ANY)] * 2,
        out_specs=(pl.BlockSpec(memory_space=pltpu.HBM),) * 2,
        scratch_shapes=[dma((2,))],
        compiler_params=pltpu.CompilerParams(vmem_limit_bytes=1_000_000),
    )(mixed, log_total)
    return mixed.reshape(seqs, rows, half), log_total.reshape(seqs, heads, rows)


def solution(mesh):
    in_specs = (
        P("dp", "kv", "tp"),
        P(),
        P(None, "tp"),
        P(None, "tp"),
        P(None, "tp"),
        P(),
        P(),
        P("tp", None),
        P("dp", "kv", None),
    )
    out_specs = (P("dp", "kv", "tp"), P("dp", "tp", "kv"))
    return jax.shard_map(
        functools.partial(shards, mesh.shape["kv"]),
        mesh=mesh, in_specs=in_specs, out_specs=out_specs, check_vma=False)
```

```python
import functools
import math

import jax
import jax.numpy as jnp
from jax import lax
from jax.experimental import pallas as pl
from jax.experimental.pallas import tpu as pltpu
from jax.sharding import PartitionSpec as P

HD = 64
BLK = 32
LANES = 128
MOST = 4
PARTS = 2
N_Y = 4
UP, DOWN, LEFT, RIGHT, FAR = range(5)

epsilon = 1e-06
alibi_reach = 4.0
LOG2E = math.log2(math.e)
F32 = jnp.float32
BF16 = jnp.bfloat16
NT = (((1,), (1,)), ((), ()))
MESH = pl.DeviceIdType.MESH


def iota(shape, dim):
    return lax.broadcasted_iota(jnp.int32, shape, dim)


def dot(a, b):
    return jnp.dot(a, b, preferred_element_type=F32)


def dot_nt(a, b):
    return lax.dot_general(a, b, NT, preferred_element_type=F32)


def kernel(
    n_kv,
    tok, gain, wq, wk, wv, qg, kg, wo, ch,
    out_ref, lt_ref,
    x_buf, ch_buf, raw_s, w_buf, wo_buf, g_buf, hg_buf,
    place_send, place_recv, code_s, index_v, index_s, left_s, right_s, far_s,
    q_s, kv0, kv1, kp_s, found_s, att_s, sum_s, part_send, part_recv,
    load_sem, x_sem, place_sem, send_sem, stage_sem, end_sem, part_sem,
):
    me = lax.axis_index("kv")
    tp = lax.axis_index("tp")
    partner = 1 - tp
    n_z = n_kv // N_Y
    z = me // N_Y
    y = me % N_Y
    rows, half = tok.shape
    q_cols = wq.shape[1]
    k_cols = wk.shape[1]
    heads = q_cols // HD
    kv_heads = k_cols // HD
    group = heads // kv_heads
    n_heads = heads * lax.axis_size("tp")
    nb, entries = ch.shape
    n_blocks = n_kv * nb
    width = half * 2
    seq_len = rows * n_kv
    alibi = alibi_reach / seq_len
    keys = entries * BLK
    picked = MOST * BLK
    kv = (kv0, kv1)

    def device(row, col):
        return lax.rem(row + n_z, n_z) * N_Y + lax.rem(col + N_Y, N_Y)

    neighbour = {
        UP: device(z + 1, y), DOWN: device(z - 1, y),
        LEFT: device(z, y - 1), RIGHT: device(z, y + 1), FAR: device(z, y + 2),
    }
    barrier = pltpu.get_barrier_semaphore()
    pl.semaphore_signal(barrier, inc=1, device_id={"tp": partner}, device_id_type=MESH)
    for target in neighbour.values():
        pl.semaphore_signal(barrier, inc=1, device_id={"kv": target}, device_id_type=MESH)

    def span(start):
        return pl.ds(pl.multiple_of(start * half, LANES), half)

    def load(sem, *pairs):
        for src, dst in pairs:
            pltpu.make_async_copy(src, dst, load_sem.at[sem]).start()

    def loaded(sem, whole):
        pltpu.make_async_copy(whole, whole, load_sem.at[sem]).wait()

    def weights(side, which):
        return (
            (wk.at[span(which), :], w_buf.at[side, :, q_cols:q_cols + k_cols]),
            (wv.at[span(which), :], w_buf.at[side, :, q_cols + k_cols:q_cols + 2 * k_cols]),
            (wq.at[span(which), :], w_buf.at[side, :, 0:q_cols]),
        )

    TABLE, TOK, GAIN, W0, W1, HEAD_GAIN, OUT, INDEX = range(8)
    load(TOK, (tok, x_buf.at[0]))
    load(TABLE, (ch, ch_buf))
    load(GAIN, (gain.at[:, span(tp)], g_buf.at[0]), (gain.at[:, span(partner)], g_buf.at[1]))
    load(W0, *weights(0, tp))
    load(W1, *weights(1, partner))
    load(HEAD_GAIN, (qg, hg_buf.at[0]), (kg, hg_buf.at[1]))

    def scaled(side):
        x = x_buf[side].astype(F32)
        return (x * g_buf[side]).astype(BF16), jnp.sum(x * x, axis=1, keepdims=True)

    loaded(TOK, x_buf.at[0])
    pl.semaphore_wait(barrier, 1 + len(neighbour))
    x_copy = pltpu.make_async_remote_copy(
        x_buf.at[0], x_buf.at[1], x_sem.at[0], x_sem.at[1],
        device_id={"tp": partner}, device_id_type=MESH)
    x_copy.start()

    loaded(TABLE, ch_buf)
    lists = ch_buf[...]
    lane_block = iota((nb, n_blocks), 1)
    hits = [lists[:, e:e + 1] == lane_block for e in range(entries)]
    hit = hits[0]
    for e in range(1, entries):
        hit = hit | hits[e]
    need = jnp.broadcast_to(jnp.max(jnp.where(hit, 1, 0), axis=0, keepdims=True), (nb, n_blocks))
    rank_of = jnp.zeros((nb, n_blocks), jnp.int32)
    for k in range(1, nb):
        rank_of = rank_of + jnp.where(lane_block % nb >= k, pltpu.roll(need, k, 1), 0)
    place_send[...] = jnp.where(need > 0, rank_of, -1).astype(F32)

    def place_copy(direction, slot):
        return pltpu.make_async_remote_copy(
            place_send, place_recv.at[slot], place_sem.at[0, slot], place_sem.at[1, slot],
            device_id={"kv": neighbour[direction]}, device_id_type=MESH)

    place_copies = [place_copy(RIGHT, 0), place_copy(LEFT, 1), place_copy(FAR, 2)]
    for copy in place_copies:
        copy.start()

    for side, which in ((0, tp), (1, partner)):
        for head in range(heads):
            to = head % group * LANES + head // group * HD
            load(OUT, (wo.at[head * HD:(head + 1) * HD, span(which)], wo_buf.at[side, to:to + HD]))

    loaded(GAIN, g_buf)
    loaded(W0, w_buf.at[0])
    y0, sq0 = scaled(0)
    raw_s[...] = dot(y0, w_buf[0])

    same_head = jnp.where(
        iota((LANES, LANES), 0) // HD == iota((LANES, LANES), 1) // HD, 1.0, 0.0).astype(BF16)

    def head_norm(v, gain_row):
        sq = v * v
        hi = sq.astype(BF16)
        lo = (sq - hi.astype(F32)).astype(BF16)
        total = dot(hi, same_head) + dot(lo, same_head)
        return v * lax.rsqrt(total / HD + epsilon) * gain_row

    loaded(HEAD_GAIN, hg_buf)
    loaded(W1, w_buf.at[1])
    qg_row = jnp.concatenate([hg_buf[0], hg_buf[0]], axis=1) * (HD ** -0.5 * LOG2E)
    kg_row = jnp.concatenate([hg_buf[1], hg_buf[1]], axis=1)
    low = iota((rows, LANES), 1) < HD
    x_copy.wait()
    y1, sq1 = scaled(1)
    row_scale = lax.rsqrt((sq0 + sq1) / width + epsilon)
    raw_kv = (raw_s[:, q_cols:] + dot(y1, w_buf[1, :, q_cols:])) * row_scale
    key_part = pltpu.roll(head_norm(raw_kv[:, 0:k_cols], kg_row), HD, 1)
    value_part = raw_kv[:, k_cols:]

    def base(row, col):
        return 1 + (row * N_Y + col) * nb

    own_tiles = (jnp.where(low, value_part, key_part), jnp.where(low, key_part, value_part))
    for tile in range(2):
        kv[tile][0] = jnp.zeros((BLK, LANES), BF16)
        kv[tile][pl.ds(base(z, y), nb)] = own_tiles[tile].astype(BF16).reshape(nb, BLK, LANES)

    last = n_z - 1
    reach_a, reach_b = n_z // 2, n_z // 2 - 1
    back_a, back_b = last - reach_a, last - reach_b
    sent = []

    def send(direction, src, dst, chain, units, arrival, when, hop=None):
        sent.append((chain, units, when, hop is not None))

        @pl.when(when(z, y, hop))
        def _():
            pltpu.make_async_remote_copy(
                src, dst, send_sem.at[chain], arrival,
                device_id={"kv": neighbour[direction]}, device_id_type=MESH).start()

    def stage(kind, row):
        return stage_sem.at[kind, row]

    def whole(kind, row, col):
        if kind < 2:
            return kv[kind].at[pl.ds(base(row, col), nb)]
        return kv0.at[pl.ds(base(row, col) + (kind - 2) * (nb // 2), nb // 2)]

    def send_whole(direction, kind, row, col, when, hop=None):
        part = whole(kind, row, col)
        send(direction, part, part, 0, 2 if kind < 2 else 1, stage(kind, row), when, hop)

    def arrive(kind, row, col, when, hop=None):
        @pl.when(when(z, y, hop))
        def _():
            part = whole(kind, row, col)
            pltpu.make_async_remote_copy(
                part, part, send_sem.at[0], stage(kind, row),
                device_id={"kv": neighbour[UP]}, device_id_type=MESH).wait_recv()

    same_row = iota((picked, rows), 0) % BLK == iota((picked, rows), 1) % BLK
    row_slot = (iota((picked, rows), 0) // BLK).astype(F32)

    def chooser(which, row):
        code = code_s[which, pl.ds(row, 1), :]
        return jnp.where(same_row & (code == row_slot), 1.0, 0.0).astype(BF16)

    def item(tile, row, col):
        return kv[tile][pl.ds(base(row, col), nb)].reshape(rows, LANES)

    def blocks(x):
        return x.astype(BF16).reshape(-1, BLK, LANES)

    def send_chosen(direction, buf, tile, row, col, when, hop=None):
        send(direction, buf, kv[tile].at[pl.ds(base(row, col), MOST)], 1, 1, end_sem.at[tile], when, hop)

    def choose_1(row, to_left, to_right, to_far, hop=None):
        @pl.when(to_left(z, y, hop) | to_right(z, y, hop) | to_far(z, y, hop))
        def _():
            code = jnp.concatenate([chooser(i, row) for i in (2, 0, 1)], axis=0)
            found = blocks(dot(code, item(1, row, y)))
            far_s[row, 1] = found[0:MOST]
            left_s[row, 1] = found[MOST:2 * MOST]
            right_s[row, 1] = found[2 * MOST:]

        send_chosen(FAR, far_s.at[row, 1], 1, row, y, to_far, hop)
        send_chosen(LEFT, left_s.at[row, 1], 1, row, y, to_left, hop)
        send_chosen(RIGHT, right_s.at[row, 1], 1, row, y, to_right, hop)

    def choose_0(row, to_left, hop=None):
        @pl.when(to_left(z, y, hop))
        def _():
            left_s[row, 0] = blocks(dot(chooser(0, row), item(0, row, y)))

        send_chosen(LEFT, left_s.at[row, 0], 0, row, y, to_left, hop)

    def choose_2(row, to_right, hop=None):
        @pl.when(to_right(z, y, hop))
        def _():
            right_s[row, 0] = blocks(dot(chooser(3, row), item(0, row, left_col)))

        send_chosen(RIGHT, right_s.at[row, 0], 0, row, left_col, to_right, hop)

    def choose_last(to_right, to_far):
        @pl.when(to_right(z, y, None))
        def _():
            code = jnp.concatenate([chooser(i, z) for i in (2, 1)], axis=0)
            found = blocks(dot(code, item(0, z, y)))
            far_s[z, 0] = found[0:MOST]
            right_s[z, 0] = found[MOST:]

        send_chosen(FAR, far_s.at[z, 0], 0, z, y, to_far)
        send_chosen(RIGHT, right_s.at[z, 0], 0, z, y, to_right)

    left_col = lax.rem(y + N_Y - 1, N_Y)
    for kind in (2, 3):
        send_whole(RIGHT, kind, z, y, lambda z, y, hop: z < last)
    for kind in (1, 0):
        send_whole(UP, kind, z, y, lambda z, y, hop: z < last)
        send_whole(DOWN, kind, z, y, lambda z, y, hop: z < back_a)

    for copy in place_copies:
        copy.wait()
    spread = jnp.where(
        iota((n_blocks, rows), 0) % nb == iota((n_blocks, rows), 1) // BLK, 1.0, 0.0).astype(BF16)
    row_owner = iota((n_z, n_blocks), 0) * N_Y
    owner_lane = iota((n_z, n_blocks), 1) // nb
    for which, (slot, col) in enumerate(((0, y), (1, y), (2, y), (1, left_col))):
        mine = jnp.where(owner_lane == row_owner + col, place_recv[slot], 0.0)
        code_s[which] = dot(mine.astype(BF16), spread)

    choose_1(z, lambda z, y, hop: y == 0, lambda z, y, hop: y < N_Y - 1, lambda z, y, hop: y < N_Y - 2)
    choose_0(z, lambda z, y, hop: y == 0)
    choose_last(
        lambda z, y, hop: (z == last) & (y < N_Y - 1), lambda z, y, hop: (z == last) & (y < N_Y - 2))

    raw = (raw_s[:, 0:q_cols] + dot(y1, w_buf[1, :, 0:q_cols])) * row_scale
    for tile in range(q_cols // LANES):
        q = head_norm(raw[:, tile * LANES:(tile + 1) * LANES], qg_row)
        turned = pltpu.roll(q, HD, 1)
        for odd in range(2):
            head = 2 * tile + odd
            side = head // group
            here = turned if odd == side else q
            here = jnp.where(low if side == 1 else ~low, here, 0.0).astype(BF16)
            for r in range(nb):
                q_s[r, head * BLK:(head + 1) * BLK] = here[r * BLK:(r + 1) * BLK]

    lane_entry = iota((nb, entries), 1)
    rank = jnp.zeros((nb, entries), jnp.int32)
    for e in range(entries):
        found = jnp.max(jnp.where(hits[e], rank_of, 0), axis=1, keepdims=True)
        rank = jnp.where(lane_entry == e, found, rank)
    owner = lists // nb
    owner_row = owner // N_Y
    col = lax.rem(owner, N_Y)
    ranked = 1 + owner * nb + rank
    for tile in range(2):
        full = col == y
        if tile == 0:
            full = full | ((col == left_col) & (owner_row != last))
        index_v[tile] = jnp.where(lists < 0, 0, jnp.where(full, 1 + lists, ranked))
    index_copy = pltpu.make_async_copy(index_v, index_s, load_sem.at[INDEX])
    index_copy.start()

    lane = iota((nb, keys), 1)
    block = jnp.full((nb, keys), -1, jnp.int32)
    for e in range(entries):
        block = jnp.where(lane // BLK == e, lists[:, e:e + 1], block)
    away = (block - (me * nb + iota((nb, keys), 0))) * BLK + lane % BLK
    kp_s[...] = jnp.where(block < 0, 1 << 24, away).astype(F32)

    for kind in (2, 3):
        arrive(kind, z, left_col, lambda z, y, hop: z < last)
        send_whole(UP, kind, z, left_col, lambda z, y, hop: z < last)
        send_whole(DOWN, kind, z, left_col, lambda z, y, hop: z < back_b)
    choose_2(z, lambda z, y, hop: (z < last) & ((y == 1) | (y == 2)))

    routes = (((1,), y, reach_a, back_a), ((0,), y, reach_a, back_a), ((2, 3), left_col, reach_b, back_b))
    hops = range(1, n_z // 2 + 1)

    def one_hop(hop, carry):
        above = lax.max(z - hop, 0)
        below = lax.rem(z + hop, n_z)
        for kinds, col, reach, back in routes:

            def from_above(z, y, hop, reach=reach):
                return (z >= hop) & (hop <= reach)

            def go_up(z, y, hop, reach=reach):
                return (z >= hop) & (hop < reach) & (z < last)

            def from_below(z, y, hop, back=back):
                return ((z + hop) % n_z < back) & (hop <= back)

            def go_down(z, y, hop, back=back):
                return ((z + hop) % n_z < back) & (hop < back)

            def use_below(z, y, hop, back=back):
                return ((z + hop) % n_z < back) & (hop <= back) & ((z + hop) % n_z < z)

            for kind in kinds:
                arrive(kind, above, col, from_above, hop)
                send_whole(UP, kind, above, col, go_up, hop)
                arrive(kind, below, col, from_below, hop)
                send_whole(DOWN, kind, below, col, go_down, hop)
            for row, use in ((above, from_above), (below, use_below)):
                if kinds == (1,):
                    choose_1(row, use, use, use, hop)
                elif kinds == (0,):
                    choose_0(row, use, hop)
                else:
                    choose_2(row, use, hop)
        return carry

    lax.fori_loop(hops.start, hops.stop, one_hop, 0)

    def settle(count, sem):
        for k in range(n_z):
            @pl.when(z == k)
            def _():
                for j in range(N_Y):
                    units = count(k, j)
                    if units:
                        @pl.when(y == j)
                        def _():
                            part = kv0.at[0:units * MOST]
                            pltpu.make_async_copy(part, part, sem).wait()

    def due(tile):
        def count(z, y):
            if tile == 1:
                return (z + (y == N_Y - 1)) + (z + (y >= 1)) + (z + (y >= 2))
            if z == last:
                return (z + (y == N_Y - 1)) + z + (y >= 1) + (y >= 2)
            return (z + (y == N_Y - 1)) + (z + (y >= 2))
        return count

    query_row = iota((BLK, keys), 0).astype(F32)
    ones = jnp.ones((keys, LANES), BF16)
    tile_low = iota((BLK, LANES), 1) < HD
    tile_lane = iota((BLK, LANES), 1)
    core_slope = jnp.where(tp == 0, 1.0, 2.0 ** (-8.0 * heads / n_heads)).astype(F32)

    def slope_of(head):
        return core_slope * (2.0 ** (-8.0 * (head + 1) / n_heads))

    def attend(r, side):
        key_pos = kp_s[pl.ds(r, 1), :]
        allowed = key_pos <= query_row
        both = jnp.concatenate([kv[side][index_s[side, r, e]] for e in range(entries)], axis=0)
        scores = dot_nt(q_s[r, side * group * BLK:(side + 1) * group * BLK], both)
        weights = []
        for t in range(group):
            bias = key_pos * (slope_of(side * group + t) * (alibi * LOG2E))
            part = jnp.exp2(scores[t * BLK:(t + 1) * BLK] + bias)
            weights.append(jnp.where(allowed, part, 0.0).astype(BF16))
        return dot(jnp.concatenate(weights, axis=0), jnp.concatenate([both, ones], axis=1))

    def combine(r, outs):
        sums = jnp.ones((BLK, LANES), F32)
        at = pl.ds(r * BLK, BLK)
        for t in range(group):
            first, second = (o[t * BLK:(t + 1) * BLK] for o in outs)
            top = jnp.where(tile_low, first[:, 0:LANES], second[:, 0:LANES])
            total = jnp.where(tile_low, first[:, LANES:], second[:, LANES:])
            att_s[at, t * LANES:(t + 1) * LANES] = (top / total).astype(BF16)
            sums = jnp.where(tile_lane == t, first[:, LANES:], sums)
            sums = jnp.where(tile_lane == t + group, second[:, LANES:], sums)
        sum_s[at] = sums

    loaded(OUT, wo_buf)
    part_rows = rows // PARTS

    def part_at(part):
        return pl.ds(part * part_rows, part_rows)

    def part_copy(part):
        at = part_at(part)
        return pltpu.make_async_remote_copy(
            part_send.at[at], part_recv.at[at], part_sem.at[0, part], part_sem.at[1, part],
            device_id={"tp": partner}, device_id_type=MESH)

    index_copy.wait()
    settle(due(1), end_sem.at[1])
    for start in range(0, nb, 4):
        second = [attend(start + i, 1) for i in range(4)]
        for i in range(4):
            found_s[start + i] = second[i]
    settle(due(0), end_sem.at[0])
    first = [attend(r, 0) for r in range(nb)]
    for r in range(nb):
        combine(r, (first[r], found_s[r]))
    for part in range(PARTS):
        at = part_at(part)
        part_send[at] = dot(att_s[at], wo_buf[1]).astype(BF16)
        part_copy(part).start()

    own = dot(att_s[...], wo_buf[0])
    row_in = (iota((rows, LANES), 0) % BLK).astype(F32)
    slopes = jnp.exp2(-8.0 / n_heads * (tp * heads + iota((rows, LANES), 1) + 1).astype(F32))
    logs = jnp.log(sum_s[...]) - slopes * alibi * row_in
    lt_ref[...] = logs.T[0:heads]

    def all_sent(which):
        return lambda z, y: sum(
            units for chain, units, when, looped in sent if chain == which
            for hop in (hops if looped else (0,)) if when(z, y, hop))

    for chain in range(2):
        settle(all_sent(chain), send_sem.at[chain])

    for part in range(PARTS):
        at = slice(part * part_rows, (part + 1) * part_rows)
        part_copy(part).wait()
        out_ref[at] = (own[at] + part_recv[at].astype(F32)).astype(BF16)


def write_out(mixed, log_total, mixed_out, log_out, sems):
    copies = [
        pltpu.make_async_copy(mixed, mixed_out, sems.at[0]),
        pltpu.make_async_copy(log_total, log_out, sems.at[1]),
    ]
    for copy in copies:
        copy.start()
    for copy in copies:
        copy.wait()


def shards(n_kv, tokens, norm_gain, w_query, w_key, w_value, q_gain, k_gain, w_out, chosen):
    seqs, rows, half = tokens.shape
    nb, entries = chosen.shape[1:]
    q_cols, k_cols = w_query.shape[1], w_key.shape[1]
    heads = q_cols // HD
    n_z = n_kv // N_Y
    vmem = pltpu.VMEM
    dma = pltpu.SemaphoreType.DMA
    mixed, log_total = pl.pallas_call(
        functools.partial(kernel, n_kv),
        out_shape=(vmem((rows, half), BF16), vmem((heads, rows), F32)),
        in_specs=[pl.BlockSpec(memory_space=pltpu.HBM)] * 9,
        out_specs=(pl.BlockSpec(memory_space=vmem), pl.BlockSpec(memory_space=vmem)),
        scratch_shapes=[
            vmem((2, rows, half), BF16),
            vmem((nb, entries), jnp.int32),
            vmem((rows, q_cols + 2 * k_cols), F32),
            vmem((2, half, q_cols + 2 * k_cols), BF16),
            vmem((2, q_cols, half), BF16),
            vmem((2, 1, half), F32),
            vmem((2, 1, HD), F32),
            vmem((nb, n_kv * nb), F32),
            vmem((3, nb, n_kv * nb), F32),
            vmem((4, n_z, rows), F32),
            vmem((2, nb, entries), jnp.int32),
            pltpu.SMEM((2, nb, entries), jnp.int32),
            vmem((n_z, 2, MOST, BLK, LANES), BF16),
            vmem((n_z, 2, MOST, BLK, LANES), BF16),
            vmem((n_z, 2, MOST, BLK, LANES), BF16),
            vmem((nb, heads * BLK, LANES), BF16),
            vmem((1 + n_kv * nb, BLK, LANES), BF16),
            vmem((1 + n_kv * nb, BLK, LANES), BF16),
            vmem((nb, entries * BLK), F32),
            vmem((nb, heads // 2 * BLK, 2 * LANES), F32),
            vmem((rows, q_cols), BF16),
            vmem((rows, LANES), F32),
            vmem((rows, half), BF16),
            vmem((rows, half), BF16),
            dma((8,)),
            dma((2,)),
            dma((2, 3)),
            dma((2,)),
            dma((4, n_z)),
            dma((2,)),
            dma((2, PARTS)),
        ],
        compiler_params=pltpu.CompilerParams(
            collective_id=0, has_side_effects=True, vmem_limit_bytes=66_700_000
        ),
    )(
        tokens.reshape(rows, half), norm_gain.reshape(1, -1), w_query, w_key, w_value,
        q_gain.reshape(1, -1), k_gain.reshape(1, -1), w_out, chosen.reshape(nb, entries),
    )
    mixed, log_total = pl.pallas_call(
        write_out,
        out_shape=(
            jax.ShapeDtypeStruct((rows, half), BF16),
            jax.ShapeDtypeStruct((heads, rows), F32),
        ),
        in_specs=[pl.BlockSpec(memory_space=pl.ANY)] * 2,
        out_specs=(pl.BlockSpec(memory_space=pltpu.HBM),) * 2,
        scratch_shapes=[dma((2,))],
        compiler_params=pltpu.CompilerParams(vmem_limit_bytes=1_000_000),
    )(mixed, log_total)
    return mixed.reshape(seqs, rows, half), log_total.reshape(seqs, heads, rows)


def solution(mesh):
    in_specs = (
        P("dp", "kv", "tp"),
        P(),
        P(None, "tp"),
        P(None, "tp"),
        P(None, "tp"),
        P(),
        P(),
        P("tp", None),
        P("dp", "kv", None),
    )
    out_specs = (P("dp", "kv", "tp"), P("dp", "tp", "kv"))
    return jax.shard_map(
        functools.partial(shards, mesh.shape["kv"]),
        mesh=mesh, in_specs=in_specs, out_specs=out_specs, check_vma=False)
```

```python
import functools
import math

import jax
import jax.numpy as jnp
from jax import lax
from jax.experimental import pallas as pl
from jax.experimental.pallas import tpu as pltpu
from jax.sharding import PartitionSpec as P

HD = 64
BLK = 32
LANES = 128
MOST = 4
PARTS = 2
N_Y = 4
UP, DOWN, LEFT, RIGHT, FAR = range(5)

epsilon = 1e-06
alibi_reach = 4.0
LOG2E = math.log2(math.e)
F32 = jnp.float32
BF16 = jnp.bfloat16
NT = (((1,), (1,)), ((), ()))
MESH = pl.DeviceIdType.MESH


def iota(shape, dim):
    return lax.broadcasted_iota(jnp.int32, shape, dim)


def dot(a, b):
    return jnp.dot(a, b, preferred_element_type=F32)


def dot_nt(a, b):
    return lax.dot_general(a, b, NT, preferred_element_type=F32)


def kernel(
    n_kv,
    tok, gain, wq, wk, wv, qg, kg, wo, ch,
    out_ref, lt_ref,
    x_buf, ch_buf, raw_s, w_buf, wo_buf, g_buf, hg_buf,
    place_send, place_recv, code_s, index_v, index_s, left_s, right_s, far_s,
    q_s, kv0, kv1, kp_s, found_s, att_s, sum_s, part_send, part_recv,
    load_sem, x_sem, place_sem, send_sem, stage_sem, end_sem, part_sem,
):
    me = lax.axis_index("kv")
    tp = lax.axis_index("tp")
    partner = 1 - tp
    n_z = n_kv // N_Y
    z = me // N_Y
    y = me % N_Y
    rows, half = tok.shape
    q_cols = wq.shape[1]
    k_cols = wk.shape[1]
    heads = q_cols // HD
    kv_heads = k_cols // HD
    group = heads // kv_heads
    n_heads = heads * lax.axis_size("tp")
    nb, entries = ch.shape
    n_blocks = n_kv * nb
    width = half * 2
    seq_len = rows * n_kv
    alibi = alibi_reach / seq_len
    keys = entries * BLK
    picked = MOST * BLK
    kv = (kv0, kv1)

    def device(row, col):
        return lax.rem(row + n_z, n_z) * N_Y + lax.rem(col + N_Y, N_Y)

    neighbour = {
        UP: device(z + 1, y), DOWN: device(z - 1, y),
        LEFT: device(z, y - 1), RIGHT: device(z, y + 1), FAR: device(z, y + 2),
    }
    barrier = pltpu.get_barrier_semaphore()
    pl.semaphore_signal(barrier, inc=1, device_id={"tp": partner}, device_id_type=MESH)
    for target in neighbour.values():
        pl.semaphore_signal(barrier, inc=1, device_id={"kv": target}, device_id_type=MESH)

    def span(start):
        return pl.ds(pl.multiple_of(start * half, LANES), half)

    def load(sem, *pairs):
        for src, dst in pairs:
            pltpu.make_async_copy(src, dst, load_sem.at[sem]).start()

    def loaded(sem, whole):
        pltpu.make_async_copy(whole, whole, load_sem.at[sem]).wait()

    def weights(side, which):
        return (
            (wk.at[span(which), :], w_buf.at[side, :, q_cols:q_cols + k_cols]),
            (wv.at[span(which), :], w_buf.at[side, :, q_cols + k_cols:q_cols + 2 * k_cols]),
            (wq.at[span(which), :], w_buf.at[side, :, 0:q_cols]),
        )

    TABLE, TOK, GAIN, W0, W1, HEAD_GAIN, OUT, INDEX = range(8)
    load(TOK, (tok, x_buf.at[0]))
    load(TABLE, (ch, ch_buf))
    load(GAIN, (gain.at[:, span(tp)], g_buf.at[0]), (gain.at[:, span(partner)], g_buf.at[1]))
    load(W0, *weights(0, tp))
    load(W1, *weights(1, partner))
    load(HEAD_GAIN, (qg, hg_buf.at[0]), (kg, hg_buf.at[1]))

    def scaled(side):
        x = x_buf[side].astype(F32)
        return (x * g_buf[side]).astype(BF16), jnp.sum(x * x, axis=1, keepdims=True)

    loaded(TOK, x_buf.at[0])
    pl.semaphore_wait(barrier, 1 + len(neighbour))
    x_copy = pltpu.make_async_remote_copy(
        x_buf.at[0], x_buf.at[1], x_sem.at[0], x_sem.at[1],
        device_id={"tp": partner}, device_id_type=MESH)
    x_copy.start()

    loaded(TABLE, ch_buf)
    lists = ch_buf[...]
    lane_block = iota((nb, n_blocks), 1)
    hits = [lists[:, e:e + 1] == lane_block for e in range(entries)]
    hit = hits[0]
    for e in range(1, entries):
        hit = hit | hits[e]
    need = jnp.broadcast_to(jnp.max(jnp.where(hit, 1, 0), axis=0, keepdims=True), (nb, n_blocks))
    rank_of = jnp.zeros((nb, n_blocks), jnp.int32)
    for k in range(1, nb):
        rank_of = rank_of + jnp.where(lane_block % nb >= k, pltpu.roll(need, k, 1), 0)
    place_send[...] = jnp.where(need > 0, rank_of, -1).astype(F32)

    def place_copy(direction, slot):
        return pltpu.make_async_remote_copy(
            place_send, place_recv.at[slot], place_sem.at[0], place_sem.at[1],
            device_id={"kv": neighbour[direction]}, device_id_type=MESH)

    place_copies = [place_copy(RIGHT, 0), place_copy(LEFT, 1), place_copy(FAR, 2)]
    for copy in place_copies:
        copy.start()


    loaded(GAIN, g_buf)
    loaded(W0, w_buf.at[0])
    y0, sq0 = scaled(0)
    raw_s[...] = dot(y0, w_buf[0])

    same_head = jnp.where(
        iota((LANES, LANES), 0) // HD == iota((LANES, LANES), 1) // HD, 1.0, 0.0).astype(BF16)

    def head_norm(v, gain_row):
        sq = v * v
        hi = sq.astype(BF16)
        lo = (sq - hi.astype(F32)).astype(BF16)
        total = dot(hi, same_head) + dot(lo, same_head)
        return v * lax.rsqrt(total / HD + epsilon) * gain_row

    loaded(HEAD_GAIN, hg_buf)
    loaded(W1, w_buf.at[1])
    qg_row = jnp.concatenate([hg_buf[0], hg_buf[0]], axis=1) * (HD ** -0.5 * LOG2E)
    kg_row = jnp.concatenate([hg_buf[1], hg_buf[1]], axis=1)
    low = iota((rows, LANES), 1) < HD
    x_copy.wait()
    y1, sq1 = scaled(1)
    row_scale = lax.rsqrt((sq0 + sq1) / width + epsilon)
    raw_kv = (raw_s[:, q_cols:] + dot(y1, w_buf[1, :, q_cols:])) * row_scale
    key_part = pltpu.roll(head_norm(raw_kv[:, 0:k_cols], kg_row), HD, 1)
    value_part = raw_kv[:, k_cols:]

    def base(row, col):
        return 1 + (row * N_Y + col) * nb

    own_tiles = (jnp.where(low, value_part, key_part), jnp.where(low, key_part, value_part))
    for tile in range(2):
        kv[tile][0] = jnp.zeros((BLK, LANES), BF16)
        kv[tile][pl.ds(base(z, y), nb)] = own_tiles[tile].astype(BF16).reshape(nb, BLK, LANES)

    last = n_z - 1
    reach_a, reach_b = n_z // 2, n_z // 2 - 1
    back_a, back_b = last - reach_a, last - reach_b
    sent = []

    def send(direction, src, dst, chain, units, arrival, when, hop=None):
        sent.append((chain, units, when, hop is not None))

        @pl.when(when(z, y, hop))
        def _():
            pltpu.make_async_remote_copy(
                src, dst, send_sem.at[chain], arrival,
                device_id={"kv": neighbour[direction]}, device_id_type=MESH).start()

    def stage(kind, row):
        return stage_sem.at[kind, row]

    def whole(kind, row, col):
        if kind < 2:
            return kv[kind].at[pl.ds(base(row, col), nb)]
        return kv0.at[pl.ds(base(row, col) + (kind - 2) * (nb // 2), nb // 2)]

    def send_whole(direction, kind, row, col, when, hop=None):
        part = whole(kind, row, col)
        send(direction, part, part, 0, 2 if kind < 2 else 1, stage(kind, row), when, hop)

    def arrive(kind, row, col, when, hop=None):
        @pl.when(when(z, y, hop))
        def _():
            part = whole(kind, row, col)
            pltpu.make_async_remote_copy(
                part, part, send_sem.at[0], stage(kind, row),
                device_id={"kv": neighbour[UP]}, device_id_type=MESH).wait_recv()

    same_row = iota((picked, rows), 0) % BLK == iota((picked, rows), 1) % BLK
    row_slot = (iota((picked, rows), 0) // BLK).astype(F32)

    def chooser(which, row):
        code = code_s[which, pl.ds(row, 1), :]
        return jnp.where(same_row & (code == row_slot), 1.0, 0.0).astype(BF16)

    def item(tile, row, col):
        return kv[tile][pl.ds(base(row, col), nb)].reshape(rows, LANES)

    def blocks(x):
        return x.astype(BF16).reshape(-1, BLK, LANES)

    def send_chosen(direction, buf, tile, row, col, when, hop=None):
        send(direction, buf, kv[tile].at[pl.ds(base(row, col), MOST)], 1, 1, end_sem.at[tile], when, hop)

    def choose_1(row, to_left, to_right, to_far, hop=None):
        @pl.when(to_left(z, y, hop) | to_right(z, y, hop) | to_far(z, y, hop))
        def _():
            code = jnp.concatenate([chooser(i, row) for i in (2, 0, 1)], axis=0)
            found = blocks(dot(code, item(1, row, y)))
            far_s[row, 1] = found[0:MOST]
            left_s[row, 1] = found[MOST:2 * MOST]
            right_s[row, 1] = found[2 * MOST:]

        send_chosen(LEFT, left_s.at[row, 1], 1, row, y, to_left, hop)
        send_chosen(RIGHT, right_s.at[row, 1], 1, row, y, to_right, hop)
        send_chosen(FAR, far_s.at[row, 1], 1, row, y, to_far, hop)

    def choose_0(row, to_left, hop=None):
        @pl.when(to_left(z, y, hop))
        def _():
            left_s[row, 0] = blocks(dot(chooser(0, row), item(0, row, y)))

        send_chosen(LEFT, left_s.at[row, 0], 0, row, y, to_left, hop)

    def choose_2(row, to_right, hop=None):
        @pl.when(to_right(z, y, hop))
        def _():
            right_s[row, 0] = blocks(dot(chooser(3, row), item(0, row, left_col)))

        send_chosen(RIGHT, right_s.at[row, 0], 0, row, left_col, to_right, hop)

    def choose_last(to_right, to_far):
        @pl.when(to_right(z, y, None))
        def _():
            code = jnp.concatenate([chooser(i, z) for i in (2, 1)], axis=0)
            found = blocks(dot(code, item(0, z, y)))
            far_s[z, 0] = found[0:MOST]
            right_s[z, 0] = found[MOST:]

        send_chosen(FAR, far_s.at[z, 0], 0, z, y, to_far)
        send_chosen(RIGHT, right_s.at[z, 0], 0, z, y, to_right)

    left_col = lax.rem(y + N_Y - 1, N_Y)
    for kind in (2, 3):
        send_whole(RIGHT, kind, z, y, lambda z, y, hop: z < last)
    for kind in (1, 0):
        send_whole(UP, kind, z, y, lambda z, y, hop: z < last)
        send_whole(DOWN, kind, z, y, lambda z, y, hop: z < back_a)

    for side, which in ((0, tp), (1, partner)):
        for head in range(heads):
            to = head % group * LANES + head // group * HD
            load(OUT, (wo.at[head * HD:(head + 1) * HD, span(which)], wo_buf.at[side, to:to + HD]))

    for sem in range(2):
        pltpu.make_async_copy(place_recv, place_recv, place_sem.at[sem]).wait()
    spread = jnp.where(
        iota((n_blocks, rows), 0) % nb == iota((n_blocks, rows), 1) // BLK, 1.0, 0.0).astype(BF16)
    row_owner = iota((n_z, n_blocks), 0) * N_Y
    owner_lane = iota((n_z, n_blocks), 1) // nb
    for which, (slot, col) in enumerate(((0, y), (1, y), (2, y), (1, left_col))):
        mine = jnp.where(owner_lane == row_owner + col, place_recv[slot], 0.0)
        code_s[which] = dot(mine.astype(BF16), spread)

    choose_1(z, lambda z, y, hop: y == 0, lambda z, y, hop: y < N_Y - 1, lambda z, y, hop: y < N_Y - 2)
    choose_0(z, lambda z, y, hop: y == 0)
    choose_last(
        lambda z, y, hop: (z == last) & (y < N_Y - 1), lambda z, y, hop: (z == last) & (y < N_Y - 2))

    raw = (raw_s[:, 0:q_cols] + dot(y1, w_buf[1, :, 0:q_cols])) * row_scale
    for tile in range(q_cols // LANES):
        q = head_norm(raw[:, tile * LANES:(tile + 1) * LANES], qg_row)
        turned = pltpu.roll(q, HD, 1)
        for odd in range(2):
            head = 2 * tile + odd
            side = head // group
            here = turned if odd == side else q
            here = jnp.where(low if side == 1 else ~low, here, 0.0).astype(BF16)
            for r in range(nb):
                q_s[r, head * BLK:(head + 1) * BLK] = here[r * BLK:(r + 1) * BLK]

    lane_entry = iota((nb, entries), 1)
    rank = jnp.zeros((nb, entries), jnp.int32)
    for e in range(entries):
        found = jnp.max(jnp.where(hits[e], rank_of, 0), axis=1, keepdims=True)
        rank = jnp.where(lane_entry == e, found, rank)
    owner = lists // nb
    owner_row = owner // N_Y
    col = lax.rem(owner, N_Y)
    ranked = 1 + owner * nb + rank
    for tile in range(2):
        full = col == y
        if tile == 0:
            full = full | ((col == left_col) & (owner_row != last))
        index_v[tile] = jnp.where(lists < 0, 0, jnp.where(full, 1 + lists, ranked))
    index_copy = pltpu.make_async_copy(index_v, index_s, load_sem.at[INDEX])
    index_copy.start()

    lane = iota((nb, keys), 1)
    block = jnp.full((nb, keys), -1, jnp.int32)
    for e in range(entries):
        block = jnp.where(lane // BLK == e, lists[:, e:e + 1], block)
    away = (block - (me * nb + iota((nb, keys), 0))) * BLK + lane % BLK
    kp_s[...] = jnp.where(block < 0, 1 << 24, away).astype(F32)

    for kind in (2, 3):
        arrive(kind, z, left_col, lambda z, y, hop: z < last)
        send_whole(UP, kind, z, left_col, lambda z, y, hop: z < last)
        send_whole(DOWN, kind, z, left_col, lambda z, y, hop: z < back_b)
    choose_2(z, lambda z, y, hop: (z < last) & ((y == 1) | (y == 2)))

    routes = (((1,), y, reach_a, back_a), ((0,), y, reach_a, back_a), ((2, 3), left_col, reach_b, back_b))
    hops = range(1, n_z // 2 + 1)

    def one_hop(hop, carry):
        above = lax.max(z - hop, 0)
        below = lax.rem(z + hop, n_z)
        for kinds, col, reach, back in routes:

            def from_above(z, y, hop, reach=reach):
                return (z >= hop) & (hop <= reach)

            def go_up(z, y, hop, reach=reach):
                return (z >= hop) & (hop < reach) & (z < last)

            def from_below(z, y, hop, back=back):
                return ((z + hop) % n_z < back) & (hop <= back)

            def go_down(z, y, hop, back=back):
                return ((z + hop) % n_z < back) & (hop < back)

            def use_below(z, y, hop, back=back):
                return ((z + hop) % n_z < back) & (hop <= back) & ((z + hop) % n_z < z)

            for kind in kinds:
                arrive(kind, above, col, from_above, hop)
                send_whole(UP, kind, above, col, go_up, hop)
                arrive(kind, below, col, from_below, hop)
                send_whole(DOWN, kind, below, col, go_down, hop)
            for row, use in ((above, from_above), (below, use_below)):
                if kinds == (1,):
                    choose_1(row, use, use, use, hop)
                elif kinds == (0,):
                    choose_0(row, use, hop)
                else:
                    choose_2(row, use, hop)
        return carry

    lax.fori_loop(hops.start, hops.stop, one_hop, 0)

    def settle(count, sem):
        for k in range(n_z):
            @pl.when(z == k)
            def _():
                for j in range(N_Y):
                    units = count(k, j)
                    if units:
                        @pl.when(y == j)
                        def _():
                            part = kv0.at[0:units * MOST]
                            pltpu.make_async_copy(part, part, sem).wait()

    def due(tile):
        def count(z, y):
            if tile == 1:
                return (z + (y == N_Y - 1)) + (z + (y >= 1)) + (z + (y >= 2))
            if z == last:
                return (z + (y == N_Y - 1)) + z + (y >= 1) + (y >= 2)
            return (z + (y == N_Y - 1)) + (z + (y >= 2))
        return count

    query_row = iota((BLK, keys), 0).astype(F32)
    ones = jnp.ones((keys, LANES), BF16)
    tile_low = iota((BLK, LANES), 1) < HD
    tile_lane = iota((BLK, LANES), 1)
    core_slope = jnp.where(tp == 0, 1.0, 2.0 ** (-8.0 * heads / n_heads)).astype(F32)

    def slope_of(head):
        return core_slope * (2.0 ** (-8.0 * (head + 1) / n_heads))

    def attend(r, side):
        key_pos = kp_s[pl.ds(r, 1), :]
        allowed = key_pos <= query_row
        both = jnp.concatenate([kv[side][index_s[side, r, e]] for e in range(entries)], axis=0)
        scores = dot_nt(q_s[r, side * group * BLK:(side + 1) * group * BLK], both)
        weights = []
        for t in range(group):
            bias = key_pos * (slope_of(side * group + t) * (alibi * LOG2E))
            part = jnp.exp2(scores[t * BLK:(t + 1) * BLK] + bias)
            weights.append(jnp.where(allowed, part, 0.0).astype(BF16))
        return dot(jnp.concatenate(weights, axis=0), jnp.concatenate([both, ones], axis=1))

    def combine(r, outs):
        sums = jnp.ones((BLK, LANES), F32)
        at = pl.ds(r * BLK, BLK)
        for t in range(group):
            first, second = (o[t * BLK:(t + 1) * BLK] for o in outs)
            top = jnp.where(tile_low, first[:, 0:LANES], second[:, 0:LANES])
            total = jnp.where(tile_low, first[:, LANES:], second[:, LANES:])
            att_s[at, t * LANES:(t + 1) * LANES] = (top / total).astype(BF16)
            sums = jnp.where(tile_lane == t, first[:, LANES:], sums)
            sums = jnp.where(tile_lane == t + group, second[:, LANES:], sums)
        sum_s[at] = sums

    loaded(OUT, wo_buf)
    part_rows = rows // PARTS

    def part_at(part):
        return pl.ds(part * part_rows, part_rows)

    def part_copy(part):
        at = part_at(part)
        return pltpu.make_async_remote_copy(
            part_send.at[at], part_recv.at[at], part_sem.at[0, part], part_sem.at[1, part],
            device_id={"tp": partner}, device_id_type=MESH)

    index_copy.wait()
    settle(due(1), end_sem.at[1])
    for start in range(0, nb, 4):
        second = [attend(start + i, 1) for i in range(4)]
        for i in range(4):
            found_s[start + i] = second[i]
    settle(due(0), end_sem.at[0])
    first = [attend(r, 0) for r in range(nb)]
    for r in range(nb):
        combine(r, (first[r], found_s[r]))
    for part in range(PARTS):
        at = part_at(part)
        part_send[at] = dot(att_s[at], wo_buf[1]).astype(BF16)
        part_copy(part).start()

    own = dot(att_s[...], wo_buf[0])
    row_in = (iota((rows, LANES), 0) % BLK).astype(F32)
    slopes = jnp.exp2(-8.0 / n_heads * (tp * heads + iota((rows, LANES), 1) + 1).astype(F32))
    logs = jnp.log(sum_s[...]) - slopes * alibi * row_in
    lt_ref[...] = logs.T[0:heads]

    def all_sent(which):
        return lambda z, y: sum(
            units for chain, units, when, looped in sent if chain == which
            for hop in (hops if looped else (0,)) if when(z, y, hop))

    for chain in range(2):
        settle(all_sent(chain), send_sem.at[chain])

    for part in range(PARTS):
        at = slice(part * part_rows, (part + 1) * part_rows)
        part_copy(part).wait()
        out_ref[at] = (own[at] + part_recv[at].astype(F32)).astype(BF16)


def write_out(mixed, log_total, mixed_out, log_out, sems):
    copies = [
        pltpu.make_async_copy(mixed, mixed_out, sems.at[0]),
        pltpu.make_async_copy(log_total, log_out, sems.at[1]),
    ]
    for copy in copies:
        copy.start()
    for copy in copies:
        copy.wait()


def shards(n_kv, tokens, norm_gain, w_query, w_key, w_value, q_gain, k_gain, w_out, chosen):
    seqs, rows, half = tokens.shape
    nb, entries = chosen.shape[1:]
    q_cols, k_cols = w_query.shape[1], w_key.shape[1]
    heads = q_cols // HD
    n_z = n_kv // N_Y
    vmem = pltpu.VMEM
    dma = pltpu.SemaphoreType.DMA
    mixed, log_total = pl.pallas_call(
        functools.partial(kernel, n_kv),
        out_shape=(vmem((rows, half), BF16), vmem((heads, rows), F32)),
        in_specs=[pl.BlockSpec(memory_space=pltpu.HBM)] * 9,
        out_specs=(pl.BlockSpec(memory_space=vmem), pl.BlockSpec(memory_space=vmem)),
        scratch_shapes=[
            vmem((2, rows, half), BF16),
            vmem((nb, entries), jnp.int32),
            vmem((rows, q_cols + 2 * k_cols), F32),
            vmem((2, half, q_cols + 2 * k_cols), BF16),
            vmem((2, q_cols, half), BF16),
            vmem((2, 1, half), F32),
            vmem((2, 1, HD), F32),
            vmem((nb, n_kv * nb), F32),
            vmem((3, nb, n_kv * nb), F32),
            vmem((4, n_z, rows), F32),
            vmem((2, nb, entries), jnp.int32),
            pltpu.SMEM((2, nb, entries), jnp.int32),
            vmem((n_z, 2, MOST, BLK, LANES), BF16),
            vmem((n_z, 2, MOST, BLK, LANES), BF16),
            vmem((n_z, 2, MOST, BLK, LANES), BF16),
            vmem((nb, heads * BLK, LANES), BF16),
            vmem((1 + n_kv * nb, BLK, LANES), BF16),
            vmem((1 + n_kv * nb, BLK, LANES), BF16),
            vmem((nb, entries * BLK), F32),
            vmem((nb, heads // 2 * BLK, 2 * LANES), F32),
            vmem((rows, q_cols), BF16),
            vmem((rows, LANES), F32),
            vmem((rows, half), BF16),
            vmem((rows, half), BF16),
            dma((8,)),
            dma((2,)),
            dma((2,)),
            dma((2,)),
            dma((4, n_z)),
            dma((2,)),
            dma((2, PARTS)),
        ],
        compiler_params=pltpu.CompilerParams(
            collective_id=0, has_side_effects=True, vmem_limit_bytes=66_700_000
        ),
    )(
        tokens.reshape(rows, half), norm_gain.reshape(1, -1), w_query, w_key, w_value,
        q_gain.reshape(1, -1), k_gain.reshape(1, -1), w_out, chosen.reshape(nb, entries),
    )
    mixed, log_total = pl.pallas_call(
        write_out,
        out_shape=(
            jax.ShapeDtypeStruct((rows, half), BF16),
            jax.ShapeDtypeStruct((heads, rows), F32),
        ),
        in_specs=[pl.BlockSpec(memory_space=pl.ANY)] * 2,
        out_specs=(pl.BlockSpec(memory_space=pltpu.HBM),) * 2,
        scratch_shapes=[dma((2,))],
        compiler_params=pltpu.CompilerParams(vmem_limit_bytes=1_000_000),
    )(mixed, log_total)
    return mixed.reshape(seqs, rows, half), log_total.reshape(seqs, heads, rows)


def solution(mesh):
    in_specs = (
        P("dp", "kv", "tp"),
        P(),
        P(None, "tp"),
        P(None, "tp"),
        P(None, "tp"),
        P(),
        P(),
        P("tp", None),
        P("dp", "kv", None),
    )
    out_specs = (P("dp", "kv", "tp"), P("dp", "tp", "kv"))
    return jax.shard_map(
        functools.partial(shards, mesh.shape["kv"]),
        mesh=mesh, in_specs=in_specs, out_specs=out_specs, check_vma=False)
```
